256 devices in a mesh: rep: 2 (over z_hi), fs: 16 (over z_lo, x), tp: 8 (over y, core).
Axes of the slice: x: 4, y: 4, z: 8 (z_hi: 2, z_lo: 4; z = z_hi * 4 + z_lo), core: 2. Of those that a mesh axis runs over, the one named last changes fastest.
Arguments:
- tokens: bfloat16 [32768, 2048], P(('rep', 'fs', 'tp')), may hold values from -6 to 6
- mixer_gain: float32 [2048], replicated, may hold values from 0.1 to 1.9
- direct_weight: float32 [2048, 1024], P('fs', 'tp'), may hold values from -0.125 to 0.125
- direct_scale: float32 [1024], P('tp'), may hold values from 0.5 to 2
- value_weight: float32 [2048, 1024], P('fs', 'tp'), may hold values from -0.125 to 0.125
- value_scale: float32 [1024], P('tp'), may hold values from 0.5 to 8, as said below
- value_gain: float32 [1024], P('tp'), may hold values from 0.1 to 1.9
- value_shift: float32 [1024], P('tp'), may hold values from -3 to 3
- spatial_weight: bfloat16 [16, 128, 128], P('tp'), may hold values from -0.25 to 0.25
- spatial_bias: float32 [16, 128], P('tp'), may hold values from 0.1 to 1.9
- merge_weight: float32 [1024, 2048], P('tp', 'fs'), may hold values from -0.1875 to 0.1875
- merge_scale: float32 [2048], P('fs'), may hold values from 0.5 to 2
- channel_gain: float32 [2048], replicated, may hold values from 0.1 to 1.9
- expand_weight: float32 [2048, 8192], P('fs', 'tp'), may hold values from -0.125 to 0.125
- expand_scale: float32 [8192], P('tp'), may hold values from 0.5 to 2
- reduce_weight: float32 [8192, 2048], P('tp', 'fs'), may hold values from -0.0625 to 0.0625
- reduce_scale: float32 [2048], P('fs'), may hold values from 0.5 to 2
Outputs:
- result: bfloat16 [32768, 2048], P(('rep', 'fs', 'tp'))
The draws below stay inside these ranges and needn't reach their ends.
Inputs may be any that keep to these rules, and one draw needn't show every extreme that they name: `value_scale`: positive column scales.
All inputs are finite; a program needn't handle non-finite values.
Results may differ from the reference program's by a relative error of at most 0.024.
Values may be sent and summed in bfloat16 or wider, within the bound.
A program may use at most 64 MiB of HBM per device.

```python
import math
import jax
import jax.numpy as jnp
from jax import lax

D = 2048
GROUPS = 16
GDIM = 64
AW = 1024
FF = 8192
BLOCK = 128
TOK_DEV = 128
TOKENS = 32768
N_TP = 8


def draw_value_scale(key, part):
    ramp = jnp.exp(jnp.log(4.0) * jnp.arange(AW, dtype=jnp.float32) / (AW - 1))
    factor = jnp.exp(jax.random.uniform(key, (AW,), jnp.float32, jnp.log(0.7), jnp.log(1.4)))
    return ramp * factor


def levels(stream_key, shape, shards, low, top_value):
    level = 1.0
    for axis_at, blocks in shards:
        draws = jax.random.uniform(jax.random.fold_in(jax.random.fold_in(stream_key, 6), axis_at), (blocks,), jnp.float32, low / len(shards), top_value / len(shards))
        level = level * jnp.repeat(jnp.exp(draws), shape[axis_at] // blocks).reshape((-1,) + (1,) * (len(shape) - 1 - axis_at))
    return level


def scatter_about(rng, extent, deviation, bound, shards=(), kind=jnp.bfloat16):
    result = jax.random.normal(rng, extent, jnp.float32) * deviation
    if len(shards) > 0:
        result = levels(rng, extent, shards, -0.22, 0.18) * result
    return jnp.clip(result, min=-bound, max=bound).astype(kind)


def setup_inputs(seed: int = 0) -> dict:
    seeds = jax.random.split(jax.random.key(seed), 18)
    tokens = scatter_about(seeds[0], (TOKENS, D), 1.0, 6.0, ((0, 256),))
    mixer_gain = jnp.clip(1.0 + 0.18 * jax.random.normal(seeds[1], (D,), jnp.float32), 0.1, 1.9)
    direct_weight = scatter_about(seeds[2], (D, AW), D ** -0.5, 0.125, ((0, 16), (1, 8)), jnp.float32)
    direct_scale = jnp.clip(jnp.exp(math.log(2.0) - 1.3862944 * jax.random.uniform(seeds[3], (AW,), jnp.float32) ** levels(seeds[3], (AW,), ((0, 8),), -0.2, 0.2)), 0.5, 2.0)
    value_weight = scatter_about(seeds[4], (D, AW), D ** -0.5, 0.125, ((0, 16), (1, 8)), jnp.float32)
    value_scale = draw_value_scale(jax.random.fold_in(seeds[17], 71), 0)
    value_gain = jnp.clip(1.0 + 0.18 * jax.random.normal(seeds[6], (AW,), jnp.float32), 0.1, 1.9)
    value_shift = scatter_about(seeds[7], (AW,), 0.5, 3.0, ((0, 8),), jnp.float32)
    spatial_weight = scatter_about(seeds[8], (GROUPS, BLOCK, BLOCK), (4 * BLOCK) ** -0.5, 0.25, ((0, 8),))
    spatial_bias = jnp.clip(1.0 + 0.18 * jax.random.normal(seeds[9], (GROUPS, BLOCK), jnp.float32), 0.1, 1.9)
    merge_weight = scatter_about(seeds[10], (AW, D), AW ** -0.5, 0.1875, ((0, 8), (1, 16)), jnp.float32)
    merge_scale = jnp.clip(jnp.exp(math.log(2.0) - 1.3862944 * jax.random.uniform(seeds[11], (D,), jnp.float32) ** levels(seeds[11], (D,), ((0, 16),), -0.2, 0.2)), 0.5, 2.0)
    channel_gain = jnp.clip(1.0 + 0.18 * jax.random.normal(seeds[12], (D,), jnp.float32), 0.1, 1.9)
    expand_weight = scatter_about(seeds[13], (D, FF), D ** -0.5, 0.125, ((0, 16), (1, 8)), jnp.float32)
    expand_scale = jnp.clip(jnp.exp(math.log(2.0) - 1.3862944 * jax.random.uniform(seeds[14], (FF,), jnp.float32) ** levels(seeds[14], (FF,), ((0, 8),), -0.2, 0.2)), 0.5, 2.0)
    reduce_weight = scatter_about(seeds[15], (FF, D), FF ** -0.5, 0.0625, ((0, 8), (1, 16)), jnp.float32)
    reduce_scale = jnp.clip(jnp.exp(math.log(2.0) - 1.3862944 * jax.random.uniform(seeds[16], (D,), jnp.float32) ** levels(seeds[16], (D,), ((0, 16),), -0.2, 0.2)), 0.5, 2.0)
    return {"tokens": tokens, "mixer_gain": mixer_gain, "direct_weight": direct_weight, "direct_scale": direct_scale, "value_weight": value_weight, "value_scale": value_scale, "value_gain": value_gain, "value_shift": value_shift, "spatial_weight": spatial_weight, "spatial_bias": spatial_bias, "merge_weight": merge_weight, "merge_scale": merge_scale, "channel_gain": channel_gain, "expand_weight": expand_weight, "expand_scale": expand_scale, "reduce_weight": reduce_weight, "reduce_scale": reduce_scale}


epsilon = 1e-06

def rms_rows(rows, gain):
    floats = rows.astype(jnp.float32)
    scaled = floats * lax.rsqrt(lax.optimization_barrier(jnp.mean(floats * floats, axis=-1, keepdims=True)) + epsilon)
    return (scaled * gain).astype(jnp.bfloat16)

def split_sum(left, right, scale, parts):
    rows = left.shape[0]
    inner = left.shape[1] // parts
    lhs = left.reshape(rows, parts, inner).astype(jnp.float32)
    rhs = right.astype(jnp.bfloat16).astype(jnp.float32).reshape(parts, inner, right.shape[1])
    terms = jnp.einsum('gtk,tkd->tgd', lhs, rhs) * scale
    terms = lax.optimization_barrier(terms.astype(jnp.bfloat16)).astype(jnp.float32)
    return lax.optimization_barrier(jnp.sum(terms, axis=0))

def reference(tokens, mixer_gain, direct_weight, direct_scale, value_weight, value_scale, value_gain, value_shift, spatial_weight, spatial_bias, merge_weight, merge_scale, channel_gain, expand_weight, expand_scale, reduce_weight, reduce_scale):
    seq_rows = TOK_DEV * N_TP

    def one_sequence(rows):
        normed = rms_rows(rows, mixer_gain)
        direct = jax.nn.gelu(jnp.dot(normed, direct_weight.astype(jnp.bfloat16), preferred_element_type=jnp.float32) * direct_scale)
        value = jax.nn.gelu(jnp.dot(normed, value_weight.astype(jnp.bfloat16), preferred_element_type=jnp.float32) * value_scale)
        total = lax.optimization_barrier(jnp.sum(value, axis=1, keepdims=True))
        squares = lax.optimization_barrier(jnp.sum(value * value, axis=1, keepdims=True))
        mean = total / AW
        var = squares / AW - mean * mean
        gated_value = ((value - mean) * lax.rsqrt(var + epsilon) * value_gain + value_shift).astype(jnp.bfloat16)
        blocks = gated_value.reshape(seq_rows // BLOCK, BLOCK, GROUPS, GDIM).astype(jnp.float32)
        mixed = jnp.einsum('gpq,nqgc->npgc', spatial_weight.astype(jnp.float32), blocks)
        mixed = mixed + jnp.transpose(spatial_bias)[None, :, :, None]
        gated = (direct * mixed.reshape(seq_rows, AW)).astype(jnp.bfloat16)
        mix = split_sum(gated, merge_weight, merge_scale, N_TP)
        middle = (rows.astype(jnp.float32) + mix).astype(jnp.bfloat16)
        normed_mid = rms_rows(middle, channel_gain)
        upper = jnp.dot(normed_mid, expand_weight.astype(jnp.bfloat16), preferred_element_type=jnp.float32) * expand_scale
        hidden = jnp.square(jax.nn.relu(upper)).astype(jnp.bfloat16)
        lower = split_sum(hidden, reduce_weight, reduce_scale, N_TP)
        return (middle.astype(jnp.float32) + lower).astype(jnp.bfloat16)
    grouped = tokens.reshape(-1, seq_rows, D)
    return lax.map(one_sequence, grouped).reshape(tokens.shape)
```

```python
import functools

import jax
import jax.numpy as jnp
from jax import lax
from jax.experimental import pallas as pl
from jax.experimental.pallas import tpu as pltpu
from jax.sharding import Mesh
from jax.sharding import PartitionSpec as P

AXES = ("zh", "zl", "x", "y", "c")
FS = ("zl", "x")
TP = ("y", "c")
EPS = 1e-6
MESH = pl.DeviceIdType.MESH
F32 = jnp.float32
BF16 = jnp.bfloat16

D = 2048
R = 128
CW = 128
HW = 1024
BRANCH = 1024
SP, SN, SF, SO = 0, 1, 2, 3
CHUNK = 32
ORDER = (0, 64, 32, 96)


def gelu(u):
    return jax.nn.gelu(u, approximate=True)


class Gather:
    def __init__(self, view, a, b, pa, pb, sib, send, send_d2d, recv_a, recv_b, recv_d2d):
        self.view, self.a, self.b, self.sib = view, a, b, sib
        self.pa, self.pb = pa, pb
        self.send, self.send_d2d = send, send_d2d
        self.recv_a, self.recv_b, self.recv_d2d = recv_a, recv_b, recv_d2d

    def item(self, da, db, half=None):
        return self.view(lax.rem(self.pa + 4 - da, 4), lax.rem(self.pb + 4 - db, 4), half)

    def copy(self, ref, sem, to):
        return pltpu.make_async_remote_copy(
            src_ref=ref, dst_ref=ref, send_sem=self.send, recv_sem=sem, device_id=to, device_id_type=MESH
        )

    def along_b(self, da):
        ref = self.item(da, 0)
        self.copy(ref, self.recv_b.at[da, 0], self.b[0]).start()
        self.copy(ref, self.recv_b.at[da, 1], self.b[1]).start()

    def across(self, da, db):
        ref = self.item(da, db)
        pltpu.make_async_remote_copy(
            src_ref=ref,
            dst_ref=ref,
            send_sem=self.send_d2d,
            recv_sem=self.recv_d2d,
            device_id=self.sib,
            device_id_type=MESH,
        ).start()

    def landed(self, ref, sem):
        self.copy(ref, sem, self.sib).wait_recv()

    def near_a(self, k):
        da = (1, 3)[k]
        self.landed(self.item(da, 0), self.recv_a.at[k])
        self.copy(self.item(da, 0, k), self.recv_a.at[2 + k], self.a[k]).start()
        self.along_b(da)
        self.across(da, 0)

    def near_b(self, da):
        for k in range(2):
            db = (1, 3)[k]
            self.landed(self.item(da, db), self.recv_b.at[da, k])
            self.copy(self.item(da, db, k), self.recv_b.at[da, 2 + k], self.b[k]).start()
            self.across(da, db)

    def far_b(self, da):
        for k in range(2):
            self.landed(self.item(da, 2, k), self.recv_b.at[da, 2 + k])
        self.across(da, 2)

    def wave0(self):
        ref = self.item(0, 0)
        for k in range(2):
            self.copy(ref, self.recv_a.at[k], self.a[k]).start()
        self.along_b(0)
        self.across(0, 0)

    def wave1(self):
        for k in range(2):
            self.near_a(k)
        self.near_b(0)

    def wave2(self):
        for k in range(2):
            self.landed(self.item(2, 0, k), self.recv_a.at[2 + k])
        self.along_b(2)
        self.across(2, 0)
        self.near_b(1)
        self.near_b(3)
        self.far_b(0)

    def wave3(self):
        self.near_b(2)
        self.far_b(1)
        self.far_b(3)

    def wave4(self):
        self.far_b(2)


def kernel(
    tokens,
    mixer_gain,
    direct_weight,
    direct_scale,
    value_weight,
    value_scale,
    value_gain,
    value_shift,
    spatial_weight,
    spatial_bias,
    merge_weight,
    merge_scale,
    channel_gain,
    expand_weight,
    expand_scale,
    reduce_weight,
    reduce_scale,
    out,
    mixw,
    we,
    wr,
    xbuf,
    x2buf,
    part1,
    part2,
    rel,
    near,
    mrg,
    hbuf,
    dbuf,
    vbuf,
    gbuf,
    rbuf,
    stat,
    small,
    swb,
    bias,
    in_sem,
    ag_send,
    ag_recv,
    rs_send,
    rs_recv,
    st_send,
    st_recv,
    sm_send,
    sm_recv,
    w_send,
    w_send_d2d,
    w_recv_a,
    w_recv_b,
    w_recv_d2d,
):
    zh, zl, x, y, c = (lax.axis_index(name) for name in AXES)
    z = zh * 4 + zl
    fs = zl * 4 + x
    other = 1 - c

    def at_z(w):
        w = lax.rem(w, 8)
        return {"zh": lax.div(w, 4), "zl": lax.rem(w, 4)}

    xs = ({"x": lax.rem(x + 1, 4)}, {"x": lax.rem(x + 3, 4)})
    zs = (at_z(z + 1), at_z(z + 7))
    ynext, yprev, yfar = ({"y": lax.rem(y + k, 4)} for k in (1, 3, 2))
    sib = {"c": other}

    own_rows = pl.ds(SO * R, R)
    pltpu.make_async_copy(tokens, xbuf.at[own_rows], in_sem).start()

    barrier = pltpu.get_barrier_semaphore()
    for to in (*xs, *zs, ynext, yprev, yfar, sib):
        pl.semaphore_signal(barrier, inc=1, device_id=to, device_id_type=MESH)
    pl.semaphore_wait(barrier, 8)

    def rcopy(src, dst, ssem, rsem, to):
        return pltpu.make_async_remote_copy(
            src_ref=src, dst_ref=dst, send_sem=ssem, recv_sem=rsem, device_id=to, device_id_type=MESH
        )

    def gather_copy(buf, phase, way, k):
        if k < 4:
            src = buf.at[pl.ds(SO * R + ORDER[k], CHUNK)]
            dst = buf.at[pl.ds((SP, SN)[way] * R + ORDER[k], CHUNK)]
        else:
            row = 64 * way + CHUNK * (k - 4)
            src = buf.at[pl.ds((SP, SN)[way] * R + row, CHUNK)]
            dst = buf.at[pl.ds(SF * R + row, CHUNK)]
        return rcopy(
            src, dst, ag_send.at[phase, way, k], ag_recv.at[phase, way, k], (ynext, yprev)[way]
        )

    def gather_pass_on(buf, phase):
        for k in range(2):
            for way in range(2):
                chunk = ORDER.index(64 * way + CHUNK * k)
                gather_copy(buf, phase, way, chunk).wait_recv()
                gather_copy(buf, phase, way, 4 + k).start()

    def gather_near(buf, phase):
        for way in range(2):
            for k in range(4):
                if ORDER[k] // 64 != way:
                    gather_copy(buf, phase, way, k).wait_recv()

    def gather_far(buf, phase):
        for way in range(2):
            for k in range(2):
                gather_copy(buf, phase, way, 4 + k).wait_recv()

    def scatter_own(part, phase, way):
        rows = pl.ds(64 * (1 - way), 64)
        src = part.at[pl.ds((SN, SP)[way] * R + 64 * (1 - way), 64)]
        return rcopy(
            src,
            near.at[phase, way, rows],
            rs_send.at[phase, way, 0],
            rs_recv.at[phase, way, 0],
            (ynext, yprev)[way],
        )

    def scatter_far(part, phase, way, k):
        row = CHUNK * k
        return rcopy(
            part.at[pl.ds(SF * R + 64 * way + row, CHUNK)],
            rel.at[phase, way, pl.ds(row, CHUNK)],
            rs_send.at[phase, way, 1 + k],
            rs_recv.at[phase, way, 1 + k],
            (ynext, yprev)[way],
        )

    def scatter_joined(phase, way, k):
        row = CHUNK * k
        return rcopy(
            mrg.at[phase, way, pl.ds(row, CHUNK)],
            near.at[phase, way, pl.ds(64 * way + row, CHUNK)],
            rs_send.at[phase, way, 3 + k],
            rs_recv.at[phase, way, 3 + k],
            (ynext, yprev)[way],
        )

    def scatter_join(part, phase):
        for k in range(2):
            for way in range(2):
                row = CHUNK * k
                scatter_far(part, phase, way, k).wait_recv()
                mine = part[pl.ds((SN, SP)[way] * R + 64 * way + row, CHUNK), :].astype(F32)
                came = rel[phase, way, pl.ds(row, CHUNK), :].astype(F32)
                mrg[phase, way, pl.ds(row, CHUNK), :] = (mine + came).astype(BF16)
                scatter_joined(phase, way, k).start()

    def scatter_finish(part, phase, base, done):
        for way in range(2):
            scatter_own(part, phase, way).wait_recv()
        for k in range(2):
            for way in range(2):
                scatter_joined(phase, way, k).wait_recv()
                row = 64 * way + CHUNK * k
                total = part[pl.ds(SO * R + row, CHUNK), :].astype(F32)
                total = total + near[phase, 0, pl.ds(row, CHUNK), :].astype(F32)
                total = total + near[phase, 1, pl.ds(row, CHUNK), :].astype(F32)
                mine = base[pl.ds(SO * R + row, CHUNK), :].astype(F32)
                done(row, (mine + total).astype(BF16))

    def view_mix(low):
        def view(pz, px, half):
            row = (pz * 4 + px) * 128 + low
            if half is None:
                return mixw.at[c, pl.ds(pl.multiple_of(row, 64), 64)]
            return mixw.at[c, pl.ds(pl.multiple_of(row + 32 * half, 32), 32)]

        return view

    def view_expand(pz, px, half):
        row = (pz * 4 + px) * 128
        if half is None:
            return we.at[c, pl.ds(pl.multiple_of(row, 128), 128)]
        return we.at[c, pl.ds(pl.multiple_of(row + 64 * half, 64), 64)]

    def view_reduce(pz, px, half):
        row = c * HW
        if half is None:
            return wr.at[pz * 4 + px, pl.ds(pl.multiple_of(row, HW), HW)]
        return wr.at[pz * 4 + px, pl.ds(pl.multiple_of(row + 512 * half, 512), 512)]

    def weight(index, view, x_first):
        if x_first:
            a, b, pa, pb, turned = xs, zs, x, zl, lambda p, q, h: view(q, p, h)
        else:
            a, b, pa, pb, turned = zs, xs, zl, x, view
        return Gather(
            turned,
            a,
            b,
            pa,
            pb,
            sib,
            w_send.at[index],
            w_send_d2d.at[index],
            w_recv_a.at[index],
            w_recv_b.at[index],
            w_recv_d2d.at[index],
        )

    mix_a = weight(0, view_mix(0), True)
    mix_b = weight(1, view_mix(64), False)
    expand = weight(2, view_expand, True)
    reduce = weight(3, view_reduce, False)

    def column(row):
        return jnp.transpose(jnp.broadcast_to(row, (128, 128)))

    pltpu.make_async_copy(tokens, xbuf.at[own_rows], in_sem).wait()
    for k in range(4):
        for way in range(2):
            gather_copy(xbuf, 0, way, k).start()

    fs_row = pl.ds(pl.multiple_of(fs * 128, 128), 128)
    gain = column(mixer_gain[pl.ds(fs, 1), :])
    mixw[c, fs_row, 0:128] = (direct_weight[...] * gain * direct_scale[...]).astype(BF16)
    mixw[c, fs_row, 128:256] = (value_weight[...] * gain * value_scale[...]).astype(BF16)
    mixw[c, fs_row, 256:384] = (merge_weight[...] * merge_scale[...]).astype(BF16)
    mix_a.wave0()
    mix_b.wave0()
    small[c, 0:1, :] = value_gain[...]
    small[c, 1:2, :] = value_shift[...]
    small[c, 2:4, :] = spatial_bias[...]
    small[c, 4:8, :] = jnp.zeros((4, 128), F32)
    swb[c] = spatial_weight[...]
    small_copy = rcopy(small.at[c], small.at[c], sm_send.at[0], sm_recv.at[0], sib)
    spatial_copy = rcopy(spatial_weight, swb.at[c], sm_send.at[1], sm_recv.at[1], sib)
    small_copy.start()
    spatial_copy.start()

    gain = column(channel_gain[pl.ds(fs, 1), :])
    for k in range(8):
        lanes = slice(k * 128, (k + 1) * 128)
        we[c, fs_row, lanes] = (expand_weight[:, lanes] * gain * expand_scale[:, lanes]).astype(BF16)
    for k in range(8):
        rows = pl.ds(pl.multiple_of(c * HW + k * 128, 128), 128)
        wr[fs, rows, :] = (reduce_weight[k * 128 : (k + 1) * 128, :] * reduce_scale[...]).astype(BF16)

    mix_a.wave1()
    mix_b.wave1()
    mix_a.wave2()
    mix_b.wave2()
    gather_pass_on(xbuf, 0)
    mix_a.wave3()
    mix_b.wave3()
    expand.wave0()
    reduce.wave0()
    mix_a.wave4()
    mix_b.wave4()

    def row_scales(buf, pair):
        @pl.loop(0, 8)
        def _(i):
            rows = pl.ds(pl.multiple_of(pair * 256 + i * 32, 32), 32)
            floats = buf[rows, :].astype(F32)
            power = jnp.mean(floats * floats, axis=-1, keepdims=True)
            rbuf[rows, :] = jnp.broadcast_to(lax.rsqrt(power + EPS), (32, 128))

    lane = lax.broadcasted_iota(jnp.int32, (128, 128), 1)
    block_of = {SP: lax.rem(y + 3, 4), SN: lax.rem(y + 1, 4), SF: lax.rem(y + 2, 4), SO: y}

    def project(pair):
        row_scales(xbuf, pair)
        for s in range(2):
            rows = pl.ds(pair * 256, 256)
            scale = rbuf[rows, :]
            both = jnp.dot(xbuf[rows, :], mixw[s, :, 0:256], preferred_element_type=F32)
            dbuf[rows, s * 128 : (s + 1) * 128] = both[:, 0:128] * scale
            vbuf[rows, s * 128 : (s + 1) * 128] = gelu(both[:, 128:256] * scale)
        for s in range(2):
            slot = pair * 2 + s
            v = vbuf[pl.ds(slot * R, R), :]
            total = jnp.sum(v, axis=1, keepdims=True)
            squares = jnp.sum(v * v, axis=1, keepdims=True)
            tile = jnp.where(lane == 0, total, jnp.where(lane == 1, squares, 0.0))
            stat[0, block_of[slot]] = jnp.transpose(tile)[0:8, :]

    def mixing(pair):
        for s in range(2):
            slot = pair * 2 + s
            rows = pl.ds(slot * R, R)
            block = block_of[slot]
            sums = stat[0, block] + stat[1, block] + stat[2, block] + stat[3, block]
            tile = jnp.transpose(jnp.concatenate([sums] * 16, axis=0))
            mean = tile[:, 0:1] / BRANCH
            var = tile[:, 1:2] / BRANCH - mean * mean
            inv = lax.rsqrt(var + EPS)
            for k in range(2):
                lanes = slice(k * 128, (k + 1) * 128)
                v = vbuf[rows, lanes]
                g = ((v - mean) * inv * small[k, 0:1, :] + small[k, 1:2, :]).astype(BF16)
                low = jnp.dot(swb[k, 0], g, preferred_element_type=F32)
                high = jnp.dot(swb[k, 1], g, preferred_element_type=F32)
                mixed = jnp.where(lane < 64, low, high) + bias[k]
                gbuf[rows, lanes] = (gelu(dbuf[rows, lanes]) * mixed).astype(BF16)
        rows = pl.ds(pair * 256, 256)

        @pl.loop(0, 8)
        def _(j):
            first = pl.ds(pl.multiple_of(j * 256, 128), 128)
            second = pl.ds(pl.multiple_of(j * 256 + 128, 128), 128)
            weights = jnp.concatenate(
                [
                    jnp.concatenate([mixw[k, first, 256:384], mixw[k, second, 256:384]], axis=1)
                    for k in range(2)
                ],
                axis=0,
            )
            product = jnp.dot(gbuf[rows, :], weights, preferred_element_type=F32)
            part1[rows, pl.ds(pl.multiple_of(j * 256, 256), 256)] = product.astype(BF16)

    def feed(pair):
        rows = pl.ds(pair * 256, 256)
        row_scales(x2buf, pair)

        @pl.loop(0, 8)
        def _(j):
            cols = pl.ds(pl.multiple_of(lax.rem(j, 4) * 256, 256), 256)
            upper = jnp.dot(x2buf[rows, :], we[lax.div(j, 4), :, cols], preferred_element_type=F32)
            scale = rbuf[rows, :]
            upper = upper * jnp.concatenate([scale, scale], axis=1)
            hidden = jnp.square(jnp.maximum(upper, 0.0)).astype(BF16)
            hbuf[:, pl.ds(pl.multiple_of(j * 256, 256), 256)] = hidden

        @pl.loop(0, 8)
        def _(j):
            weights = jnp.concatenate([wr[2 * j], wr[2 * j + 1]], axis=1)
            product = jnp.dot(hbuf[...], weights, preferred_element_type=F32)
            part2[rows, pl.ds(pl.multiple_of(j * 256, 256), 256)] = product.astype(BF16)

    gather_near(xbuf, 0)
    pltpu.make_async_remote_copy(
        src_ref=mixw.at[other, pl.ds(0, 1024)],
        dst_ref=mixw.at[other, pl.ds(0, 1024)],
        send_sem=w_send_d2d.at[0],
        recv_sem=w_recv_d2d.at[0],
        device_id=sib,
        device_id_type=MESH,
    ).wait_recv()
    pltpu.make_async_remote_copy(
        src_ref=mixw.at[other, pl.ds(1024, 1024)],
        dst_ref=mixw.at[other, pl.ds(1024, 1024)],
        send_sem=w_send_d2d.at[1],
        recv_sem=w_recv_d2d.at[1],
        device_id=sib,
        device_id_type=MESH,
    ).wait_recv()
    project(0)
    gather_far(xbuf, 0)
    project(1)
    stat_copies = [
        rcopy(stat.at[0], stat.at[k + 1], st_send.at[k], st_recv.at[k], to)
        for k, to in enumerate((ynext, yprev, yfar))
    ]
    for copy in stat_copies:
        copy.start()
    rcopy(small.at[other], small.at[other], sm_send.at[0], sm_recv.at[0], sib).wait_recv()
    rcopy(swb.at[other], swb.at[other], sm_send.at[1], sm_recv.at[1], sib).wait_recv()
    for k in range(2):
        rows = jnp.concatenate(
            [jnp.broadcast_to(small[k, 2 + g : 3 + g, :], (64, 128)) for g in range(2)], axis=0
        )
        bias[k] = jnp.transpose(rows)
    for copy in stat_copies:
        copy.wait_recv()
    mixing(0)
    for way in range(2):
        scatter_own(part1, 0, way).start()
    mixing(1)
    for k in range(2):
        for way in range(2):
            scatter_far(part1, 0, way, k).start()
    expand.wave1()
    reduce.wave1()
    scatter_join(part1, 0)

    def middle_done(row, value):
        x2buf[pl.ds(SO * R + row, CHUNK), :] = value
        for way in range(2):
            gather_copy(x2buf, 1, way, ORDER.index(row)).start()

    scatter_finish(part1, 0, xbuf, middle_done)
    expand.wave2()
    reduce.wave2()
    gather_pass_on(x2buf, 1)
    expand.wave3()
    reduce.wave3()
    expand.wave4()
    reduce.wave4()

    gather_near(x2buf, 1)
    rcopy(we.at[other], we.at[other], w_send_d2d.at[2], w_recv_d2d.at[2], sib).wait_recv()
    half = wr.at[:, pl.ds(pl.multiple_of(other * HW, HW), HW)]
    rcopy(half, half, w_send_d2d.at[3], w_recv_d2d.at[3], sib).wait_recv()
    feed(0)
    for way in range(2):
        scatter_own(part2, 1, way).start()
    gather_far(x2buf, 1)
    feed(1)
    for k in range(2):
        for way in range(2):
            scatter_far(part2, 1, way, k).start()
    scatter_join(part2, 1)

    def result_done(row, value):
        out[pl.ds(row, CHUNK), :] = value

    scatter_finish(part2, 1, x2buf, result_done)

    for phase, buf, part in ((0, xbuf, part1), (1, x2buf, part2)):
        for way in range(2):
            for k in range(6):
                gather_copy(buf, phase, way, k).wait_send()
            scatter_own(part, phase, way).wait_send()
            for k in range(2):
                scatter_far(part, phase, way, k).wait_send()
                scatter_joined(phase, way, k).wait_send()
    for copy in (*stat_copies, small_copy, spatial_copy):
        copy.wait_send()
    sent = (
        (mixw.at[c, pl.ds(0, 960)], mixw.at[c, pl.ds(0, 1024)]),
        (mixw.at[c, pl.ds(0, 960)], mixw.at[c, pl.ds(0, 1024)]),
        (we.at[c, pl.ds(0, 1920)], we.at[c]),
        (wr.at[pl.ds(0, 15), pl.ds(0, HW)], wr.at[:, pl.ds(0, HW)]),
    )
    for index, (torus, across) in enumerate(sent):
        rcopy(torus, torus, w_send.at[index], w_recv_d2d.at[index], sib).wait_send()
        rcopy(across, across, w_send_d2d.at[index], w_recv_d2d.at[index], sib).wait_send()


def layer(*args):
    (
        tokens,
        mixer_gain,
        direct_weight,
        direct_scale,
        value_weight,
        value_scale,
        value_gain,
        value_shift,
        spatial_weight,
        spatial_bias,
        merge_weight,
        merge_scale,
        channel_gain,
        expand_weight,
        expand_scale,
        reduce_weight,
        reduce_scale,
    ) = args
    operands = (
        tokens,
        mixer_gain.reshape(16, 128),
        direct_weight,
        direct_scale.reshape(1, CW),
        value_weight,
        value_scale.reshape(1, CW),
        value_gain.reshape(1, CW),
        value_shift.reshape(1, CW),
        spatial_weight,
        spatial_bias,
        merge_weight,
        merge_scale.reshape(1, 128),
        channel_gain.reshape(16, 128),
        expand_weight,
        expand_scale.reshape(1, HW),
        reduce_weight,
        reduce_scale.reshape(1, 128),
    )
    vmem = pl.BlockSpec(memory_space=pltpu.VMEM)
    dma = pltpu.SemaphoreType.DMA
    return pl.pallas_call(
        kernel,
        out_shape=jax.ShapeDtypeStruct((R, D), BF16),
        in_specs=[pl.BlockSpec(memory_space=pl.ANY)] + [vmem] * 16,
        out_specs=vmem,
        scratch_shapes=[
            pltpu.VMEM((2, D, 384), BF16),
            pltpu.VMEM((2, D, HW), BF16),
            pltpu.VMEM((16, 2 * HW, 128), BF16),
            pltpu.VMEM((4 * R, D), BF16),
            pltpu.VMEM((4 * R, D), BF16),
            pltpu.VMEM((4 * R, D), BF16),
            pltpu.VMEM((4 * R, D), BF16),
            pltpu.VMEM((2, 2, 64, D), BF16),
            pltpu.VMEM((2, 2, R, D), BF16),
            pltpu.VMEM((2, 2, 64, D), BF16),
            pltpu.VMEM((2 * R, D), BF16),
            pltpu.VMEM((4 * R, 256), F32),
            pltpu.VMEM((4 * R, 256), F32),
            pltpu.VMEM((4 * R, 256), BF16),
            pltpu.VMEM((4 * R, 128), F32),
            pltpu.VMEM((4, 4, 8, 128), F32),
            pltpu.VMEM((2, 8, 128), F32),
            pltpu.VMEM((2, 2, 128, 128), BF16),
            pltpu.VMEM((2, 128, 128), F32),
            dma,
            dma((2, 2, 6)),
            dma((2, 2, 6)),
            dma((2, 2, 5)),
            dma((2, 2, 5)),
            dma((3,)),
            dma((3,)),
            dma((2,)),
            dma((2,)),
            dma((4,)),
            dma((4,)),
            dma((4, 4)),
            dma((4, 4, 4)),
            dma((4,)),
        ],
        compiler_params=pltpu.CompilerParams(
            collective_id=0, has_side_effects=True, vmem_limit_bytes=60 * 1024 * 1024
        ),
        name="layer",
    )(*operands)


def solution(mesh):
    finer = Mesh(mesh.devices.reshape(2, 4, 4, 4, 2), AXES)
    in_specs = (
        P(AXES, None),
        P(),
        P(FS, TP),
        P(TP),
        P(FS, TP),
        P(TP),
        P(TP),
        P(TP),
        P(TP, None, None),
        P(TP, None),
        P(TP, FS),
        P(FS),
        P(),
        P(FS, TP),
        P(TP),
        P(TP, FS),
        P(FS),
    )
    return jax.shard_map(layer, mesh=finer, in_specs=in_specs, out_specs=P(AXES, None), check_vma=False)
```

```python
import functools

import jax
import jax.numpy as jnp
from jax import lax
from jax.experimental import pallas as pl
from jax.experimental.pallas import tpu as pltpu
from jax.sharding import Mesh
from jax.sharding import PartitionSpec as P

AXES = ("zh", "zl", "x", "y", "c")
FS = ("zl", "x")
TP = ("y", "c")
EPS = 1e-6
MESH = pl.DeviceIdType.MESH
F32 = jnp.float32
BF16 = jnp.bfloat16

D = 2048
R = 128
CW = 128
HW = 1024
BRANCH = 1024
SN, SP, SF, SO = 0, 1, 2, 3
CHUNK = 32


def gelu(u):
    return jax.nn.gelu(u, approximate=True)


class Gather:
    def __init__(self, view, a, b, pa, pb, sib, send, send_d2d, recv_a, recv_b, recv_d2d):
        self.view, self.a, self.b, self.sib = view, a, b, sib
        self.pa, self.pb = pa, pb
        self.send, self.send_d2d = send, send_d2d
        self.recv_a, self.recv_b, self.recv_d2d = recv_a, recv_b, recv_d2d

    def item(self, da, db, half=None):
        return self.view(lax.rem(self.pa + 4 - da, 4), lax.rem(self.pb + 4 - db, 4), half)

    def copy(self, ref, sem, to):
        return pltpu.make_async_remote_copy(
            src_ref=ref, dst_ref=ref, send_sem=self.send, recv_sem=sem, device_id=to, device_id_type=MESH
        )

    def along_b(self, da):
        ref = self.item(da, 0)
        self.copy(ref, self.recv_b.at[da, 0], self.b[0]).start()
        self.copy(ref, self.recv_b.at[da, 1], self.b[1]).start()

    def across(self, da, db):
        ref = self.item(da, db)
        pltpu.make_async_remote_copy(
            src_ref=ref,
            dst_ref=ref,
            send_sem=self.send_d2d,
            recv_sem=self.recv_d2d,
            device_id=self.sib,
            device_id_type=MESH,
        ).start()

    def landed(self, ref, sem):
        self.copy(ref, sem, self.sib).wait_recv()

    def near_a(self, k):
        da = (1, 3)[k]
        self.landed(self.item(da, 0), self.recv_a.at[k])
        self.copy(self.item(da, 0, k), self.recv_a.at[2 + k], self.a[k]).start()
        self.along_b(da)
        self.across(da, 0)

    def near_b(self, da):
        for k in range(2):
            db = (1, 3)[k]
            self.landed(self.item(da, db), self.recv_b.at[da, k])
            self.copy(self.item(da, db, k), self.recv_b.at[da, 2 + k], self.b[k]).start()
            self.across(da, db)

    def far_b(self, da):
        for k in range(2):
            self.landed(self.item(da, 2, k), self.recv_b.at[da, 2 + k])
        self.across(da, 2)

    def wave0(self):
        ref = self.item(0, 0)
        for k in range(2):
            self.copy(ref, self.recv_a.at[k], self.a[k]).start()
        self.along_b(0)
        self.across(0, 0)

    def wave1(self):
        for k in range(2):
            self.near_a(k)
        self.near_b(0)

    def wave2(self):
        for k in range(2):
            self.landed(self.item(2, 0, k), self.recv_a.at[2 + k])
        self.along_b(2)
        self.across(2, 0)
        self.near_b(1)
        self.near_b(3)
        self.far_b(0)

    def wave3(self):
        self.near_b(2)
        self.far_b(1)
        self.far_b(3)

    def wave4(self):
        self.far_b(2)


def kernel(
    tokens,
    mixer_gain_hbm,
    direct_weight_hbm,
    direct_scale_hbm,
    value_weight_hbm,
    value_scale_hbm,
    value_gain_hbm,
    value_shift_hbm,
    spatial_weight_hbm,
    spatial_bias_hbm,
    merge_weight_hbm,
    merge_scale_hbm,
    channel_gain_hbm,
    expand_weight_hbm,
    expand_scale_hbm,
    reduce_weight_hbm,
    reduce_scale_hbm,
    out,
    mixer_gain,
    direct_weight,
    direct_scale,
    value_weight,
    value_scale,
    value_gain,
    value_shift,
    spatial_weight,
    spatial_bias,
    merge_weight,
    merge_scale,
    channel_gain,
    expand_weight,
    expand_scale,
    reduce_weight,
    reduce_scale,
    valw,
    dmw,
    we,
    wr,
    xbuf,
    x2buf,
    part1,
    part2,
    rel,
    near,
    mrg,
    hbuf,
    dbuf,
    vbuf,
    gbuf,
    rbuf,
    stat,
    small,
    swb,
    bias,
    in_sem,
    ag_send,
    ag_recv,
    rs_send,
    rs_recv,
    st_send,
    st_recv,
    sm_send,
    sm_recv,
    w_send,
    w_send_d2d,
    w_recv_a,
    w_recv_b,
    w_recv_d2d,
):
    zh, zl, x, y, c = (lax.axis_index(name) for name in AXES)
    z = zh * 4 + zl
    fs = zl * 4 + x
    other = 1 - c
    scope = jax.named_scope

    def at_z(w):
        w = lax.rem(w, 8)
        return {"zh": lax.div(w, 4), "zl": lax.rem(w, 4)}

    xs = ({"x": lax.rem(x + 1, 4)}, {"x": lax.rem(x + 3, 4)})
    zs = (at_z(z + 1), at_z(z + 7))
    ynext, yprev, yfar = ({"y": lax.rem(y + k, 4)} for k in (1, 3, 2))
    sib = {"c": other}

    barrier = pltpu.get_barrier_semaphore()
    for to in (*xs, *zs, ynext, yprev, yfar, sib):
        pl.semaphore_signal(barrier, inc=1, device_id=to, device_id_type=MESH)

    inputs = [
        pltpu.make_async_copy(src, dst, in_sem.at[k])
        for k, (src, dst) in enumerate(
            (
                (tokens, xbuf.at[pl.ds(SO * R, R)]),
                (mixer_gain_hbm, mixer_gain),
                (direct_weight_hbm, direct_weight),
                (direct_scale_hbm, direct_scale),
                (value_weight_hbm, value_weight),
                (value_scale_hbm, value_scale),
                (merge_weight_hbm, merge_weight),
                (merge_scale_hbm, merge_scale),
                (channel_gain_hbm, channel_gain),
                (expand_weight_hbm, expand_weight),
                (expand_scale_hbm, expand_scale),
                (reduce_weight_hbm, reduce_weight),
                (reduce_scale_hbm, reduce_scale),
                (value_gain_hbm, value_gain),
                (value_shift_hbm, value_shift),
                (spatial_bias_hbm, spatial_bias),
                (spatial_weight_hbm, spatial_weight),
            )
        )
    ]
    for copy in inputs:
        copy.start()

    def rcopy(src, dst, ssem, rsem, to):
        return pltpu.make_async_remote_copy(
            src_ref=src, dst_ref=dst, send_sem=ssem, recv_sem=rsem, device_id=to, device_id_type=MESH
        )

    def gather_copy(buf, phase, way, k):
        if k < 4:
            src = buf.at[pl.ds(SO * R + CHUNK * k, CHUNK)]
            dst = buf.at[pl.ds((SP, SN)[way] * R + CHUNK * k, CHUNK)]
        else:
            row = 64 * way + CHUNK * (k - 4)
            src = buf.at[pl.ds((SP, SN)[way] * R + row, CHUNK)]
            dst = buf.at[pl.ds(SF * R + row, CHUNK)]
        return rcopy(
            src, dst, ag_send.at[phase, way, k], ag_recv.at[phase, way, k], (ynext, yprev)[way]
        )

    def gather_pass_on(buf, phase, k):
        for way in range(2):
            gather_copy(buf, phase, way, 2 * way + k).wait_recv()
            gather_copy(buf, phase, way, 4 + k).start()

    def gather_near(buf, phase):
        for way in range(2):
            for k in range(2):
                gather_copy(buf, phase, way, 2 * (1 - way) + k).wait_recv()

    def gather_far(buf, phase):
        for way in range(2):
            for k in range(2):
                gather_copy(buf, phase, way, 4 + k).wait_recv()

    def scatter_own(part, phase, way):
        rows = pl.ds(64 * (1 - way), 64)
        src = part.at[pl.ds((SN, SP)[way] * R + 64 * (1 - way), 64)]
        return rcopy(
            src,
            near.at[phase, way, rows],
            rs_send.at[phase, way, 0],
            rs_recv.at[phase, way, 0],
            (ynext, yprev)[way],
        )

    def scatter_far(part, phase, way, k):
        row = CHUNK * k
        return rcopy(
            part.at[pl.ds(SF * R + 64 * way + row, CHUNK)],
            rel.at[phase, way, pl.ds(row, CHUNK)],
            rs_send.at[phase, way, 1 + k],
            rs_recv.at[phase, way, 1 + k],
            (ynext, yprev)[way],
        )

    def scatter_joined(phase, way, k):
        row = CHUNK * k
        return rcopy(
            mrg.at[phase, way, pl.ds(row, CHUNK)],
            near.at[phase, way, pl.ds(64 * way + row, CHUNK)],
            rs_send.at[phase, way, 3 + k],
            rs_recv.at[phase, way, 3 + k],
            (ynext, yprev)[way],
        )

    def scatter_join(part, phase, k):
        for way in range(2):
            row = CHUNK * k
            scatter_far(part, phase, way, k).wait_recv()
            mine = part[pl.ds((SN, SP)[way] * R + 64 * way + row, CHUNK), :].astype(F32)
            came = rel[phase, way, pl.ds(row, CHUNK), :].astype(F32)
            mrg[phase, way, pl.ds(row, CHUNK), :] = (mine + came).astype(BF16)
            scatter_joined(phase, way, k).start()

    def scatter_finish(part, phase, base, done, k):
        if k == 0:
            for way in range(2):
                scatter_own(part, phase, way).wait_recv()
        for way in range(2):
            scatter_joined(phase, way, k).wait_recv()
            row = 64 * way + CHUNK * k
            total = part[pl.ds(SO * R + row, CHUNK), :].astype(F32)
            total = total + near[phase, 0, pl.ds(row, CHUNK), :].astype(F32)
            total = total + near[phase, 1, pl.ds(row, CHUNK), :].astype(F32)
            mine = base[pl.ds(SO * R + row, CHUNK), :].astype(F32)
            done(row, (mine + total).astype(BF16))

    def view_rows(ref, low):
        def view(pz, px, half):
            row = (pz * 4 + px) * 128 + low
            if half is None:
                return ref.at[c, pl.ds(pl.multiple_of(row, 64), 64)]
            return ref.at[c, pl.ds(pl.multiple_of(row + 32 * half, 32), 32)]

        return view

    def view_reduce(low):
        def view(pz, px, half):
            row = c * HW + low
            if half is None:
                return wr.at[pz * 4 + px, pl.ds(pl.multiple_of(row, 512), 512)]
            return wr.at[pz * 4 + px, pl.ds(pl.multiple_of(row + 256 * half, 256), 256)]

        return view

    def weight(index, view, x_first):
        if x_first:
            a, b, pa, pb, turned = xs, zs, x, zl, lambda p, q, h: view(q, p, h)
        else:
            a, b, pa, pb, turned = zs, xs, zl, x, view
        return Gather(
            turned,
            a,
            b,
            pa,
            pb,
            sib,
            w_send.at[index],
            w_send_d2d.at[index],
            w_recv_a.at[index],
            w_recv_b.at[index],
            w_recv_d2d.at[index],
        )

    class Pair:
        def __init__(self, index, low, high):
            self.halves = (weight(index, low, True), weight(index + 1, high, False))

        def wave(self, k):
            for half in self.halves:
                getattr(half, f"wave{k}")()

    value_blocks = Pair(0, view_rows(valw, 0), view_rows(valw, 64))
    dm_blocks = Pair(2, view_rows(dmw, 0), view_rows(dmw, 64))
    expand_blocks = Pair(4, view_rows(we, 0), view_rows(we, 64))
    reduce_blocks = Pair(6, view_reduce(0), view_reduce(512))

    def column(row):
        return jnp.transpose(jnp.broadcast_to(row, (128, 128)))

    with scope("wait_tokens"):
        inputs[0].wait()
    with scope("wait_barrier"):
        pl.semaphore_wait(barrier, 8)
    for k in range(4):
        for way in range(2):
            gather_copy(xbuf, 0, way, (k + 2 * way) % 4).start()
    with scope("wait_mix"):
        for copy in inputs[1:8]:
            copy.wait()

    fs_row = pl.ds(pl.multiple_of(fs * 128, 128), 128)
    gain = column(mixer_gain[pl.ds(fs, 1), :])
    valw[c, fs_row, :] = (value_weight[...] * gain * value_scale[...]).astype(BF16)
    dmw[c, fs_row, 0:128] = (direct_weight[...] * gain * direct_scale[...]).astype(BF16)
    dmw[c, fs_row, 128:256] = (merge_weight[...] * merge_scale[...]).astype(BF16)
    value_blocks.wave(0)
    dm_blocks.wave(0)
    for copy in inputs[8:]:
        copy.wait()
    gain = column(channel_gain[pl.ds(fs, 1), :])
    for k in range(8):
        lanes = slice(k * 128, (k + 1) * 128)
        we[c, fs_row, lanes] = (expand_weight[:, lanes] * gain * expand_scale[:, lanes]).astype(BF16)
    for k in range(8):
        rows = pl.ds(pl.multiple_of(c * HW + k * 128, 128), 128)
        wr[fs, rows, :] = (reduce_weight[k * 128 : (k + 1) * 128, :] * reduce_scale[...]).astype(BF16)
    small[c, 0:1, :] = value_gain[...]
    small[c, 1:2, :] = value_shift[...]
    small[c, 2:4, :] = spatial_bias[...]
    small[c, 4:8, :] = jnp.zeros((4, 128), F32)
    swb[c] = spatial_weight[...]
    small_copy = rcopy(small.at[c], small.at[c], sm_send.at[0], sm_recv.at[0], sib)
    spatial_copy = rcopy(spatial_weight, swb.at[c], sm_send.at[1], sm_recv.at[1], sib)
    small_copy.start()
    spatial_copy.start()

    with scope("v_w1"):
        value_blocks.wave(1)
    with scope("dm_w1"):
        dm_blocks.wave(1)
    expand_blocks.halves[0].wave0()
    with scope("v_w2"):
        value_blocks.wave(2)
    with scope("pass1_0"):
        gather_pass_on(xbuf, 0, 0)
    with scope("dm_w2"):
        dm_blocks.wave(2)
    with scope("v_w3"):
        value_blocks.wave(3)
    expand_blocks.halves[1].wave0()
    with scope("pass1_1"):
        gather_pass_on(xbuf, 0, 1)
    with scope("dm_w3"):
        dm_blocks.wave(3)
    with scope("v_w4"):
        value_blocks.wave(4)
    with scope("e_w1"):
        expand_blocks.wave(1)

    def row_scales(buf, start, count):
        @pl.loop(0, count // 32)
        def _(i):
            rows = pl.ds(pl.multiple_of(start + i * 32, 32), 32)
            floats = buf[rows, :].astype(F32)
            power = jnp.mean(floats * floats, axis=-1, keepdims=True)
            rbuf[rows, :] = jnp.broadcast_to(lax.rsqrt(power + EPS), (32, 128))

    lane = lax.broadcasted_iota(jnp.int32, (128, 128), 1)
    block_of = {SP: lax.rem(y + 3, 4), SN: lax.rem(y + 1, 4), SF: lax.rem(y + 2, 4), SO: y}

    def project(slots):
        start, count = slots[0] * R, len(slots) * R
        row_scales(xbuf, start, count)
        rows = pl.ds(start, count)
        weights = jnp.concatenate([valw[0], valw[1]], axis=1)
        value = jnp.dot(xbuf[rows, :], weights, preferred_element_type=F32)
        scale = rbuf[rows, :]
        vbuf[rows, :] = gelu(value * jnp.concatenate([scale, scale], axis=1))
        for slot in slots:
            v = vbuf[pl.ds(slot * R, R), :]
            total = jnp.sum(v, axis=1, keepdims=True)
            squares = jnp.sum(v * v, axis=1, keepdims=True)
            tile = jnp.where(lane == 0, total, jnp.where(lane == 1, squares, 0.0))
            stat[0, block_of[slot]] = jnp.transpose(tile)[0:8, :]

    def project_direct():
        weights = jnp.concatenate([dmw[0, :, 0:128], dmw[1, :, 0:128]], axis=1)

        @pl.loop(0, 2)
        def _(i):
            rows = pl.ds(pl.multiple_of(i * 256, 256), 256)
            direct = jnp.dot(xbuf[rows, :], weights, preferred_element_type=F32)
            scale = rbuf[rows, :]
            dbuf[rows, :] = gelu(direct * jnp.concatenate([scale, scale], axis=1))

    def mixing(slots):
        for slot in slots:
            rows = pl.ds(slot * R, R)
            block = block_of[slot]
            sums = stat[0, block] + stat[1, block] + stat[2, block] + stat[3, block]
            tile = jnp.transpose(jnp.concatenate([sums] * 16, axis=0))
            mean = tile[:, 0:1] / BRANCH
            var = tile[:, 1:2] / BRANCH - mean * mean
            inv = lax.rsqrt(var + EPS)
            for k in range(2):
                lanes = slice(k * 128, (k + 1) * 128)
                v = vbuf[rows, lanes]
                g = ((v - mean) * inv * small[k, 0:1, :] + small[k, 1:2, :]).astype(BF16)
                low = jnp.dot(swb[k, 0], g, preferred_element_type=F32)
                high = jnp.dot(swb[k, 1], g, preferred_element_type=F32)
                mixed = jnp.where(lane < 64, low, high) + bias[k]
                gbuf[rows, lanes] = (dbuf[rows, lanes] * mixed).astype(BF16)
        rows = pl.ds(slots[0] * R, len(slots) * R)

        @pl.loop(0, 2)
        def _(j):
            weights = jnp.concatenate(
                [
                    jnp.concatenate(
                        [
                            dmw[k, pl.ds(pl.multiple_of(j * 1024 + i * 128, 128), 128), 128:256]
                            for i in range(8)
                        ],
                        axis=1,
                    )
                    for k in range(2)
                ],
                axis=0,
            )
            product = jnp.dot(gbuf[rows, :], weights, preferred_element_type=F32)
            part1[rows, pl.ds(pl.multiple_of(j * 1024, 1024), 1024)] = product.astype(BF16)

    def gathered_rows(ref, pieces):
        loaded = [ref[pl.ds(start, count), :] for start, count in pieces]
        return loaded[0] if len(loaded) == 1 else jnp.concatenate(loaded, axis=0)

    def store_rows(ref, pieces, cols, values):
        at = 0
        for start, count in pieces:
            ref[pl.ds(start, count), cols] = values[at : at + count, :]
            at += count

    def feed_up(pieces):
        for start, count in pieces:
            row_scales(x2buf, start, count)

        @pl.loop(0, 2)
        def _(j):
            upper = jnp.dot(gathered_rows(x2buf, pieces), we[j], preferred_element_type=F32)
            upper = upper * jnp.concatenate([gathered_rows(rbuf, pieces)] * 8, axis=1)
            hidden = jnp.square(jnp.maximum(upper, 0.0)).astype(BF16)
            store_rows(hbuf, pieces, pl.ds(pl.multiple_of(j * HW, HW), HW), hidden)

    def feed_down(pieces):
        @pl.loop(0, 2)
        def _(j):
            weights = jnp.concatenate([wr[8 * j + i] for i in range(8)], axis=1)
            product = jnp.dot(gathered_rows(hbuf, pieces), weights, preferred_element_type=F32)
            store_rows(part2, pieces, pl.ds(pl.multiple_of(j * 1024, 1024), 1024), product.astype(BF16))

    def shared(ref, index):
        rcopy(ref, ref, w_send_d2d.at[index], w_recv_d2d.at[index], sib).wait_recv()

    with scope("v_d2d"):
        shared(valw.at[other, pl.ds(0, 1024)], 0)
        shared(valw.at[other, pl.ds(1024, 1024)], 1)
    with scope("project_own"):
        project((SO,))
    with scope("dm_w4"):
        dm_blocks.wave(4)
    with scope("near1"):
        gather_near(xbuf, 0)
    with scope("project_near"):
        project((SN, SP))
    with scope("far1"):
        gather_far(xbuf, 0)
    with scope("project_far"):
        project((SF,))
    stat_copies = [
        rcopy(stat.at[0], stat.at[k + 1], st_send.at[k], st_recv.at[k], to)
        for k, to in enumerate((ynext, yprev, yfar))
    ]
    for copy in stat_copies:
        copy.start()
    reduce_blocks.wave(0)
    with scope("dm_d2d"):
        shared(dmw.at[other, pl.ds(0, 1024)], 2)
        shared(dmw.at[other, pl.ds(1024, 1024)], 3)
    with scope("direct"):
        project_direct()
        rcopy(small.at[other], small.at[other], sm_send.at[0], sm_recv.at[0], sib).wait_recv()
        rcopy(swb.at[other], swb.at[other], sm_send.at[1], sm_recv.at[1], sib).wait_recv()
        for k in range(2):
            rows = jnp.concatenate(
                [jnp.broadcast_to(small[k, 2 + g : 3 + g, :], (64, 128)) for g in range(2)], axis=0
            )
            bias[k] = jnp.transpose(rows)
    with scope("wait_stats"):
        for copy in stat_copies:
            copy.wait_recv()
    with scope("mixing_near"):
        mixing((SN, SP))
    for way in range(2):
        scatter_own(part1, 0, way).start()
    with scope("mixing_far"):
        mixing((SF,))
    for k in range(2):
        for way in range(2):
            scatter_far(part1, 0, way, k).start()
    with scope("mixing_own"):
        mixing((SO,))
    with scope("e_w2"):
        expand_blocks.wave(2)
    with scope("r_w1"):
        reduce_blocks.wave(1)
    with scope("join1_0"):
        scatter_join(part1, 0, 0)
    with scope("join1_1"):
        scatter_join(part1, 0, 1)
    with scope("e_w3"):
        expand_blocks.wave(3)

    def middle_done(row, value):
        x2buf[pl.ds(SO * R + row, CHUNK), :] = value

    with scope("finish1_0"):
        scatter_finish(part1, 0, xbuf, middle_done, 0)
    for way in range(2):
        gather_copy(x2buf, 1, way, 2 * way).start()
    with scope("finish1_1"):
        scatter_finish(part1, 0, xbuf, middle_done, 1)
    for way in range(2):
        gather_copy(x2buf, 1, way, 2 * way + 1).start()
    with scope("r_w2"):
        reduce_blocks.wave(2)
    with scope("pass2_0"):
        gather_pass_on(x2buf, 1, 0)
    with scope("e_w4"):
        expand_blocks.wave(4)
    with scope("pass2_1"):
        gather_pass_on(x2buf, 1, 1)
    for k in range(2):
        for way in range(2):
            gather_copy(x2buf, 1, way, 2 * (1 - way) + k).start()

    outer, inner = ((64, 128),), ((0, 64), (192, 64))
    far, own = ((SF * R, R),), ((SO * R, R),)
    with scope("e_d2d"):
        shared(we.at[other, pl.ds(0, 1024)], 4)
        shared(we.at[other, pl.ds(1024, 1024)], 5)
    with scope("up_outer"):
        feed_up(outer)
    with scope("r_w3"):
        reduce_blocks.wave(3)
    with scope("up_own"):
        feed_up(own)
    with scope("r_w4"):
        reduce_blocks.wave(4)
    with scope("r_d2d"):
        shared(wr.at[pl.ds(0, 8), pl.ds(pl.multiple_of(other * HW, HW), HW)], 6)
        shared(wr.at[pl.ds(8, 8), pl.ds(pl.multiple_of(other * HW, HW), HW)], 7)
    with scope("down_outer"):
        feed_down(outer)
    for way in range(2):
        scatter_own(part2, 1, way).start()
    with scope("far2"):
        gather_far(x2buf, 1)
    with scope("feed_far"):
        feed_up(far)
        feed_down(far)
    for k in range(2):
        for way in range(2):
            scatter_far(part2, 1, way, k).start()
    with scope("near2"):
        gather_near(x2buf, 1)
    with scope("feed_inner"):
        feed_up(inner)
        feed_down(inner)
    with scope("down_own"):
        feed_down(own)
    with scope("join2_0"):
        scatter_join(part2, 1, 0)
    with scope("join2_1"):
        scatter_join(part2, 1, 1)

    def result_done(row, value):
        out[pl.ds(row, CHUNK), :] = value

    with scope("finish2_0"):
        scatter_finish(part2, 1, x2buf, result_done, 0)
    with scope("finish2_1"):
        scatter_finish(part2, 1, x2buf, result_done, 1)

    with scope("drain"):
        for phase, buf, part in ((0, xbuf, part1), (1, x2buf, part2)):
            for way in range(2):
                for k in range(6):
                    gather_copy(buf, phase, way, k).wait_send()
                scatter_own(part, phase, way).wait_send()
                for k in range(2):
                    scatter_far(part, phase, way, k).wait_send()
                    scatter_joined(phase, way, k).wait_send()
        for copy in (*stat_copies, small_copy, spatial_copy):
            copy.wait_send()
        sent = (
            *[(valw.at[c, pl.ds(0, 960)], valw.at[c, pl.ds(0, 1024)])] * 2,
            *[(dmw.at[c, pl.ds(0, 960)], dmw.at[c, pl.ds(0, 1024)])] * 2,
            *[(we.at[c, pl.ds(0, 960)], we.at[c, pl.ds(0, 1024)])] * 2,
            *[(wr.at[pl.ds(0, 15), pl.ds(0, 512)], wr.at[:, pl.ds(0, 512)])] * 2,
        )
        for index, (torus, across) in enumerate(sent):
            rcopy(torus, torus, w_send.at[index], w_recv_d2d.at[index], sib).wait_send()
            rcopy(across, across, w_send_d2d.at[index], w_recv_d2d.at[index], sib).wait_send()


def layer(*args):
    (
        tokens,
        mixer_gain,
        direct_weight,
        direct_scale,
        value_weight,
        value_scale,
        value_gain,
        value_shift,
        spatial_weight,
        spatial_bias,
        merge_weight,
        merge_scale,
        channel_gain,
        expand_weight,
        expand_scale,
        reduce_weight,
        reduce_scale,
    ) = args
    operands = (
        tokens,
        mixer_gain.reshape(16, 128),
        direct_weight,
        direct_scale.reshape(1, CW),
        value_weight,
        value_scale.reshape(1, CW),
        value_gain.reshape(1, CW),
        value_shift.reshape(1, CW),
        spatial_weight,
        spatial_bias,
        merge_weight,
        merge_scale.reshape(1, 128),
        channel_gain.reshape(16, 128),
        expand_weight,
        expand_scale.reshape(1, HW),
        reduce_weight,
        reduce_scale.reshape(1, 128),
    )
    vmem = pl.BlockSpec(memory_space=pltpu.VMEM)
    dma = pltpu.SemaphoreType.DMA
    return pl.pallas_call(
        kernel,
        out_shape=jax.ShapeDtypeStruct((R, D), BF16),
        in_specs=[pl.BlockSpec(memory_space=pl.ANY)] * 17,
        out_specs=vmem,
        scratch_shapes=[
            *(pltpu.VMEM(operand.shape, operand.dtype) for operand in operands[1:]),
            pltpu.VMEM((2, D, 128), BF16),
            pltpu.VMEM((2, D, 256), BF16),
            pltpu.VMEM((2, D, HW), BF16),
            pltpu.VMEM((16, 2 * HW, 128), BF16),
            pltpu.VMEM((4 * R, D), BF16),
            pltpu.VMEM((4 * R, D), BF16),
            pltpu.VMEM((4 * R, D), BF16),
            pltpu.VMEM((4 * R, D), BF16),
            pltpu.VMEM((2, 2, 64, D), BF16),
            pltpu.VMEM((2, 2, R, D), BF16),
            pltpu.VMEM((2, 2, 64, D), BF16),
            pltpu.VMEM((4 * R, D), BF16),
            pltpu.VMEM((4 * R, 256), F32),
            pltpu.VMEM((4 * R, 256), F32),
            pltpu.VMEM((4 * R, 256), BF16),
            pltpu.VMEM((4 * R, 128), F32),
            pltpu.VMEM((4, 4, 8, 128), F32),
            pltpu.VMEM((2, 8, 128), F32),
            pltpu.VMEM((2, 2, 128, 128), BF16),
            pltpu.VMEM((2, 128, 128), F32),
            dma((17,)),
            dma((2, 2, 6)),
            dma((2, 2, 6)),
            dma((2, 2, 5)),
            dma((2, 2, 5)),
            dma((3,)),
            dma((3,)),
            dma((2,)),
            dma((2,)),
            dma((8,)),
            dma((8,)),
            dma((8, 4)),
            dma((8, 4, 4)),
            dma((8,)),
        ],
        compiler_params=pltpu.CompilerParams(
            collective_id=0, has_side_effects=True, vmem_limit_bytes=60 * 1024 * 1024
        ),
        name="layer",
    )(*operands)


def solution(mesh):
    finer = Mesh(mesh.devices.reshape(2, 4, 4, 4, 2), AXES)
    in_specs = (
        P(AXES, None),
        P(),
        P(FS, TP),
        P(TP),
        P(FS, TP),
        P(TP),
        P(TP),
        P(TP),
        P(TP, None, None),
        P(TP, None),
        P(TP, FS),
        P(FS),
        P(),
        P(FS, TP),
        P(TP),
        P(TP, FS),
        P(FS),
    )
    return jax.shard_map(layer, mesh=finer, in_specs=in_specs, out_specs=P(AXES, None), check_vma=False)
```

```python
import functools

import jax
import jax.numpy as jnp
from jax import lax
from jax.experimental import pallas as pl
from jax.experimental.pallas import tpu as pltpu
from jax.sharding import Mesh
from jax.sharding import PartitionSpec as P

AXES = ("zh", "zl", "x", "y", "c")
FS = ("zl", "x")
TP = ("y", "c")
EPS = 1e-6
MESH = pl.DeviceIdType.MESH
F32 = jnp.float32
BF16 = jnp.bfloat16

D = 2048
R = 128
CW = 128
HW = 1024
BRANCH = 1024
SN, SP, SF, SO = 0, 1, 2, 3
CHUNK = 32


def gelu(u):
    return jax.nn.gelu(u, approximate=True)


class Gather:
    def __init__(self, view, span, a, b, pa, pb, sib, send, send_d2d, recv, recv_d2d):
        self.view, self.span = view, span
        self.a, self.b, self.pa, self.pb, self.sib = a, b, pa, pb, sib
        self.send, self.send_d2d, self.recv, self.recv_d2d = send, send_d2d, recv, recv_d2d

    def item(self, da, db, half=None):
        return self.view(lax.rem(self.pa + 4 - da, 4), lax.rem(self.pb + 4 - db, 4), half)

    def copy(self, ref, stage, to):
        return pltpu.make_async_remote_copy(
            src_ref=ref,
            dst_ref=ref,
            send_sem=self.send,
            recv_sem=self.recv.at[stage],
            device_id=to,
            device_id_type=MESH,
        )

    def landed(self, stage, count):
        self.copy(self.span(count), stage, self.sib).wait_recv()

    def along_b(self, da, stage):
        for k in range(2):
            self.copy(self.item(da, 0), stage, self.b[k]).start()

    def across(self, da, db):
        ref = self.item(da, db)
        pltpu.make_async_remote_copy(
            src_ref=ref,
            dst_ref=ref,
            send_sem=self.send_d2d,
            recv_sem=self.recv_d2d,
            device_id=self.sib,
            device_id_type=MESH,
        ).start()

    def on_b(self, da, stage):
        for k in range(2):
            db = (1, 3)[k]
            self.copy(self.item(da, db, k), stage, self.b[k]).start()
            self.across(da, db)

    def wave0(self):
        for k in range(2):
            self.copy(self.item(0, 0), 0, self.a[k]).start()
        self.along_b(0, 1)
        self.across(0, 0)

    def wave1(self):
        self.landed(0, 2)
        for k in range(2):
            da = (1, 3)[k]
            self.copy(self.item(da, 0, k), 2, self.a[k]).start()
            self.along_b(da, 3)
            self.across(da, 0)
        self.landed(1, 2)
        self.on_b(0, 4)

    def wave2(self):
        self.landed(2, 1)
        self.along_b(2, 5)
        self.across(2, 0)
        self.landed(3, 4)
        self.on_b(1, 6)
        self.on_b(3, 6)
        self.landed(4, 1)
        self.across(0, 2)

    def wave3(self):
        self.landed(5, 2)
        self.on_b(2, 7)
        self.landed(6, 2)
        self.across(1, 2)
        self.across(3, 2)

    def wave4(self):
        self.landed(7, 1)
        self.across(2, 2)


def kernel(
    tokens,
    mixer_gain_hbm,
    direct_weight_hbm,
    direct_scale_hbm,
    value_weight_hbm,
    value_scale_hbm,
    value_gain_hbm,
    value_shift_hbm,
    spatial_weight_hbm,
    spatial_bias_hbm,
    merge_weight_hbm,
    merge_scale_hbm,
    channel_gain_hbm,
    expand_weight_hbm,
    expand_scale_hbm,
    reduce_weight_hbm,
    reduce_scale_hbm,
    out,
    mixer_gain,
    direct_weight,
    direct_scale,
    value_weight,
    value_scale,
    value_gain,
    value_shift,
    spatial_weight,
    spatial_bias,
    merge_weight,
    merge_scale,
    channel_gain,
    expand_weight,
    expand_scale,
    reduce_weight,
    reduce_scale,
    valw,
    dmw,
    we,
    wr,
    xbuf,
    x2buf,
    part1,
    part2,
    rel,
    near,
    mrg,
    hbuf,
    dbuf,
    vbuf,
    gbuf,
    rbuf,
    stat,
    small,
    swb,
    bias,
    result,
    in_sem,
    out_sem,
    ag_send,
    ag_recv,
    rs_send,
    rs_recv,
    st_send,
    st_recv,
    sm_send,
    sm_recv,
    w_send,
    w_send_d2d,
    w_recv,
    w_recv_d2d,
):
    zh, zl, x, y, c = (lax.axis_index(name) for name in AXES)
    z = zh * 4 + zl
    fs = zl * 4 + x
    other = 1 - c
    scope = jax.named_scope

    def at_z(w):
        w = lax.rem(w, 8)
        return {"zh": lax.div(w, 4), "zl": lax.rem(w, 4)}

    xs = ({"x": lax.rem(x + 1, 4)}, {"x": lax.rem(x + 3, 4)})
    zs = (at_z(z + 1), at_z(z + 7))
    ynext, yprev, yfar = ({"y": lax.rem(y + k, 4)} for k in (1, 3, 2))
    sib = {"c": other}

    barrier = pltpu.get_barrier_semaphore()
    for to in (*xs, *zs, ynext, yprev, yfar, sib):
        pl.semaphore_signal(barrier, inc=1, device_id=to, device_id_type=MESH)

    inputs = [
        pltpu.make_async_copy(src, dst, in_sem.at[k])
        for k, (src, dst) in enumerate(
            (
                (tokens, xbuf.at[pl.ds(SO * R, R)]),
                (mixer_gain_hbm, mixer_gain),
                (direct_weight_hbm, direct_weight),
                (direct_scale_hbm, direct_scale),
                (value_weight_hbm, value_weight),
                (value_scale_hbm, value_scale),
                (merge_weight_hbm, merge_weight),
                (merge_scale_hbm, merge_scale),
                (channel_gain_hbm, channel_gain),
                (expand_weight_hbm, expand_weight),
                (expand_scale_hbm, expand_scale),
                (reduce_weight_hbm, reduce_weight),
                (reduce_scale_hbm, reduce_scale),
                (value_gain_hbm, value_gain),
                (value_shift_hbm, value_shift),
                (spatial_bias_hbm, spatial_bias),
                (spatial_weight_hbm, spatial_weight),
            )
        )
    ]
    for copy in inputs:
        copy.start()

    def rcopy(src, dst, ssem, rsem, to):
        return pltpu.make_async_remote_copy(
            src_ref=src, dst_ref=dst, send_sem=ssem, recv_sem=rsem, device_id=to, device_id_type=MESH
        )

    def gather_copy(buf, phase, way, k):
        if k < 4:
            src = buf.at[pl.ds(SO * R + CHUNK * k, CHUNK)]
            dst = buf.at[pl.ds((SP, SN)[way] * R + CHUNK * k, CHUNK)]
            stage = k - 2 * way if k // 2 == way else 2
        else:
            row = 64 * way + CHUNK * (k - 4)
            src = buf.at[pl.ds((SP, SN)[way] * R + row, CHUNK)]
            dst = buf.at[pl.ds(SF * R + row, CHUNK)]
            stage = 3
        return rcopy(src, dst, ag_send.at[phase], ag_recv.at[phase, stage], (ynext, yprev)[way])

    def gather_landed(buf, phase, stage, chunks):
        ref = buf.at[pl.ds(0, chunks * CHUNK)]
        rcopy(ref, ref, ag_send.at[phase], ag_recv.at[phase, stage], sib).wait_recv()

    def gather_pass_on(buf, phase, k):
        gather_landed(buf, phase, k, 2)
        for way in range(2):
            gather_copy(buf, phase, way, 4 + k).start()

    def gather_near(buf, phase):
        gather_landed(buf, phase, 2, 4)

    def gather_far(buf, phase):
        gather_landed(buf, phase, 3, 4)

    def scatter_copy(src, dst, phase, way, stage):
        return rcopy(src, dst, rs_send.at[phase], rs_recv.at[phase, stage], (ynext, yprev)[way])

    def scatter_landed(part, phase, stage, rows):
        ref = part.at[pl.ds(0, rows)]
        rcopy(ref, ref, rs_send.at[phase], rs_recv.at[phase, stage], sib).wait_recv()

    def scatter_own(part, phase):
        for way in range(2):
            src = part.at[pl.ds((SN, SP)[way] * R + 64 * (1 - way), 64)]
            scatter_copy(src, near.at[phase, way, pl.ds(64 * (1 - way), 64)], phase, way, 0).start()

    def scatter_far(part, phase):
        for k in range(2):
            for way in range(2):
                row = CHUNK * k
                src = part.at[pl.ds(SF * R + 64 * way + row, CHUNK)]
                scatter_copy(src, rel.at[phase, way, pl.ds(row, CHUNK)], phase, way, 1 + k).start()

    def scatter_join(part, phase, k):
        scatter_landed(part, phase, 1 + k, 2 * CHUNK)
        for way in range(2):
            row = CHUNK * k
            mine = part[pl.ds((SN, SP)[way] * R + 64 * way + row, CHUNK), :].astype(F32)
            came = rel[phase, way, pl.ds(row, CHUNK), :].astype(F32)
            joined = mrg.at[phase, way, pl.ds(row, CHUNK)]
            joined[...] = (mine + came).astype(BF16)
            scatter_copy(
                joined, near.at[phase, way, pl.ds(64 * way + row, CHUNK)], phase, way, 3 + k
            ).start()

    def scatter_finish(part, phase, base, done, k):
        if k == 0:
            scatter_landed(part, phase, 0, 128)
        scatter_landed(part, phase, 3 + k, 2 * CHUNK)
        for way in range(2):
            row = 64 * way + CHUNK * k
            total = part[pl.ds(SO * R + row, CHUNK), :].astype(F32)
            total = total + near[phase, 0, pl.ds(row, CHUNK), :].astype(F32)
            total = total + near[phase, 1, pl.ds(row, CHUNK), :].astype(F32)
            mine = base[pl.ds(SO * R + row, CHUNK), :].astype(F32)
            done(row, (mine + total).astype(BF16))

    def view_rows(ref, low):
        def view(pz, px, half):
            row = (pz * 4 + px) * 128 + low
            if half is None:
                return ref.at[c, pl.ds(pl.multiple_of(row, 64), 64)]
            return ref.at[c, pl.ds(pl.multiple_of(row + 32 * half, 32), 32)]

        return view

    def span_rows(ref):
        return lambda count: ref.at[c, pl.ds(0, 64 * count)]

    def view_reduce(low):
        def view(pz, px, half):
            row = c * HW + low
            if half is None:
                return wr.at[pz * 4 + px, pl.ds(pl.multiple_of(row, 256), 256)]
            return wr.at[pz * 4 + px, pl.ds(pl.multiple_of(row + 128 * half, 128), 128)]

        return view

    def span_reduce(count):
        return wr.at[pl.ds(0, count), pl.ds(0, 256)]

    def weight(index, view, span, x_first):
        if x_first:
            a, b, pa, pb, turned = xs, zs, x, zl, lambda p, q, h: view(q, p, h)
        else:
            a, b, pa, pb, turned = zs, xs, zl, x, view
        return Gather(
            turned,
            span,
            a,
            b,
            pa,
            pb,
            sib,
            w_send.at[index],
            w_send_d2d.at[index],
            w_recv.at[index],
            w_recv_d2d.at[index],
        )

    class Pair:
        def __init__(self, index, low, high, span):
            self.index, self.span = index, span
            self.halves = (weight(index, low, span, True), weight(index + 1, high, span, False))

        def wave(self, k):
            for half in self.halves:
                getattr(half, f"wave{k}")()

        def shared(self):
            for half in self.halves:
                ref = self.span(16)
                rcopy(ref, ref, half.send_d2d, half.recv_d2d, sib).wait_recv()

        def sent(self):
            for half in self.halves:
                ref = self.span(15)
                rcopy(ref, ref, half.send, half.recv_d2d, sib).wait_send()
                ref = self.span(16)
                rcopy(ref, ref, half.send_d2d, half.recv_d2d, sib).wait_send()

    value_blocks = Pair(0, view_rows(valw, 0), view_rows(valw, 64), span_rows(valw))
    dm_blocks = Pair(2, view_rows(dmw, 0), view_rows(dmw, 64), span_rows(dmw))
    expand_blocks = Pair(4, view_rows(we, 0), view_rows(we, 64), span_rows(we))
    reduce_low = Pair(6, view_reduce(0), view_reduce(256), span_reduce)
    reduce_high = Pair(8, view_reduce(512), view_reduce(768), span_reduce)

    def column(row):
        return jnp.transpose(jnp.broadcast_to(row, (128, 128)))

    with scope("wait_tokens"):
        inputs[0].wait()
    with scope("wait_barrier"):
        pl.semaphore_wait(barrier, 8)
    for k in range(4):
        for way in range(2):
            gather_copy(xbuf, 0, way, (k + 2 * way) % 4).start()
    with scope("wait_mix"):
        for copy in inputs[1:8]:
            copy.wait()

    fs_row = pl.ds(pl.multiple_of(fs * 128, 128), 128)
    gain = column(mixer_gain[pl.ds(fs, 1), :])
    valw[c, fs_row, :] = (value_weight[...] * gain * value_scale[...]).astype(BF16)
    dmw[c, fs_row, 0:128] = (direct_weight[...] * gain * direct_scale[...]).astype(BF16)
    dmw[c, fs_row, 128:256] = (merge_weight[...] * merge_scale[...]).astype(BF16)
    value_blocks.wave(0)
    dm_blocks.wave(0)
    for copy in inputs[8:]:
        copy.wait()
    gain = column(channel_gain[pl.ds(fs, 1), :])
    for k in range(8):
        lanes = slice(k * 128, (k + 1) * 128)
        we[c, fs_row, lanes] = (expand_weight[:, lanes] * gain * expand_scale[:, lanes]).astype(BF16)
    for k in range(8):
        rows = pl.ds(pl.multiple_of(c * HW + k * 128, 128), 128)
        wr[fs, rows, :] = (reduce_weight[k * 128 : (k + 1) * 128, :] * reduce_scale[...]).astype(BF16)
    small[c, 0:1, :] = value_gain[...]
    small[c, 1:2, :] = value_shift[...]
    small[c, 2:4, :] = spatial_bias[...]
    small[c, 4:8, :] = jnp.zeros((4, 128), F32)
    swb[c] = spatial_weight[...]
    small_copy = rcopy(small.at[c], small.at[c], sm_send.at[0], sm_recv.at[0], sib)
    spatial_copy = rcopy(spatial_weight, swb.at[c], sm_send.at[1], sm_recv.at[1], sib)
    small_copy.start()
    spatial_copy.start()

    def row_scales(buf, start, count):
        @pl.loop(0, count // 32)
        def _(i):
            rows = pl.ds(pl.multiple_of(start + i * 32, 32), 32)
            floats = buf[rows, :].astype(F32)
            power = jnp.mean(floats * floats, axis=-1, keepdims=True)
            rbuf[rows, :] = jnp.broadcast_to(lax.rsqrt(power + EPS), (32, 128))

    lane = lax.broadcasted_iota(jnp.int32, (128, 128), 1)
    block_of = {SP: lax.rem(y + 3, 4), SN: lax.rem(y + 1, 4), SF: lax.rem(y + 2, 4), SO: y}

    def project(slots):
        start, count = slots[0] * R, len(slots) * R
        rows = pl.ds(start, count)
        weights = jnp.concatenate([valw[0], valw[1]], axis=1)
        value = jnp.dot(xbuf[rows, :], weights, preferred_element_type=F32)
        scale = rbuf[rows, :]
        vbuf[rows, :] = gelu(value * jnp.concatenate([scale, scale], axis=1))
        for slot in slots:
            v = vbuf[pl.ds(slot * R, R), :]
            total = jnp.sum(v, axis=1, keepdims=True)
            squares = jnp.sum(v * v, axis=1, keepdims=True)
            tile = jnp.where(lane == 0, total, jnp.where(lane == 1, squares, 0.0))
            stat[0, block_of[slot]] = jnp.transpose(tile)[0:8, :]

    def project_direct():
        weights = jnp.concatenate([dmw[0, :, 0:128], dmw[1, :, 0:128]], axis=1)

        @pl.loop(0, 2)
        def _(i):
            rows = pl.ds(pl.multiple_of(i * 256, 256), 256)
            direct = jnp.dot(xbuf[rows, :], weights, preferred_element_type=F32)
            scale = rbuf[rows, :]
            dbuf[rows, :] = gelu(direct * jnp.concatenate([scale, scale], axis=1))

    def mixing(slots):
        for slot in slots:
            rows = pl.ds(slot * R, R)
            block = block_of[slot]
            sums = stat[0, block] + stat[1, block] + stat[2, block] + stat[3, block]
            tile = jnp.transpose(jnp.concatenate([sums] * 16, axis=0))
            mean = tile[:, 0:1] / BRANCH
            var = tile[:, 1:2] / BRANCH - mean * mean
            inv = lax.rsqrt(var + EPS)
            for k in range(2):
                lanes = slice(k * 128, (k + 1) * 128)
                v = vbuf[rows, lanes]
                g = ((v - mean) * inv * small[k, 0:1, :] + small[k, 1:2, :]).astype(BF16)
                low = jnp.dot(swb[k, 0], g, preferred_element_type=F32)
                high = jnp.dot(swb[k, 1], g, preferred_element_type=F32)
                mixed = jnp.where(lane < 64, low, high) + bias[k]
                gbuf[rows, lanes] = (dbuf[rows, lanes] * mixed).astype(BF16)
        rows = pl.ds(slots[0] * R, len(slots) * R)

        @pl.loop(0, 2)
        def _(j):
            weights = jnp.concatenate(
                [
                    jnp.concatenate(
                        [
                            dmw[k, pl.ds(pl.multiple_of(j * 1024 + i * 128, 128), 128), 128:256]
                            for i in range(8)
                        ],
                        axis=1,
                    )
                    for k in range(2)
                ],
                axis=0,
            )
            product = jnp.dot(gbuf[rows, :], weights, preferred_element_type=F32)
            part1[rows, pl.ds(pl.multiple_of(j * 1024, 1024), 1024)] = product.astype(BF16)

    def gathered_rows(ref, pieces):
        loaded = [ref[pl.ds(start, count), :] for start, count in pieces]
        return loaded[0] if len(loaded) == 1 else jnp.concatenate(loaded, axis=0)

    def store_rows(ref, pieces, cols, values):
        at = 0
        for start, count in pieces:
            ref[pl.ds(start, count), cols] = values[at : at + count, :]
            at += count

    def feed_up(pieces):
        for start, count in pieces:
            row_scales(x2buf, start, count)

        @pl.loop(0, 2)
        def _(j):
            upper = jnp.dot(gathered_rows(x2buf, pieces), we[j], preferred_element_type=F32)
            upper = upper * jnp.concatenate([gathered_rows(rbuf, pieces)] * 8, axis=1)
            hidden = jnp.square(jnp.maximum(upper, 0.0)).astype(BF16)
            store_rows(hbuf, pieces, pl.ds(pl.multiple_of(j * HW, HW), HW), hidden)

    def feed_down(pieces):
        @pl.loop(0, 2)
        def _(j):
            weights = jnp.concatenate([wr[8 * j + i] for i in range(8)], axis=1)
            product = jnp.dot(gathered_rows(hbuf, pieces), weights, preferred_element_type=F32)
            store_rows(part2, pieces, pl.ds(pl.multiple_of(j * 1024, 1024), 1024), product.astype(BF16))

    row_scales(xbuf, SO * R, R)
    with scope("v_w1"):
        value_blocks.wave(1)
    with scope("dm_w1"):
        dm_blocks.wave(1)
    expand_blocks.halves[0].wave0()
    with scope("v_w2"):
        value_blocks.wave(2)
    with scope("pass1_0"):
        gather_pass_on(xbuf, 0, 0)
    with scope("dm_w2"):
        dm_blocks.wave(2)
    with scope("v_w3"):
        value_blocks.wave(3)
    expand_blocks.halves[1].wave0()
    with scope("pass1_1"):
        gather_pass_on(xbuf, 0, 1)
    with scope("dm_w3"):
        dm_blocks.wave(3)
    with scope("near1"):
        gather_near(xbuf, 0)
    with scope("scales_near"):
        row_scales(xbuf, 0, 2 * R)
    with scope("v_w4"):
        value_blocks.wave(4)
    with scope("v_d2d"):
        value_blocks.shared()
    with scope("project_own"):
        project((SO,))
    with scope("e_w1"):
        expand_blocks.wave(1)
    with scope("project_near"):
        project((SN, SP))
    with scope("dm_w4"):
        dm_blocks.wave(4)
    with scope("far1"):
        gather_far(xbuf, 0)
    with scope("project_far"):
        row_scales(xbuf, SF * R, R)
        project((SF,))
    stat_copies = [
        rcopy(stat.at[0], stat.at[k + 1], st_send.at[0], st_recv.at[0], to)
        for k, to in enumerate((ynext, yprev, yfar))
    ]
    for copy in stat_copies:
        copy.start()
    reduce_low.wave(0)
    reduce_high.wave(0)
    with scope("dm_d2d"):
        dm_blocks.shared()
    with scope("direct"):
        project_direct()
        rcopy(small.at[other], small.at[other], sm_send.at[0], sm_recv.at[0], sib).wait_recv()
        rcopy(swb.at[other], swb.at[other], sm_send.at[1], sm_recv.at[1], sib).wait_recv()
        for k in range(2):
            rows = jnp.concatenate(
                [jnp.broadcast_to(small[k, 2 + g : 3 + g, :], (64, 128)) for g in range(2)], axis=0
            )
            bias[k] = jnp.transpose(rows)
    with scope("wait_stats"):
        all_stats = stat.at[pl.ds(1, 3)]
        rcopy(all_stats, all_stats, st_send.at[0], st_recv.at[0], sib).wait_recv()
    with scope("mixing_near"):
        mixing((SN, SP))
    scatter_own(part1, 0)
    with scope("mixing_far"):
        mixing((SF,))
    scatter_far(part1, 0)
    with scope("mixing_own"):
        mixing((SO,))
    with scope("e_w2"):
        expand_blocks.wave(2)
    with scope("r0_w1"):
        reduce_low.wave(1)
    with scope("join1_0"):
        scatter_join(part1, 0, 0)
    with scope("join1_1"):
        scatter_join(part1, 0, 1)
    with scope("e_w3"):
        expand_blocks.wave(3)
    with scope("r1_w1"):
        reduce_high.wave(1)

    def middle_done(row, value):
        x2buf[pl.ds(SO * R + row, CHUNK), :] = value

    with scope("finish1_0"):
        scatter_finish(part1, 0, xbuf, middle_done, 0)
    for way in range(2):
        gather_copy(x2buf, 1, way, 2 * way).start()
    with scope("r0_w2"):
        reduce_low.wave(2)
    with scope("finish1_1"):
        scatter_finish(part1, 0, xbuf, middle_done, 1)
    for way in range(2):
        gather_copy(x2buf, 1, way, 2 * way + 1).start()
    with scope("e_w4"):
        expand_blocks.wave(4)
    with scope("pass2_0"):
        gather_pass_on(x2buf, 1, 0)
    with scope("r1_w2"):
        reduce_high.wave(2)
    with scope("pass2_1"):
        gather_pass_on(x2buf, 1, 1)
    for k in range(2):
        for way in range(2):
            gather_copy(x2buf, 1, way, 2 * (1 - way) + k).start()

    outer, inner = ((64, 128),), ((0, 64), (192, 64))
    far, own = ((SF * R, R),), ((SO * R, R),)
    with scope("e_d2d"):
        expand_blocks.shared()
    with scope("up_outer"):
        feed_up(outer)
    with scope("r0_w3"):
        reduce_low.wave(3)
    with scope("r1_w3"):
        reduce_high.wave(3)
    with scope("up_own"):
        feed_up(own)
    with scope("r0_w4"):
        reduce_low.wave(4)
    with scope("r1_w4"):
        reduce_high.wave(4)
    with scope("r_d2d"):
        reduce_low.shared()
        reduce_high.shared()
    with scope("down_outer"):
        feed_down(outer)
    scatter_own(part2, 1)
    with scope("far2"):
        gather_far(x2buf, 1)
    with scope("feed_far"):
        feed_up(far)
        feed_down(far)
    scatter_far(part2, 1)
    with scope("near2"):
        gather_near(x2buf, 1)
    with scope("feed_inner"):
        feed_up(inner)
        feed_down(inner)
    with scope("down_own"):
        feed_down(own)
    with scope("join2_0"):
        scatter_join(part2, 1, 0)
    with scope("join2_1"):
        scatter_join(part2, 1, 1)

    def result_done(row, value):
        result[pl.ds(row, CHUNK), :] = value

    def result_copy(row):
        rows = pl.ds(row, CHUNK)
        return pltpu.make_async_copy(result.at[rows], out.at[rows], out_sem.at[row // CHUNK])

    for k in range(2):
        with scope(f"finish2_{k}"):
            scatter_finish(part2, 1, x2buf, result_done, k)
        for way in range(2):
            result_copy(64 * way + CHUNK * k).start()

    with scope("drain"):
        for phase, buf, part in ((0, xbuf, part1), (1, x2buf, part2)):
            ref = buf.at[pl.ds(0, 12 * CHUNK)]
            rcopy(ref, ref, ag_send.at[phase], ag_recv.at[phase, 0], sib).wait_send()
            ref = part.at[pl.ds(0, 12 * CHUNK)]
            rcopy(ref, ref, rs_send.at[phase], rs_recv.at[phase, 0], sib).wait_send()
        rcopy(all_stats, all_stats, st_send.at[0], st_recv.at[0], sib).wait_send()
        for copy in (small_copy, spatial_copy):
            copy.wait_send()
        for blocks in (value_blocks, dm_blocks, expand_blocks, reduce_low, reduce_high):
            blocks.sent()
        for k in range(4):
            result_copy(CHUNK * k).wait()


def layer(*args):
    (
        tokens,
        mixer_gain,
        direct_weight,
        direct_scale,
        value_weight,
        value_scale,
        value_gain,
        value_shift,
        spatial_weight,
        spatial_bias,
        merge_weight,
        merge_scale,
        channel_gain,
        expand_weight,
        expand_scale,
        reduce_weight,
        reduce_scale,
    ) = args
    operands = (
        tokens,
        mixer_gain.reshape(16, 128),
        direct_weight,
        direct_scale.reshape(1, CW),
        value_weight,
        value_scale.reshape(1, CW),
        value_gain.reshape(1, CW),
        value_shift.reshape(1, CW),
        spatial_weight,
        spatial_bias,
        merge_weight,
        merge_scale.reshape(1, 128),
        channel_gain.reshape(16, 128),
        expand_weight,
        expand_scale.reshape(1, HW),
        reduce_weight,
        reduce_scale.reshape(1, 128),
    )
    dma = pltpu.SemaphoreType.DMA
    return pl.pallas_call(
        kernel,
        out_shape=jax.ShapeDtypeStruct((R, D), BF16),
        in_specs=[pl.BlockSpec(memory_space=pl.ANY)] * 17,
        out_specs=pl.BlockSpec(memory_space=pl.ANY),
        scratch_shapes=[
            *(pltpu.VMEM(operand.shape, operand.dtype) for operand in operands[1:]),
            pltpu.VMEM((2, D, 128), BF16),
            pltpu.VMEM((2, D, 256), BF16),
            pltpu.VMEM((2, D, HW), BF16),
            pltpu.VMEM((16, 2 * HW, 128), BF16),
            pltpu.VMEM((4 * R, D), BF16),
            pltpu.VMEM((4 * R, D), BF16),
            pltpu.VMEM((4 * R, D), BF16),
            pltpu.VMEM((4 * R, D), BF16),
            pltpu.VMEM((2, 2, 64, D), BF16),
            pltpu.VMEM((2, 2, R, D), BF16),
            pltpu.VMEM((2, 2, 64, D), BF16),
            pltpu.VMEM((4 * R, D), BF16),
            pltpu.VMEM((4 * R, 256), F32),
            pltpu.VMEM((4 * R, 256), F32),
            pltpu.VMEM((4 * R, 256), BF16),
            pltpu.VMEM((4 * R, 128), F32),
            pltpu.VMEM((4, 4, 8, 128), F32),
            pltpu.VMEM((2, 8, 128), F32),
            pltpu.VMEM((2, 2, 128, 128), BF16),
            pltpu.VMEM((2, 128, 128), F32),
            pltpu.VMEM((R, D), BF16),
            dma((17,)),
            dma((4,)),
            dma((2,)),
            dma((2, 4)),
            dma((2,)),
            dma((2, 5)),
            dma((1,)),
            dma((1,)),
            dma((2,)),
            dma((2,)),
            dma((10,)),
            dma((10,)),
            dma((10, 8)),
            dma((10,)),
        ],
        compiler_params=pltpu.CompilerParams(
            collective_id=0, has_side_effects=True, vmem_limit_bytes=60 * 1024 * 1024
        ),
        name="layer",
    )(*operands)


def solution(mesh):
    finer = Mesh(mesh.devices.reshape(2, 4, 4, 4, 2), AXES)
    in_specs = (
        P(AXES, None),
        P(),
        P(FS, TP),
        P(TP),
        P(FS, TP),
        P(TP),
        P(TP),
        P(TP),
        P(TP, None, None),
        P(TP, None),
        P(TP, FS),
        P(FS),
        P(),
        P(FS, TP),
        P(TP),
        P(TP, FS),
        P(FS),
    )
    return jax.shard_map(layer, mesh=finer, in_specs=in_specs, out_specs=P(AXES, None), check_vma=False)
```

```python
import functools

import jax
import jax.numpy as jnp
from jax import lax
from jax.experimental import pallas as pl
from jax.experimental.pallas import tpu as pltpu
from jax.sharding import Mesh
from jax.sharding import PartitionSpec as P

AXES = ("zh", "zl", "x", "y", "c")
FS = ("zl", "x")
TP = ("y", "c")
EPS = 1e-6
MESH = pl.DeviceIdType.MESH
F32 = jnp.float32
BF16 = jnp.bfloat16

D = 2048
R = 128
CW = 128
HW = 1024
BRANCH = 1024
SN, SP, SF, SO = 0, 1, 2, 3
CHUNK = 32


def gelu(u):
    return jax.nn.gelu(u, approximate=True)


FIRST = ((0, 0), (1, 0), (3, 0), (0, 1), (0, 3), (1, 1), (1, 3), (3, 1))
LAST = ((3, 3), (2, 0), (0, 2), (2, 1), (2, 3), (1, 2), (3, 2), (2, 2))


class Gather:
    def __init__(self, view, span, a, b, pa, pb, sib, send, send_d2d, recv, recv_d2d):
        self.view, self.span = view, span
        self.a, self.b, self.pa, self.pb, self.sib = a, b, pa, pb, sib
        self.send, self.send_d2d, self.recv, self.recv_d2d = send, send_d2d, recv, recv_d2d

    def item(self, da, db, half=None):
        return self.view(lax.rem(self.pa + 4 - da, 4), lax.rem(self.pb + 4 - db, 4), half)

    def copy(self, ref, stage, to):
        return pltpu.make_async_remote_copy(
            src_ref=ref,
            dst_ref=ref,
            send_sem=self.send,
            recv_sem=self.recv.at[stage],
            device_id=to,
            device_id_type=MESH,
        )

    def landed(self, stage, count):
        self.copy(self.span(count), stage, self.sib).wait_recv()

    def along_b(self, da, stage):
        for k in range(2):
            self.copy(self.item(da, 0), stage, self.b[k]).start()

    def across(self, da, db):
        ref = self.item(da, db)
        pltpu.make_async_remote_copy(
            src_ref=ref,
            dst_ref=ref,
            send_sem=self.send_d2d,
            recv_sem=self.recv_d2d.at[0 if (da, db) in FIRST else 1],
            device_id=self.sib,
            device_id_type=MESH,
        ).start()

    def on_b(self, da, stage):
        for k in range(2):
            db = (1, 3)[k]
            self.copy(self.item(da, db, k), stage, self.b[k]).start()
            self.across(da, db)

    def wave0(self):
        for k in range(2):
            self.copy(self.item(0, 0), 0, self.a[k]).start()
        self.along_b(0, 1)
        self.across(0, 0)

    def wave1(self):
        self.landed(0, 2)
        for k in range(2):
            da = (1, 3)[k]
            self.copy(self.item(da, 0, k), 2, self.a[k]).start()
            self.along_b(da, 3)
            self.across(da, 0)
        self.landed(1, 2)
        self.on_b(0, 4)

    def wave2(self):
        self.landed(2, 1)
        self.along_b(2, 5)
        self.across(2, 0)
        self.landed(3, 4)
        self.on_b(1, 6)
        self.on_b(3, 6)
        self.landed(4, 1)
        self.across(0, 2)

    def wave3(self):
        self.landed(5, 2)
        self.on_b(2, 7)
        self.landed(6, 2)
        self.across(1, 2)
        self.across(3, 2)

    def wave4(self):
        self.landed(7, 1)
        self.across(2, 2)


def kernel(
    tokens,
    mixer_gain_hbm,
    direct_weight_hbm,
    direct_scale_hbm,
    value_weight_hbm,
    value_scale_hbm,
    value_gain_hbm,
    value_shift_hbm,
    spatial_weight_hbm,
    spatial_bias_hbm,
    merge_weight_hbm,
    merge_scale_hbm,
    channel_gain_hbm,
    expand_weight_hbm,
    expand_scale_hbm,
    reduce_weight_hbm,
    reduce_scale_hbm,
    out,
    mixer_gain,
    direct_weight,
    direct_scale,
    value_weight,
    value_scale,
    value_gain,
    value_shift,
    spatial_weight,
    spatial_bias,
    merge_weight,
    merge_scale,
    channel_gain,
    expand_weight,
    expand_scale,
    reduce_weight,
    reduce_scale,
    valw,
    dmw,
    we,
    wr,
    xbuf,
    x2buf,
    part1,
    part2,
    rel1,
    near1,
    mrg1,
    rel2,
    near2,
    mrg2,
    hbuf,
    dbuf,
    vbuf,
    gbuf,
    rbuf,
    stat,
    totals,
    small,
    swb,
    bias,
    result,
    in_sem,
    out_sem,
    ag_send,
    ag_recv,
    rs_send,
    rs_recv,
    st_send,
    st_recv,
    sm_send,
    sm_recv,
    w_send,
    w_send_d2d,
    w_recv,
    w_recv_d2d,
):
    zh, zl, x, y, c = (lax.axis_index(name) for name in AXES)
    z = zh * 4 + zl
    fs = zl * 4 + x
    other = 1 - c
    scope = jax.named_scope

    def at_z(w):
        w = lax.rem(w, 8)
        return {"zh": lax.div(w, 4), "zl": lax.rem(w, 4)}

    xs = ({"x": lax.rem(x + 1, 4)}, {"x": lax.rem(x + 3, 4)})
    zs = (at_z(z + 1), at_z(z + 7))
    ynext, yprev, yfar = ({"y": lax.rem(y + k, 4)} for k in (1, 3, 2))
    sib = {"c": other}

    barrier = pltpu.get_barrier_semaphore()
    for to in (*xs, *zs, ynext, yprev, yfar, sib):
        pl.semaphore_signal(barrier, inc=1, device_id=to, device_id_type=MESH)

    inputs = [
        pltpu.make_async_copy(src, dst, in_sem.at[k])
        for k, (src, dst) in enumerate(
            (
                (tokens, xbuf.at[pl.ds(SO * R, R)]),
                (mixer_gain_hbm, mixer_gain),
                (direct_weight_hbm, direct_weight),
                (direct_scale_hbm, direct_scale),
                (value_weight_hbm, value_weight),
                (value_scale_hbm, value_scale),
                (merge_weight_hbm, merge_weight),
                (merge_scale_hbm, merge_scale),
                (channel_gain_hbm, channel_gain),
                (expand_weight_hbm, expand_weight),
                (expand_scale_hbm, expand_scale),
                (reduce_weight_hbm, reduce_weight),
                (reduce_scale_hbm, reduce_scale),
                (value_gain_hbm, value_gain),
                (value_shift_hbm, value_shift),
                (spatial_bias_hbm, spatial_bias),
                (spatial_weight_hbm, spatial_weight),
            )
        )
    ]
    for copy in inputs:
        copy.start()

    def rcopy(src, dst, ssem, rsem, to):
        return pltpu.make_async_remote_copy(
            src_ref=src, dst_ref=dst, send_sem=ssem, recv_sem=rsem, device_id=to, device_id_type=MESH
        )

    def gather_copy(buf, phase, way, k):
        if k < 4:
            src = buf.at[pl.ds(SO * R + CHUNK * k, CHUNK)]
            dst = buf.at[pl.ds((SP, SN)[way] * R + CHUNK * k, CHUNK)]
            stage = k - 2 * way if k // 2 == way else 2
        else:
            row = 64 * way + CHUNK * (k - 4)
            src = buf.at[pl.ds((SP, SN)[way] * R + row, CHUNK)]
            dst = buf.at[pl.ds(SF * R + row, CHUNK)]
            stage = 3
        return rcopy(src, dst, ag_send.at[phase], ag_recv.at[phase, stage], (ynext, yprev)[way])

    def gather_landed(buf, phase, stage, chunks):
        ref = buf.at[pl.ds(0, chunks * CHUNK)]
        rcopy(ref, ref, ag_send.at[phase], ag_recv.at[phase, stage], sib).wait_recv()

    def gather_pass_on(buf, phase, k):
        gather_landed(buf, phase, k, 2)
        for way in range(2):
            gather_copy(buf, phase, way, 4 + k).start()

    def gather_near(buf, phase):
        gather_landed(buf, phase, 2, 4)

    def gather_far(buf, phase):
        gather_landed(buf, phase, 3, 4)

    class Scatter:
        def __init__(self, stage, part, near, rel, mrg):
            self.stage, self.part, self.near, self.rel, self.mrg = stage, part, near, rel, mrg

        def copy(self, src, dst, way, k):
            return rcopy(
                src, dst, rs_send.at[self.stage], rs_recv.at[self.stage, k], (ynext, yprev)[way]
            )

        def landed(self, k, rows):
            ref = self.part.at[pl.ds(0, rows)]
            rcopy(ref, ref, rs_send.at[self.stage], rs_recv.at[self.stage, k], sib).wait_recv()

        def own(self):
            for way in range(2):
                row = 64 * (1 - way)
                src = self.part.at[pl.ds((SN, SP)[way] * R + row, 64)]
                self.copy(src, self.near.at[way, pl.ds(row, 64)], way, 0).start()

        def far(self):
            for k in range(2):
                for way in range(2):
                    row = CHUNK * k
                    src = self.part.at[pl.ds(SF * R + 64 * way + row, CHUNK)]
                    self.copy(src, self.rel.at[way, pl.ds(row, CHUNK)], way, 1 + k).start()

        def join(self, k):
            self.landed(1 + k, 2 * CHUNK)
            for way in range(2):
                row = CHUNK * k
                mine = self.part[pl.ds((SN, SP)[way] * R + 64 * way + row, CHUNK), :].astype(F32)
                came = self.rel[way, pl.ds(row, CHUNK), :].astype(F32)
                joined = self.mrg.at[way, pl.ds(row, CHUNK)]
                joined[...] = (mine + came).astype(BF16)
                self.copy(joined, self.near.at[way, pl.ds(64 * way + row, CHUNK)], way, 3 + k).start()

        def finish(self, k, done):
            if k == 0:
                self.landed(0, 128)
            self.landed(3 + k, 2 * CHUNK)
            for way in range(2):
                row = 64 * way + CHUNK * k
                total = self.part[pl.ds(SO * R + row, CHUNK), :].astype(F32)
                total = total + self.near[0, pl.ds(row, CHUNK), :].astype(F32)
                done(row, total + self.near[1, pl.ds(row, CHUNK), :].astype(F32))

    mixer_sums = Scatter(0, part1, near1, rel1, mrg1)
    ff_sums = [Scatter(1 + g, part2.at[g], near2.at[g], rel2.at[g], mrg2.at[g]) for g in range(2)]

    def view_rows(ref, low):
        def view(pz, px, half):
            row = (pz * 4 + px) * 128 + low
            if half is None:
                return ref.at[c, pl.ds(pl.multiple_of(row, 64), 64)]
            return ref.at[c, pl.ds(pl.multiple_of(row + 32 * half, 32), 32)]

        return view

    def span_rows(ref):
        return lambda count: ref.at[c, pl.ds(0, 64 * count)]

    def view_reduce(low):
        def view(pz, px, half):
            row = c * HW + low
            if half is None:
                return wr.at[pz * 4 + px, pl.ds(pl.multiple_of(row, 256), 256)]
            return wr.at[pz * 4 + px, pl.ds(pl.multiple_of(row + 128 * half, 128), 128)]

        return view

    def span_reduce(count):
        return wr.at[pl.ds(0, count), pl.ds(0, 256)]

    def weight(index, view, span, x_first):
        if x_first:
            a, b, pa, pb, turned = xs, zs, x, zl, lambda p, q, h: view(q, p, h)
        else:
            a, b, pa, pb, turned = zs, xs, zl, x, view
        return Gather(
            turned,
            span,
            a,
            b,
            pa,
            pb,
            sib,
            w_send.at[index],
            w_send_d2d.at[index],
            w_recv.at[index],
            w_recv_d2d.at[index],
        )

    class Pair:
        def __init__(self, index, low, high, span):
            self.index, self.span = index, span
            self.halves = (weight(index, low, span, True), weight(index + 1, high, span, False))

        def wave(self, k):
            for half in self.halves:
                getattr(half, f"wave{k}")()

        def shared(self, group):
            for half in self.halves:
                ref = self.span(8)
                rcopy(ref, ref, half.send_d2d, half.recv_d2d.at[group], sib).wait_recv()

        def sent(self):
            for half in self.halves:
                ref = self.span(15)
                rcopy(ref, ref, half.send, half.recv_d2d.at[0], sib).wait_send()
                ref = self.span(16)
                rcopy(ref, ref, half.send_d2d, half.recv_d2d.at[0], sib).wait_send()

    value_blocks = Pair(0, view_rows(valw, 0), view_rows(valw, 64), span_rows(valw))
    dm_blocks = Pair(2, view_rows(dmw, 0), view_rows(dmw, 64), span_rows(dmw))
    expand_blocks = Pair(4, view_rows(we, 0), view_rows(we, 64), span_rows(we))
    reduce_low = Pair(6, view_reduce(0), view_reduce(256), span_reduce)
    reduce_high = Pair(8, view_reduce(512), view_reduce(768), span_reduce)

    def column(row):
        return jnp.transpose(jnp.broadcast_to(row, (128, 128)))

    with scope("wait_tokens"):
        inputs[0].wait()
    with scope("wait_barrier"):
        pl.semaphore_wait(barrier, 8)

    def send_tokens():
        for k in range(4):
            for way in range(2):
                gather_copy(xbuf, 0, way, (k + 2 * way) % 4).start()

    pl.when(c == 1)(send_tokens)
    with scope("wait_mix"):
        for copy in inputs[1:8]:
            copy.wait()

    fs_row = pl.ds(pl.multiple_of(fs * 128, 128), 128)
    gain = column(mixer_gain[pl.ds(fs, 1), :])
    valw[c, fs_row, :] = (value_weight[...] * gain * value_scale[...]).astype(BF16)
    dmw[c, fs_row, 0:128] = (direct_weight[...] * gain * direct_scale[...]).astype(BF16)
    dmw[c, fs_row, 128:256] = (merge_weight[...] * merge_scale[...]).astype(BF16)
    value_blocks.wave(0)
    dm_blocks.wave(0)
    for copy in inputs[8:]:
        copy.wait()
    gain = column(channel_gain[pl.ds(fs, 1), :])
    for k in range(8):
        lanes = slice(k * 128, (k + 1) * 128)
        we[c, fs_row, lanes] = (expand_weight[:, lanes] * gain * expand_scale[:, lanes]).astype(BF16)
    for k in range(8):
        rows = pl.ds(pl.multiple_of(c * HW + k * 128, 128), 128)
        wr[fs, rows, :] = (reduce_weight[k * 128 : (k + 1) * 128, :] * reduce_scale[...]).astype(BF16)
    small[c, 0:1, :] = value_gain[...]
    small[c, 1:2, :] = value_shift[...]
    small[c, 2:4, :] = spatial_bias[...]
    small[c, 4:8, :] = jnp.zeros((4, 128), F32)
    swb[c] = spatial_weight[...]
    small_copy = rcopy(small.at[c], small.at[c], sm_send.at[0], sm_recv.at[0], sib)
    spatial_copy = rcopy(spatial_weight, swb.at[c], sm_send.at[1], sm_recv.at[1], sib)
    small_copy.start()
    spatial_copy.start()

    def row_scales(buf, start, count):
        @pl.loop(0, count // 32)
        def _(i):
            rows = pl.ds(pl.multiple_of(start + i * 32, 32), 32)
            floats = buf[rows, :].astype(F32)
            power = jnp.mean(floats * floats, axis=-1, keepdims=True)
            rbuf[rows, :] = jnp.broadcast_to(lax.rsqrt(power + EPS), (32, 128))

    lane = lax.broadcasted_iota(jnp.int32, (128, 128), 1)
    block_of = {SP: lax.rem(y + 3, 4), SN: lax.rem(y + 1, 4), SF: lax.rem(y + 2, 4), SO: y}

    def project(slots):
        start, count = slots[0] * R, len(slots) * R
        rows = pl.ds(start, count)
        weights = jnp.concatenate([valw[0], valw[1]], axis=1)
        value = jnp.dot(xbuf[rows, :], weights, preferred_element_type=F32)
        scale = rbuf[rows, :]
        vbuf[rows, :] = gelu(value * jnp.concatenate([scale, scale], axis=1))
        for slot in slots:
            v = vbuf[pl.ds(slot * R, R), :]
            total = jnp.sum(v, axis=1, keepdims=True)
            squares = jnp.sum(v * v, axis=1, keepdims=True)
            tile = jnp.where(lane == 0, total, jnp.where(lane == 1, squares, 0.0))
            sums = jnp.transpose(tile)
            stat[0, pl.ds(block_of[slot], 1), :] = sums[0:1, :]
            stat[0, pl.ds(4 + block_of[slot], 1), :] = sums[1:2, :]

    def project_direct():
        weights = jnp.concatenate([dmw[0, :, 0:128], dmw[1, :, 0:128]], axis=1)

        @pl.loop(0, 2)
        def _(i):
            rows = pl.ds(pl.multiple_of(i * 256, 256), 256)
            direct = jnp.dot(xbuf[rows, :], weights, preferred_element_type=F32)
            scale = rbuf[rows, :]
            dbuf[rows, :] = gelu(direct * jnp.concatenate([scale, scale], axis=1))

    def mixing(slots):
        for slot in slots:
            rows = pl.ds(slot * R, R)
            block = block_of[slot]
            mean = column(totals[pl.ds(block, 1), :]) / BRANCH
            var = column(totals[pl.ds(4 + block, 1), :]) / BRANCH - mean * mean
            inv = lax.rsqrt(var + EPS)
            for k in range(2):
                lanes = slice(k * 128, (k + 1) * 128)
                v = vbuf[rows, lanes]
                g = ((v - mean) * inv * small[k, 0:1, :] + small[k, 1:2, :]).astype(BF16)
                low = jnp.dot(swb[k, 0], g, preferred_element_type=F32)
                high = jnp.dot(swb[k, 1], g, preferred_element_type=F32)
                mixed = jnp.where(lane < 64, low, high) + bias[k]
                gbuf[rows, lanes] = (dbuf[rows, lanes] * mixed).astype(BF16)
        rows = pl.ds(slots[0] * R, len(slots) * R)

        @pl.loop(0, 2)
        def _(j):
            weights = jnp.concatenate(
                [
                    jnp.concatenate(
                        [
                            dmw[k, pl.ds(pl.multiple_of(j * 1024 + i * 128, 128), 128), 128:256]
                            for i in range(8)
                        ],
                        axis=1,
                    )
                    for k in range(2)
                ],
                axis=0,
            )
            product = jnp.dot(gbuf[rows, :], weights, preferred_element_type=F32)
            part1[rows, pl.ds(pl.multiple_of(j * 1024, 1024), 1024)] = product.astype(BF16)

    def gathered_rows(ref, pieces):
        loaded = [ref[pl.ds(start, count), :] for start, count in pieces]
        return loaded[0] if len(loaded) == 1 else jnp.concatenate(loaded, axis=0)

    def store_rows(ref, pieces, cols, values):
        at = 0
        for start, count in pieces:
            ref[pl.ds(start, count), cols] = values[at : at + count, :]
            at += count

    def feed_up(pieces):
        for start, count in pieces:
            row_scales(x2buf, start, count)

        @pl.loop(0, 2)
        def _(j):
            upper = jnp.dot(gathered_rows(x2buf, pieces), we[j], preferred_element_type=F32)
            upper = upper * jnp.concatenate([gathered_rows(rbuf, pieces)] * 8, axis=1)
            hidden = jnp.square(jnp.maximum(upper, 0.0)).astype(BF16)
            store_rows(hbuf, pieces, pl.ds(pl.multiple_of(j * HW, HW), HW), hidden)

    def shard_of(dx, dz):
        return lax.rem(zl + 4 - dz, 4) * 4 + lax.rem(x + 4 - dx, 4)

    columns = [[shard_of(*offsets) for offsets in group] for group in (FIRST, LAST)]

    def feed_down(pieces, g):
        weights = jnp.concatenate([wr[shard] for shard in columns[g]], axis=1)
        product = jnp.dot(gathered_rows(hbuf, pieces), weights, preferred_element_type=F32)
        store_rows(part2.at[g], pieces, slice(None), product.astype(BF16))

    row_scales(xbuf, SO * R, R)
    with scope("v_w1"):
        value_blocks.wave(1)
    with scope("dm_w1"):
        dm_blocks.wave(1)

    @pl.when(c == 1)
    def _():
        gather_pass_on(xbuf, 0, 0)
        gather_pass_on(xbuf, 0, 1)

    with scope("v_w2"):
        value_blocks.wave(2)
    pl.when(c == 0)(send_tokens)
    with scope("dm_w2"):
        dm_blocks.wave(2)
    with scope("v_w3"):
        value_blocks.wave(3)
    expand_blocks.wave(0)

    @pl.when(c == 1)
    def _():
        with scope("scales_1"):
            gather_near(xbuf, 0)
            gather_far(xbuf, 0)
            row_scales(xbuf, 0, 3 * R)

    @pl.when(c == 0)
    def _():
        with scope("pass1_0"):
            gather_pass_on(xbuf, 0, 0)

    with scope("v_w4"):
        value_blocks.wave(4)
    with scope("dm_w3"):
        dm_blocks.wave(3)
    reduce_low.wave(0)

    @pl.when(c == 0)
    def _():
        with scope("pass1_1"):
            gather_pass_on(xbuf, 0, 1)

    with scope("v_d2d"):
        value_blocks.shared(0)
        value_blocks.shared(1)
    with scope("project_own"):
        project((SO,))

    @pl.when(c == 0)
    def _():
        with scope("scales_0"):
            gather_near(xbuf, 0)
            row_scales(xbuf, 0, 2 * R)

    with scope("project_near"):
        project((SN, SP))
    with scope("dm_w4"):
        dm_blocks.wave(4)

    @pl.when(c == 0)
    def _():
        with scope("e_w1_0"):
            expand_blocks.wave(1)
        with scope("far1"):
            gather_far(xbuf, 0)
            row_scales(xbuf, 2 * R, R)

    with scope("project_far"):
        project((SF,))
    stat_copies = [
        rcopy(stat.at[0], stat.at[k + 1], st_send.at[0], st_recv.at[0], to)
        for k, to in enumerate((ynext, yprev, yfar))
    ]
    for copy in stat_copies:
        copy.start()

    @pl.when(c == 1)
    def _():
        with scope("e_w1_1"):
            expand_blocks.wave(1)

    reduce_high.wave(0)
    with scope("dm_d2d"):
        dm_blocks.shared(0)
        dm_blocks.shared(1)
    with scope("direct"):
        project_direct()
        rcopy(small.at[other], small.at[other], sm_send.at[0], sm_recv.at[0], sib).wait_recv()
        rcopy(swb.at[other], swb.at[other], sm_send.at[1], sm_recv.at[1], sib).wait_recv()
        for k in range(2):
            rows = jnp.concatenate(
                [jnp.broadcast_to(small[k, 2 + g : 3 + g, :], (64, 128)) for g in range(2)], axis=0
            )
            bias[k] = jnp.transpose(rows)
    with scope("wait_stats"):
        all_stats = stat.at[pl.ds(1, 3)]
        rcopy(all_stats, all_stats, st_send.at[0], st_recv.at[0], sib).wait_recv()
        totals[...] = stat[0] + stat[1] + stat[2] + stat[3]
    with scope("mixing_near"):
        mixing((SN, SP))
    mixer_sums.own()
    with scope("mixing_far"):
        mixing((SF,))
    mixer_sums.far()
    with scope("mixing_own"):
        mixing((SO,))
    with scope("e_w2"):
        expand_blocks.wave(2)
    with scope("r0_w1"):
        reduce_low.wave(1)
    with scope("join1_0"):
        mixer_sums.join(0)
    with scope("join1_1"):
        mixer_sums.join(1)
    with scope("e_w3"):
        expand_blocks.wave(3)
    with scope("r1_w1"):
        reduce_high.wave(1)

    def middle_done(row, total):
        rows = pl.ds(SO * R + row, CHUNK)
        x2buf[rows, :] = (xbuf[rows, :].astype(F32) + total).astype(BF16)

    with scope("finish1_0"):
        mixer_sums.finish(0, middle_done)
    for way in range(2):
        gather_copy(x2buf, 1, way, 2 * way).start()
    with scope("r0_w2"):
        reduce_low.wave(2)
    with scope("finish1_1"):
        mixer_sums.finish(1, middle_done)
    for way in range(2):
        gather_copy(x2buf, 1, way, 2 * way + 1).start()
    with scope("e_w4"):
        expand_blocks.wave(4)
    with scope("pass2_0"):
        gather_pass_on(x2buf, 1, 0)
    with scope("r1_w2"):
        reduce_high.wave(2)
    with scope("pass2_1"):
        gather_pass_on(x2buf, 1, 1)
    for k in range(2):
        for way in range(2):
            gather_copy(x2buf, 1, way, 2 * (1 - way) + k).start()

    outer, inner = ((64, 128),), ((0, 64), (192, 64))
    far, own = ((SF * R, R),), ((SO * R, R),)
    with scope("e_d2d"):
        expand_blocks.shared(0)
        expand_blocks.shared(1)
    with scope("up_outer"):
        feed_up(outer)
    with scope("r0_w3"):
        reduce_low.wave(3)
    with scope("r_d2d_0"):
        reduce_low.shared(0)
        reduce_high.shared(0)
    with scope("down_outer_0"):
        feed_down(outer, 0)
    ff_sums[0].own()
    with scope("r1_w3"):
        reduce_high.wave(3)
    with scope("far2"):
        gather_far(x2buf, 1)
    with scope("feed_far_0"):
        feed_up(far)
        feed_down(far, 0)
    ff_sums[0].far()
    with scope("r0_w4"):
        reduce_low.wave(4)
    with scope("r1_w4"):
        reduce_high.wave(4)
    with scope("r_d2d_1"):
        reduce_low.shared(1)
        reduce_high.shared(1)
    with scope("down_outer_1"):
        feed_down(outer, 1)
    ff_sums[1].own()
    with scope("down_far_1"):
        feed_down(far, 1)
    ff_sums[1].far()
    with scope("near2"):
        gather_near(x2buf, 1)
    with scope("feed_inner_0"):
        feed_up(inner)
        feed_down(inner, 0)
    with scope("join2_0"):
        ff_sums[0].join(0)
        ff_sums[0].join(1)
    with scope("feed_inner_1"):
        feed_down(inner, 1)
    with scope("feed_own"):
        feed_up(own)
        feed_down(own, 0)
        feed_down(own, 1)
    with scope("join2_1"):
        ff_sums[1].join(0)
        ff_sums[1].join(1)

    def result_done(g):
        def done(row, total):
            for p, shard in enumerate(columns[g]):
                lanes = pl.ds(pl.multiple_of(shard * 128, 128), 128)
                mine = x2buf[pl.ds(SO * R + row, CHUNK), lanes].astype(F32)
                added = mine + total[:, p * 128 : (p + 1) * 128]
                result[pl.ds(row, CHUNK), lanes] = added.astype(BF16)

        return done

    def result_copy(row):
        rows = pl.ds(row, CHUNK)
        return pltpu.make_async_copy(result.at[rows], out.at[rows], out_sem.at[row // CHUNK])

    for g in range(2):
        for k in range(2):
            with scope(f"finish2_{g}_{k}"):
                ff_sums[g].finish(k, result_done(g))
            if g == 1:
                for way in range(2):
                    result_copy(64 * way + CHUNK * k).start()

    with scope("drain"):
        for phase, buf in ((0, xbuf), (1, x2buf)):
            ref = buf.at[pl.ds(0, 12 * CHUNK)]
            rcopy(ref, ref, ag_send.at[phase], ag_recv.at[phase, 0], sib).wait_send()
        for sums in (mixer_sums, *ff_sums):
            ref = sums.part.at[pl.ds(0, 12 * CHUNK)]
            rcopy(ref, ref, rs_send.at[sums.stage], rs_recv.at[sums.stage, 0], sib).wait_send()
        rcopy(all_stats, all_stats, st_send.at[0], st_recv.at[0], sib).wait_send()
        for copy in (small_copy, spatial_copy):
            copy.wait_send()
        for blocks in (value_blocks, dm_blocks, expand_blocks, reduce_low, reduce_high):
            blocks.sent()
        for k in range(4):
            result_copy(CHUNK * k).wait()


def layer(*args):
    (
        tokens,
        mixer_gain,
        direct_weight,
        direct_scale,
        value_weight,
        value_scale,
        value_gain,
        value_shift,
        spatial_weight,
        spatial_bias,
        merge_weight,
        merge_scale,
        channel_gain,
        expand_weight,
        expand_scale,
        reduce_weight,
        reduce_scale,
    ) = args
    operands = (
        tokens,
        mixer_gain.reshape(16, 128),
        direct_weight,
        direct_scale.reshape(1, CW),
        value_weight,
        value_scale.reshape(1, CW),
        value_gain.reshape(1, CW),
        value_shift.reshape(1, CW),
        spatial_weight,
        spatial_bias,
        merge_weight,
        merge_scale.reshape(1, 128),
        channel_gain.reshape(16, 128),
        expand_weight,
        expand_scale.reshape(1, HW),
        reduce_weight,
        reduce_scale.reshape(1, 128),
    )
    dma = pltpu.SemaphoreType.DMA
    return pl.pallas_call(
        kernel,
        out_shape=jax.ShapeDtypeStruct((R, D), BF16),
        in_specs=[pl.BlockSpec(memory_space=pl.ANY)] * 17,
        out_specs=pl.BlockSpec(memory_space=pl.ANY),
        scratch_shapes=[
            *(pltpu.VMEM(operand.shape, operand.dtype) for operand in operands[1:]),
            pltpu.VMEM((2, D, 128), BF16),
            pltpu.VMEM((2, D, 256), BF16),
            pltpu.VMEM((2, D, HW), BF16),
            pltpu.VMEM((16, 2 * HW, 128), BF16),
            pltpu.VMEM((4 * R, D), BF16),
            pltpu.VMEM((4 * R, D), BF16),
            pltpu.VMEM((4 * R, D), BF16),
            pltpu.VMEM((2, 4 * R, D // 2), BF16),
            pltpu.VMEM((2, 64, D), BF16),
            pltpu.VMEM((2, R, D), BF16),
            pltpu.VMEM((2, 64, D), BF16),
            pltpu.VMEM((2, 2, 64, D // 2), BF16),
            pltpu.VMEM((2, 2, R, D // 2), BF16),
            pltpu.VMEM((2, 2, 64, D // 2), BF16),
            pltpu.VMEM((4 * R, D), BF16),
            pltpu.VMEM((4 * R, 256), F32),
            pltpu.VMEM((4 * R, 256), F32),
            pltpu.VMEM((4 * R, 256), BF16),
            pltpu.VMEM((4 * R, 128), F32),
            pltpu.VMEM((4, 8, 128), F32),
            pltpu.VMEM((8, 128), F32),
            pltpu.VMEM((2, 8, 128), F32),
            pltpu.VMEM((2, 2, 128, 128), BF16),
            pltpu.VMEM((2, 128, 128), F32),
            pltpu.VMEM((R, D), BF16),
            dma((17,)),
            dma((4,)),
            dma((2,)),
            dma((2, 4)),
            dma((3,)),
            dma((3, 5)),
            dma((1,)),
            dma((1,)),
            dma((2,)),
            dma((2,)),
            dma((10,)),
            dma((10,)),
            dma((10, 8)),
            dma((10, 2)),
        ],
        compiler_params=pltpu.CompilerParams(
            collective_id=0, has_side_effects=True, vmem_limit_bytes=60 * 1024 * 1024
        ),
        name="layer",
    )(*operands)


def solution(mesh):
    finer = Mesh(mesh.devices.reshape(2, 4, 4, 4, 2), AXES)
    in_specs = (
        P(AXES, None),
        P(),
        P(FS, TP),
        P(TP),
        P(FS, TP),
        P(TP),
        P(TP),
        P(TP),
        P(TP, None, None),
        P(TP, None),
        P(TP, FS),
        P(FS),
        P(),
        P(FS, TP),
        P(TP),
        P(TP, FS),
        P(FS),
    )
    return jax.shard_map(layer, mesh=finer, in_specs=in_specs, out_specs=P(AXES, None), check_vma=False)
```

```python
import functools

import jax
import jax.numpy as jnp
from jax import lax
from jax.experimental import pallas as pl
from jax.experimental.pallas import tpu as pltpu
from jax.sharding import Mesh
from jax.sharding import PartitionSpec as P

AXES = ("zh", "zl", "x", "y", "c")
FS = ("zl", "x")
TP = ("y", "c")
EPS = 1e-6
MESH = pl.DeviceIdType.MESH
F32 = jnp.float32
BF16 = jnp.bfloat16

D = 2048
R = 128
CW = 128
HW = 1024
BRANCH = 1024
SN, SP, SF, SO = 0, 1, 2, 3
CHUNK = 32


def gelu(u):
    return jax.nn.gelu(u, approximate=True)


FIRST = ((0, 0), (1, 0), (3, 0), (0, 1), (0, 3), (1, 1), (1, 3), (3, 1))
LAST = ((3, 3), (2, 0), (0, 2), (2, 1), (2, 3), (1, 2), (3, 2), (2, 2))


class Gather:
    def __init__(self, view, span, a, b, pa, pb, sib, send, send_d2d, recv, recv_d2d):
        self.view, self.span = view, span
        self.a, self.b, self.pa, self.pb, self.sib = a, b, pa, pb, sib
        self.send, self.send_d2d, self.recv, self.recv_d2d = send, send_d2d, recv, recv_d2d

    def item(self, da, db, half=None):
        return self.view(lax.rem(self.pa + 4 - da, 4), lax.rem(self.pb + 4 - db, 4), half)

    def copy(self, ref, stage, to):
        return pltpu.make_async_remote_copy(
            src_ref=ref,
            dst_ref=ref,
            send_sem=self.send,
            recv_sem=self.recv.at[stage],
            device_id=to,
            device_id_type=MESH,
        )

    def landed(self, stage, count):
        self.copy(self.span(count), stage, self.sib).wait_recv()

    def along_b(self, da, stage):
        for k in range(2):
            self.copy(self.item(da, 0), stage, self.b[k]).start()

    def across(self, da, db):
        ref = self.item(da, db)
        pltpu.make_async_remote_copy(
            src_ref=ref,
            dst_ref=ref,
            send_sem=self.send_d2d,
            recv_sem=self.recv_d2d.at[0 if (da, db) in FIRST else 1],
            device_id=self.sib,
            device_id_type=MESH,
        ).start()

    def on_b(self, da, stage):
        for k in range(2):
            db = (1, 3)[k]
            self.copy(self.item(da, db, k), stage, self.b[k]).start()
            self.across(da, db)

    def wave0(self):
        for k in range(2):
            self.copy(self.item(0, 0), 0, self.a[k]).start()
        self.along_b(0, 1)
        self.across(0, 0)

    def wave1(self):
        self.landed(0, 2)
        for k in range(2):
            da = (1, 3)[k]
            self.copy(self.item(da, 0, k), 2, self.a[k]).start()
            self.along_b(da, 3)
            self.across(da, 0)
        self.landed(1, 2)
        self.on_b(0, 4)

    def wave2(self):
        self.landed(2, 1)
        self.along_b(2, 5)
        self.across(2, 0)
        self.landed(3, 4)
        self.on_b(1, 6)
        self.on_b(3, 6)
        self.landed(4, 1)
        self.across(0, 2)

    def wave3(self):
        self.landed(5, 2)
        self.on_b(2, 7)
        self.landed(6, 2)
        self.across(1, 2)
        self.across(3, 2)

    def wave4(self):
        self.landed(7, 1)
        self.across(2, 2)


class DirectGather(Gather):
    def wave0(self):
        for k in range(2):
            self.copy(self.item(0, 0), 0, self.a[k]).start()
        for k in range(2):
            self.copy(self.item(0, 0, k), 0, self.far_a[k]).start()
        self.along_b(0, 1)
        self.across(0, 0)

    def wave1(self):
        self.landed(0, 3)
        for da in (1, 3, 2):
            self.along_b(da, 2)
        self.landed(1, 2)
        self.on_b(0, 3)
        for da in (1, 3, 2):
            self.across(da, 0)

    def wave2(self):
        self.landed(2, 6)
        for da in (1, 3, 2):
            self.on_b(da, 4)
        self.landed(3, 1)
        self.across(0, 2)

    def wave3(self):
        self.landed(4, 3)
        for da in (1, 3, 2):
            self.across(da, 2)


def kernel(
    tokens,
    mixer_gain_hbm,
    direct_weight_hbm,
    direct_scale_hbm,
    value_weight_hbm,
    value_scale_hbm,
    value_gain_hbm,
    value_shift_hbm,
    spatial_weight_hbm,
    spatial_bias_hbm,
    merge_weight_hbm,
    merge_scale_hbm,
    channel_gain_hbm,
    expand_weight_hbm,
    expand_scale_hbm,
    reduce_weight_hbm,
    reduce_scale_hbm,
    out,
    mixer_gain,
    direct_weight,
    direct_scale,
    value_weight,
    value_scale,
    value_gain,
    value_shift,
    spatial_weight,
    spatial_bias,
    merge_weight,
    merge_scale,
    channel_gain,
    expand_weight,
    expand_scale,
    reduce_weight,
    reduce_scale,
    valw,
    dmw,
    we,
    wr,
    xbuf,
    x2buf,
    part1,
    part2,
    rel1,
    near1,
    mrg1,
    rel2,
    near2,
    mrg2,
    hbuf,
    dbuf,
    vbuf,
    gbuf,
    rbuf,
    stat,
    totals,
    small,
    swb,
    bias,
    result,
    base,
    in_sem,
    out_sem,
    ag_send,
    ag_recv,
    rs_send,
    rs_recv,
    st_send,
    st_recv,
    sm_send,
    sm_recv,
    w_send,
    w_send_d2d,
    w_recv,
    w_recv_d2d,
):
    zh, zl, x, y, c = (lax.axis_index(name) for name in AXES)
    z = zh * 4 + zl
    fs = zl * 4 + x
    other = 1 - c
    scope = jax.named_scope

    def at_z(w):
        w = lax.rem(w, 8)
        return {"zh": lax.div(w, 4), "zl": lax.rem(w, 4)}

    xs = ({"x": lax.rem(x + 1, 4)}, {"x": lax.rem(x + 3, 4)})
    zs = (at_z(z + 1), at_z(z + 7))
    xs_far = ({"x": lax.rem(x + 2, 4)},) * 2
    zs_far = (at_z(z + 2), at_z(z + 6))
    ynext, yprev, yfar = ({"y": lax.rem(y + k, 4)} for k in (1, 3, 2))
    sib = {"c": other}

    barrier = pltpu.get_barrier_semaphore()
    for to in (*xs, xs_far[0], *zs, *zs_far, ynext, yprev, yfar, sib):
        pl.semaphore_signal(barrier, inc=1, device_id=to, device_id_type=MESH)

    inputs = [
        pltpu.make_async_copy(src, dst, in_sem.at[k])
        for k, (src, dst) in enumerate(
            (
                (tokens, xbuf.at[pl.ds(SO * R, R)]),
                (mixer_gain_hbm, mixer_gain),
                (direct_weight_hbm, direct_weight),
                (direct_scale_hbm, direct_scale),
                (value_weight_hbm, value_weight),
                (value_scale_hbm, value_scale),
                (merge_weight_hbm, merge_weight),
                (merge_scale_hbm, merge_scale),
                (channel_gain_hbm, channel_gain),
                (expand_weight_hbm, expand_weight),
                (expand_scale_hbm, expand_scale),
                (reduce_weight_hbm, reduce_weight),
                (reduce_scale_hbm, reduce_scale),
                (value_gain_hbm, value_gain),
                (value_shift_hbm, value_shift),
                (spatial_bias_hbm, spatial_bias),
                (spatial_weight_hbm, spatial_weight),
            )
        )
    ]
    for copy in inputs:
        copy.start()

    def rcopy(src, dst, ssem, rsem, to):
        return pltpu.make_async_remote_copy(
            src_ref=src, dst_ref=dst, send_sem=ssem, recv_sem=rsem, device_id=to, device_id_type=MESH
        )

    def gather_copy(buf, phase, way, k):
        if k < 4:
            src = buf.at[pl.ds(SO * R + CHUNK * k, CHUNK)]
            dst = buf.at[pl.ds((SP, SN)[way] * R + CHUNK * k, CHUNK)]
            stage = k - 2 * way if k // 2 == way else 2
        else:
            row = 64 * way + CHUNK * (k - 4)
            src = buf.at[pl.ds((SP, SN)[way] * R + row, CHUNK)]
            dst = buf.at[pl.ds(SF * R + row, CHUNK)]
            stage = 3
        return rcopy(src, dst, ag_send.at[phase], ag_recv.at[phase, stage], (ynext, yprev)[way])

    def gather_landed(buf, phase, stage, chunks):
        ref = buf.at[pl.ds(0, chunks * CHUNK)]
        rcopy(ref, ref, ag_send.at[phase], ag_recv.at[phase, stage], sib).wait_recv()

    def gather_pass_on(buf, phase, k):
        gather_landed(buf, phase, k, 2)
        for way in range(2):
            gather_copy(buf, phase, way, 4 + k).start()

    def gather_near(buf, phase):
        gather_landed(buf, phase, 2, 4)

    def gather_far(buf, phase):
        gather_landed(buf, phase, 3, 4)

    class Scatter:
        def __init__(self, stage, part, near, rel, mrg, mine):
            self.stage, self.part, self.near, self.rel, self.mrg = stage, part, near, rel, mrg
            self.mine = mine

        def copy(self, src, dst, way, k):
            return rcopy(
                src, dst, rs_send.at[self.stage], rs_recv.at[self.stage, k], (ynext, yprev)[way]
            )

        def landed(self, k, rows):
            ref = self.part.at[pl.ds(0, rows)]
            rcopy(ref, ref, rs_send.at[self.stage], rs_recv.at[self.stage, k], sib).wait_recv()

        def own(self):
            for way in range(2):
                row = 64 * (1 - way)
                src = self.part.at[pl.ds((SN, SP)[way] * R + row, 64)]
                self.copy(src, self.near.at[way, pl.ds(row, 64)], way, 0).start()

        def far(self):
            for k in range(2):
                for way in range(2):
                    row = CHUNK * k
                    src = self.part.at[pl.ds(SF * R + 64 * way + row, CHUNK)]
                    self.copy(src, self.rel.at[way, pl.ds(row, CHUNK)], way, 1 + k).start()

        def join(self, k):
            self.landed(1 + k, 2 * CHUNK)
            for way in range(2):
                row = CHUNK * k
                mine = self.part[pl.ds((SN, SP)[way] * R + 64 * way + row, CHUNK), :].astype(F32)
                came = self.rel[way, pl.ds(row, CHUNK), :].astype(F32)
                joined = self.mrg.at[way, pl.ds(row, CHUNK)]
                joined[...] = (mine + came).astype(BF16)
                self.copy(joined, self.near.at[way, pl.ds(64 * way + row, CHUNK)], way, 3 + k).start()

        def finish(self, k, done):
            if k == 0:
                self.landed(0, 128)
            self.landed(3 + k, 2 * CHUNK)
            for way in range(2):
                row = 64 * way + CHUNK * k
                total = self.mine(row) + self.near[0, pl.ds(row, CHUNK), :].astype(F32)
                done(row, total + self.near[1, pl.ds(row, CHUNK), :].astype(F32))

    mixer_sums = Scatter(
        0, part1, near1, rel1, mrg1, lambda row: part1[pl.ds(SO * R + row, CHUNK), :].astype(F32)
    )
    ff_sums = [
        Scatter(
            1 + g,
            part2.at[g],
            near2.at[g],
            rel2.at[g],
            mrg2.at[g],
            lambda row, g=g: base[g, pl.ds(row, CHUNK), :],
        )
        for g in range(2)
    ]

    def view_rows(ref, low):
        def view(pz, px, half):
            row = (pz * 4 + px) * 128 + low
            if half is None:
                return ref.at[c, pl.ds(pl.multiple_of(row, 64), 64)]
            return ref.at[c, pl.ds(pl.multiple_of(row + 32 * half, 32), 32)]

        return view

    def span_rows(ref):
        return lambda count: ref.at[c, pl.ds(0, 64 * count)]

    def view_reduce(low):
        def view(pz, px, half):
            row = c * HW + low
            if half is None:
                return wr.at[pz * 4 + px, pl.ds(pl.multiple_of(row, 256), 256)]
            return wr.at[pz * 4 + px, pl.ds(pl.multiple_of(row + 128 * half, 128), 128)]

        return view

    def span_reduce(count):
        return wr.at[pl.ds(0, count), pl.ds(0, 256)]

    def weight(index, view, span, x_first, form=Gather):
        if x_first:
            a, b, pa, pb, turned = xs, zs, x, zl, lambda p, q, h: view(q, p, h)
        else:
            a, b, pa, pb, turned = zs, xs, zl, x, view
        blocks = form(
            turned,
            span,
            a,
            b,
            pa,
            pb,
            sib,
            w_send.at[index],
            w_send_d2d.at[index],
            w_recv.at[index],
            w_recv_d2d.at[index],
        )
        blocks.far_a = xs_far if x_first else zs_far
        return blocks

    class Pair:
        def __init__(self, index, low, high, span, form=Gather):
            self.index, self.span = index, span
            self.halves = (
                weight(index, low, span, True, form),
                weight(index + 1, high, span, False, form),
            )

        def wave(self, k):
            for half in self.halves:
                getattr(half, f"wave{k}")()

        def shared(self, group):
            for half in self.halves:
                ref = self.span(8)
                rcopy(ref, ref, half.send_d2d, half.recv_d2d.at[group], sib).wait_recv()

        def sent(self):
            for half in self.halves:
                ref = self.span(15)
                rcopy(ref, ref, half.send, half.recv_d2d.at[0], sib).wait_send()
                ref = self.span(16)
                rcopy(ref, ref, half.send_d2d, half.recv_d2d.at[0], sib).wait_send()

    value_blocks = Pair(0, view_rows(valw, 0), view_rows(valw, 64), span_rows(valw), DirectGather)
    dm_blocks = Pair(2, view_rows(dmw, 0), view_rows(dmw, 64), span_rows(dmw), DirectGather)
    expand_blocks = Pair(4, view_rows(we, 0), view_rows(we, 64), span_rows(we))
    reduce_low = Pair(6, view_reduce(0), view_reduce(256), span_reduce)
    reduce_high = Pair(8, view_reduce(512), view_reduce(768), span_reduce)

    def column(row):
        return jnp.transpose(jnp.broadcast_to(row, (128, 128)))

    with scope("wait_tokens"):
        inputs[0].wait()
    with scope("wait_barrier"):
        pl.semaphore_wait(barrier, 11)

    def send_tokens():
        for k in range(4):
            for way in range(2):
                gather_copy(xbuf, 0, way, (k + 2 * way) % 4).start()

    pl.when(c == 1)(send_tokens)
    with scope("wait_mix"):
        for copy in inputs[1:8]:
            copy.wait()

    fs_row = pl.ds(pl.multiple_of(fs * 128, 128), 128)
    gain = column(mixer_gain[pl.ds(fs, 1), :])
    valw[c, fs_row, :] = (value_weight[...] * gain * value_scale[...]).astype(BF16)
    dmw[c, fs_row, 0:128] = (direct_weight[...] * gain * direct_scale[...]).astype(BF16)
    dmw[c, fs_row, 128:256] = (merge_weight[...] * merge_scale[...]).astype(BF16)
    value_blocks.wave(0)
    dm_blocks.wave(0)
    for copy in inputs[8:]:
        copy.wait()
    gain = column(channel_gain[pl.ds(fs, 1), :])
    for k in range(8):
        lanes = slice(k * 128, (k + 1) * 128)
        we[c, fs_row, lanes] = (expand_weight[:, lanes] * gain * expand_scale[:, lanes]).astype(BF16)
    for k in range(8):
        rows = pl.ds(pl.multiple_of(c * HW + k * 128, 128), 128)
        wr[fs, rows, :] = (reduce_weight[k * 128 : (k + 1) * 128, :] * reduce_scale[...]).astype(BF16)
    small[c, 0:1, :] = value_gain[...]
    small[c, 1:2, :] = value_shift[...]
    small[c, 2:4, :] = spatial_bias[...]
    small[c, 4:8, :] = jnp.zeros((4, 128), F32)
    swb[c] = spatial_weight[...]
    small_copy = rcopy(small.at[c], small.at[c], sm_send.at[0], sm_recv.at[0], sib)
    spatial_copy = rcopy(spatial_weight, swb.at[c], sm_send.at[1], sm_recv.at[1], sib)
    small_copy.start()
    spatial_copy.start()

    def row_scales(buf, start, count):
        @pl.loop(0, count // 32)
        def _(i):
            rows = pl.ds(pl.multiple_of(start + i * 32, 32), 32)
            floats = buf[rows, :].astype(F32)
            power = jnp.mean(floats * floats, axis=-1, keepdims=True)
            rbuf[rows, :] = jnp.broadcast_to(lax.rsqrt(power + EPS), (32, 128))

    lane = lax.broadcasted_iota(jnp.int32, (128, 128), 1)
    block_of = {SP: lax.rem(y + 3, 4), SN: lax.rem(y + 1, 4), SF: lax.rem(y + 2, 4), SO: y}

    def project(slots):
        start, count = slots[0] * R, len(slots) * R
        rows = pl.ds(start, count)
        weights = jnp.concatenate([valw[0], valw[1]], axis=1)
        value = jnp.dot(xbuf[rows, :], weights, preferred_element_type=F32)
        scale = rbuf[rows, :]
        vbuf[rows, :] = gelu(value * jnp.concatenate([scale, scale], axis=1))
        for slot in slots:
            v = vbuf[pl.ds(slot * R, R), :]
            total = jnp.sum(v, axis=1, keepdims=True)
            squares = jnp.sum(v * v, axis=1, keepdims=True)
            tile = jnp.where(lane == 0, total, jnp.where(lane == 1, squares, 0.0))
            sums = jnp.transpose(tile)
            stat[0, pl.ds(block_of[slot], 1), :] = sums[0:1, :]
            stat[0, pl.ds(4 + block_of[slot], 1), :] = sums[1:2, :]

    def project_direct():
        weights = jnp.concatenate([dmw[0, :, 0:128], dmw[1, :, 0:128]], axis=1)

        @pl.loop(0, 2)
        def _(i):
            rows = pl.ds(pl.multiple_of(i * 256, 256), 256)
            direct = jnp.dot(xbuf[rows, :], weights, preferred_element_type=F32)
            scale = rbuf[rows, :]
            dbuf[rows, :] = gelu(direct * jnp.concatenate([scale, scale], axis=1))

    def mixing(slots):
        for slot in slots:
            rows = pl.ds(slot * R, R)
            block = block_of[slot]
            mean = column(totals[pl.ds(block, 1), :]) / BRANCH
            var = column(totals[pl.ds(4 + block, 1), :]) / BRANCH - mean * mean
            inv = lax.rsqrt(var + EPS)
            for k in range(2):
                lanes = slice(k * 128, (k + 1) * 128)
                v = vbuf[rows, lanes]
                g = ((v - mean) * inv * small[k, 0:1, :] + small[k, 1:2, :]).astype(BF16)
                low = jnp.dot(swb[k, 0], g, preferred_element_type=F32)
                high = jnp.dot(swb[k, 1], g, preferred_element_type=F32)
                mixed = jnp.where(lane < 64, low, high) + bias[k]
                gbuf[rows, lanes] = (dbuf[rows, lanes] * mixed).astype(BF16)
        rows = pl.ds(slots[0] * R, len(slots) * R)

        @pl.loop(0, 2)
        def _(j):
            weights = jnp.concatenate(
                [
                    jnp.concatenate(
                        [
                            dmw[k, pl.ds(pl.multiple_of(j * 1024 + i * 128, 128), 128), 128:256]
                            for i in range(8)
                        ],
                        axis=1,
                    )
                    for k in range(2)
                ],
                axis=0,
            )
            product = jnp.dot(gbuf[rows, :], weights, preferred_element_type=F32)
            part1[rows, pl.ds(pl.multiple_of(j * 1024, 1024), 1024)] = product.astype(BF16)

    def gathered_rows(ref, pieces):
        loaded = [ref[pl.ds(start, count), :] for start, count in pieces]
        return loaded[0] if len(loaded) == 1 else jnp.concatenate(loaded, axis=0)

    def store_rows(ref, pieces, cols, values):
        at = 0
        for start, count in pieces:
            ref[pl.ds(start, count), cols] = values[at : at + count, :]
            at += count

    def feed_up(pieces):
        for start, count in pieces:
            row_scales(x2buf, start, count)

        @pl.loop(0, 2)
        def _(j):
            upper = jnp.dot(gathered_rows(x2buf, pieces), we[j], preferred_element_type=F32)
            upper = upper * jnp.concatenate([gathered_rows(rbuf, pieces)] * 8, axis=1)
            hidden = jnp.square(jnp.maximum(upper, 0.0)).astype(BF16)
            store_rows(hbuf, pieces, pl.ds(pl.multiple_of(j * HW, HW), HW), hidden)

    def shard_of(dx, dz):
        return lax.rem(zl + 4 - dz, 4) * 4 + lax.rem(x + 4 - dx, 4)

    columns = [[shard_of(*offsets) for offsets in group] for group in (FIRST, LAST)]

    def feed_down(pieces, g):
        weights = jnp.concatenate([wr[shard] for shard in columns[g]], axis=1)
        product = jnp.dot(gathered_rows(hbuf, pieces), weights, preferred_element_type=F32)
        store_rows(part2.at[g], pieces, slice(None), product.astype(BF16))

    def feed_own(g):
        weights = jnp.concatenate([wr[shard] for shard in columns[g]], axis=1)
        rows = pl.ds(SO * R, R)
        middle = [x2buf[rows, pl.ds(pl.multiple_of(shard * 128, 128), 128)] for shard in columns[g]]
        product = jnp.dot(hbuf[rows, :], weights, preferred_element_type=F32)
        base[g] = jnp.concatenate(middle, axis=1).astype(F32) + product.astype(BF16).astype(F32)

    row_scales(xbuf, SO * R, R)
    with scope("v_w1"):
        value_blocks.wave(1)
    with scope("dm_w1"):
        dm_blocks.wave(1)
    pl.when(c == 0)(send_tokens)

    @pl.when(c == 1)
    def _():
        gather_pass_on(xbuf, 0, 0)
        gather_pass_on(xbuf, 0, 1)

    with scope("v_w2"):
        value_blocks.wave(2)
    expand_blocks.halves[0].wave0()

    @pl.when(c == 1)
    def _():
        with scope("scales_1"):
            gather_near(xbuf, 0)
            row_scales(xbuf, 0, 2 * R)

    @pl.when(c == 0)
    def _():
        with scope("pass1_0"):
            gather_pass_on(xbuf, 0, 0)

    with scope("dm_w2"):
        dm_blocks.wave(2)
    expand_blocks.halves[1].wave0()
    reduce_low.wave(0)
    with scope("v_w3"):
        value_blocks.wave(3)

    @pl.when(c == 1)
    def _():
        gather_far(xbuf, 0)
        row_scales(xbuf, 2 * R, R)

    @pl.when(c == 0)
    def _():
        with scope("pass1_1"):
            gather_pass_on(xbuf, 0, 1)

    with scope("v_d2d"):
        value_blocks.shared(0)
        value_blocks.shared(1)
    with scope("project_own"):
        project((SO,))

    @pl.when(c == 1)
    def _():
        project((SN, SP))

    with scope("dm_w3"):
        dm_blocks.wave(3)

    @pl.when(c == 0)
    def _():
        with scope("scales_0"):
            gather_near(xbuf, 0)
            row_scales(xbuf, 0, 2 * R)
        with scope("project_near"):
            project((SN, SP))
        with scope("e_w1_0"):
            expand_blocks.wave(1)
        with scope("far1"):
            gather_far(xbuf, 0)
            row_scales(xbuf, 2 * R, R)

    with scope("project_far"):
        project((SF,))
    stat_copies = [
        rcopy(stat.at[0], stat.at[k + 1], st_send.at[0], st_recv.at[0], to)
        for k, to in enumerate((ynext, yprev, yfar))
    ]
    for copy in stat_copies:
        copy.start()
    reduce_high.wave(0)
    with scope("dm_d2d"):
        dm_blocks.shared(0)
        dm_blocks.shared(1)
    with scope("direct"):
        project_direct()
        rcopy(small.at[other], small.at[other], sm_send.at[0], sm_recv.at[0], sib).wait_recv()
        rcopy(swb.at[other], swb.at[other], sm_send.at[1], sm_recv.at[1], sib).wait_recv()
        for k in range(2):
            rows = jnp.concatenate(
                [jnp.broadcast_to(small[k, 2 + g : 3 + g, :], (64, 128)) for g in range(2)], axis=0
            )
            bias[k] = jnp.transpose(rows)

    @pl.when(c == 1)
    def _():
        with scope("e_w1_1"):
            expand_blocks.wave(1)

    with scope("wait_stats"):
        all_stats = stat.at[pl.ds(1, 3)]
        rcopy(all_stats, all_stats, st_send.at[0], st_recv.at[0], sib).wait_recv()
        totals[...] = stat[0] + stat[1] + stat[2] + stat[3]
    with scope("mixing_near"):
        mixing((SN, SP))
    mixer_sums.own()
    with scope("mixing_far"):
        mixing((SF,))
    mixer_sums.far()
    with scope("mixing_own"):
        mixing((SO,))

    @pl.when(c == 1)
    def _():
        with scope("join1_0_1"):
            mixer_sums.join(0)

    with scope("e_w2"):
        expand_blocks.wave(2)
    with scope("r0_w1"):
        reduce_low.wave(1)

    @pl.when(c == 0)
    def _():
        with scope("join1_0_0"):
            mixer_sums.join(0)

    with scope("join1_1"):
        mixer_sums.join(1)
    with scope("e_w3"):
        expand_blocks.wave(3)
    with scope("r1_w1"):
        reduce_high.wave(1)

    def middle_done(row, total):
        rows = pl.ds(SO * R + row, CHUNK)
        x2buf[rows, :] = (xbuf[rows, :].astype(F32) + total).astype(BF16)

    with scope("finish1_0"):
        mixer_sums.finish(0, middle_done)
    for way in range(2):
        gather_copy(x2buf, 1, way, 2 * way).start()
    with scope("finish1_1"):
        mixer_sums.finish(1, middle_done)
    for way in range(2):
        gather_copy(x2buf, 1, way, 2 * way + 1).start()
    with scope("r0_w2"):
        reduce_low.wave(2)
    with scope("e_w4"):
        expand_blocks.wave(4)
    with scope("pass2_0"):
        gather_pass_on(x2buf, 1, 0)
    with scope("r1_w2"):
        reduce_high.wave(2)
    with scope("pass2_1"):
        gather_pass_on(x2buf, 1, 1)
    for k in range(2):
        for way in range(2):
            gather_copy(x2buf, 1, way, 2 * (1 - way) + k).start()

    outer, inner = ((64, 128),), ((0, 64), (192, 64))
    far, own = ((SF * R, R),), ((SO * R, R),)
    with scope("e_d2d"):
        expand_blocks.shared(0)
        expand_blocks.shared(1)
    with scope("up_outer"):
        feed_up(outer)
    with scope("r0_w3"):
        reduce_low.wave(3)
    with scope("r_d2d_0"):
        reduce_low.shared(0)
        reduce_high.shared(0)
    with scope("down_outer_0"):
        feed_down(outer, 0)
    ff_sums[0].own()
    with scope("r1_w3"):
        reduce_high.wave(3)
    with scope("up_own"):
        feed_up(own)
    with scope("far2"):
        gather_far(x2buf, 1)
    with scope("r0_w4"):
        reduce_low.wave(4)
    with scope("r1_w4"):
        reduce_high.wave(4)
    with scope("feed_far_0"):
        feed_up(far)
        feed_down(far, 0)
    ff_sums[0].far()
    with scope("down_own_0"):
        feed_own(0)
    with scope("r_d2d_1"):
        reduce_low.shared(1)
        reduce_high.shared(1)
    with scope("down_outer_1"):
        feed_down(outer, 1)
    ff_sums[1].own()
    with scope("down_far_1"):
        feed_down(far, 1)
    ff_sums[1].far()
    with scope("near2"):
        gather_near(x2buf, 1)
    with scope("feed_inner_0"):
        feed_up(inner)
        feed_down(inner, 0)
    with scope("join2_0"):
        ff_sums[0].join(0)
        ff_sums[0].join(1)
    with scope("feed_inner_1"):
        feed_down(inner, 1)
    with scope("join2_1_0"):
        ff_sums[1].join(0)
    with scope("join2_1_1"):
        ff_sums[1].join(1)
    with scope("down_own_1"):
        feed_own(1)

    def result_done(g):
        def done(row, total):
            result[g, pl.ds(row, CHUNK), :] = total.astype(BF16)

        return done

    for g in range(2):
        for k in range(2):
            with scope(f"finish2_{g}_{k}"):
                ff_sums[g].finish(k, result_done(g))
        for p, shard in enumerate(columns[g]):
            pltpu.make_async_copy(
                result.at[g, :, pl.ds(p * 128, 128)],
                out.at[:, pl.ds(pl.multiple_of(shard * 128, 128), 128)],
                out_sem.at[0],
            ).start()

    with scope("drain"):
        for phase, buf in ((0, xbuf), (1, x2buf)):
            ref = buf.at[pl.ds(0, 12 * CHUNK)]
            rcopy(ref, ref, ag_send.at[phase], ag_recv.at[phase, 0], sib).wait_send()
        for sums in (mixer_sums, *ff_sums):
            ref = sums.part.at[pl.ds(0, 12 * CHUNK)]
            rcopy(ref, ref, rs_send.at[sums.stage], rs_recv.at[sums.stage, 0], sib).wait_send()
        rcopy(all_stats, all_stats, st_send.at[0], st_recv.at[0], sib).wait_send()
        for copy in (small_copy, spatial_copy):
            copy.wait_send()
        for blocks in (value_blocks, dm_blocks, expand_blocks, reduce_low, reduce_high):
            blocks.sent()
        pltpu.make_async_copy(result, result, out_sem.at[0]).wait()


def layer(*args):
    (
        tokens,
        mixer_gain,
        direct_weight,
        direct_scale,
        value_weight,
        value_scale,
        value_gain,
        value_shift,
        spatial_weight,
        spatial_bias,
        merge_weight,
        merge_scale,
        channel_gain,
        expand_weight,
        expand_scale,
        reduce_weight,
        reduce_scale,
    ) = args
    operands = (
        tokens,
        mixer_gain.reshape(16, 128),
        direct_weight,
        direct_scale.reshape(1, CW),
        value_weight,
        value_scale.reshape(1, CW),
        value_gain.reshape(1, CW),
        value_shift.reshape(1, CW),
        spatial_weight,
        spatial_bias,
        merge_weight,
        merge_scale.reshape(1, 128),
        channel_gain.reshape(16, 128),
        expand_weight,
        expand_scale.reshape(1, HW),
        reduce_weight,
        reduce_scale.reshape(1, 128),
    )
    dma = pltpu.SemaphoreType.DMA
    return pl.pallas_call(
        kernel,
        out_shape=jax.ShapeDtypeStruct((R, D), BF16),
        in_specs=[pl.BlockSpec(memory_space=pl.ANY)] * 17,
        out_specs=pl.BlockSpec(memory_space=pl.ANY),
        scratch_shapes=[
            *(pltpu.VMEM(operand.shape, operand.dtype) for operand in operands[1:]),
            pltpu.VMEM((2, D, 128), BF16),
            pltpu.VMEM((2, D, 256), BF16),
            pltpu.VMEM((2, D, HW), BF16),
            pltpu.VMEM((16, 2 * HW, 128), BF16),
            pltpu.VMEM((4 * R, D), BF16),
            pltpu.VMEM((4 * R, D), BF16),
            pltpu.VMEM((4 * R, D), BF16),
            pltpu.VMEM((2, 4 * R, D // 2), BF16),
            pltpu.VMEM((2, 64, D), BF16),
            pltpu.VMEM((2, R, D), BF16),
            pltpu.VMEM((2, 64, D), BF16),
            pltpu.VMEM((2, 2, 64, D // 2), BF16),
            pltpu.VMEM((2, 2, R, D // 2), BF16),
            pltpu.VMEM((2, 2, 64, D // 2), BF16),
            pltpu.VMEM((4 * R, D), BF16),
            pltpu.VMEM((4 * R, 256), F32),
            pltpu.VMEM((4 * R, 256), F32),
            pltpu.VMEM((4 * R, 256), BF16),
            pltpu.VMEM((4 * R, 128), F32),
            pltpu.VMEM((4, 8, 128), F32),
            pltpu.VMEM((8, 128), F32),
            pltpu.VMEM((2, 8, 128), F32),
            pltpu.VMEM((2, 2, 128, 128), BF16),
            pltpu.VMEM((2, 128, 128), F32),
            pltpu.VMEM((2, R, D // 2), BF16),
            pltpu.VMEM((2, R, D // 2), F32),
            dma((17,)),
            dma((1,)),
            dma((2,)),
            dma((2, 4)),
            dma((3,)),
            dma((3, 5)),
            dma((1,)),
            dma((1,)),
            dma((2,)),
            dma((2,)),
            dma((10,)),
            dma((10,)),
            dma((10, 8)),
            dma((10, 2)),
        ],
        compiler_params=pltpu.CompilerParams(
            collective_id=0, has_side_effects=True, vmem_limit_bytes=60 * 1024 * 1024
        ),
        name="layer",
    )(*operands)


def solution(mesh):
    finer = Mesh(mesh.devices.reshape(2, 4, 4, 4, 2), AXES)
    in_specs = (
        P(AXES, None),
        P(),
        P(FS, TP),
        P(TP),
        P(FS, TP),
        P(TP),
        P(TP),
        P(TP),
        P(TP, None, None),
        P(TP, None),
        P(TP, FS),
        P(FS),
        P(),
        P(FS, TP),
        P(TP),
        P(TP, FS),
        P(FS),
    )
    return jax.shard_map(layer, mesh=finer, in_specs=in_specs, out_specs=P(AXES, None), check_vma=False)
```

```python
import functools

import jax
import jax.numpy as jnp
from jax import lax
from jax.experimental import pallas as pl
from jax.experimental.pallas import tpu as pltpu
from jax.sharding import Mesh
from jax.sharding import PartitionSpec as P

AXES = ("zh", "zl", "x", "y", "c")
FS = ("zl", "x")
TP = ("y", "c")
EPS = 1e-6
MESH = pl.DeviceIdType.MESH
F32 = jnp.float32
BF16 = jnp.bfloat16

D = 2048
R = 128
CW = 128
HW = 1024
BRANCH = 1024
SN, SP, SF, SO = 0, 1, 2, 3
CHUNK = 32


def gelu(u):
    return jax.nn.gelu(u, approximate=True)


FIRST = ((0, 0), (1, 0), (3, 0), (0, 1), (0, 3), (1, 1), (1, 3), (3, 1))
LAST = ((3, 3), (2, 0), (0, 2), (2, 1), (2, 3), (1, 2), (3, 2), (2, 2))


class Gather:
    def __init__(self, view, span, a, b, pa, pb, sib, send, send_d2d, recv, recv_d2d):
        self.view, self.span = view, span
        self.a, self.b, self.pa, self.pb, self.sib = a, b, pa, pb, sib
        self.send, self.send_d2d, self.recv, self.recv_d2d = send, send_d2d, recv, recv_d2d

    def item(self, da, db, half=None):
        return self.view(lax.rem(self.pa + 4 - da, 4), lax.rem(self.pb + 4 - db, 4), half)

    def copy(self, ref, stage, to):
        return pltpu.make_async_remote_copy(
            src_ref=ref,
            dst_ref=ref,
            send_sem=self.send,
            recv_sem=self.recv.at[stage],
            device_id=to,
            device_id_type=MESH,
        )

    def landed(self, stage, count):
        self.copy(self.span(count), stage, self.sib).wait_recv()

    def along_b(self, da, stage):
        for k in range(2):
            self.copy(self.item(da, 0), stage, self.b[k]).start()

    def across(self, da, db):
        ref = self.item(da, db)
        pltpu.make_async_remote_copy(
            src_ref=ref,
            dst_ref=ref,
            send_sem=self.send_d2d,
            recv_sem=self.recv_d2d.at[0 if (da, db) in FIRST else 1],
            device_id=self.sib,
            device_id_type=MESH,
        ).start()

    def on_b(self, da, stage):
        for k in range(2):
            db = (1, 3)[k]
            self.copy(self.item(da, db, k), stage, self.b[k]).start()
            self.across(da, db)

    def wave0(self):
        for k in range(2):
            self.copy(self.item(0, 0), 0, self.a[k]).start()
        self.along_b(0, 1)
        self.across(0, 0)

    def wave1(self):
        self.landed(0, 2)
        for k in range(2):
            da = (1, 3)[k]
            self.copy(self.item(da, 0, k), 2, self.a[k]).start()
            self.along_b(da, 3)
            self.across(da, 0)
        self.landed(1, 2)
        self.on_b(0, 4)

    def wave2(self):
        self.landed(2, 1)
        self.along_b(2, 5)
        self.across(2, 0)
        self.landed(3, 4)
        self.on_b(1, 6)
        self.on_b(3, 6)
        self.landed(4, 1)
        self.across(0, 2)

    def wave3(self):
        self.landed(5, 2)
        self.on_b(2, 7)
        self.landed(6, 2)
        self.across(1, 2)
        self.across(3, 2)

    def wave4(self):
        self.landed(7, 1)
        self.across(2, 2)


class DirectGather(Gather):
    def wave0(self):
        for k in range(2):
            self.copy(self.item(0, 0), 0, self.a[k]).start()
        for k in range(2):
            self.copy(self.item(0, 0, k), 0, self.far_a[k]).start()
        self.along_b(0, 1)
        self.across(0, 0)

    def wave1(self):
        self.landed(0, 3)
        for da in (1, 3, 2):
            self.along_b(da, 2)
        self.landed(1, 2)
        self.on_b(0, 3)
        for da in (1, 3, 2):
            self.across(da, 0)

    def wave2(self):
        self.landed(2, 6)
        for da in (1, 3, 2):
            self.on_b(da, 4)
        self.landed(3, 1)
        self.across(0, 2)

    def wave3(self):
        self.landed(4, 3)
        for da in (1, 3, 2):
            self.across(da, 2)


def kernel(
    tokens,
    mixer_gain_hbm,
    direct_weight_hbm,
    direct_scale_hbm,
    value_weight_hbm,
    value_scale_hbm,
    value_gain_hbm,
    value_shift_hbm,
    spatial_weight_hbm,
    spatial_bias_hbm,
    merge_weight_hbm,
    merge_scale_hbm,
    channel_gain_hbm,
    expand_weight_hbm,
    expand_scale_hbm,
    reduce_weight_hbm,
    reduce_scale_hbm,
    out,
    mixer_gain,
    direct_weight,
    direct_scale,
    value_weight,
    value_scale,
    value_gain,
    value_shift,
    spatial_weight,
    spatial_bias,
    merge_weight,
    merge_scale,
    channel_gain,
    expand_weight,
    expand_scale,
    reduce_weight,
    reduce_scale,
    valw,
    dmw,
    we,
    wr,
    xbuf,
    x2buf,
    part1,
    part2,
    rel1,
    near1,
    mrg1,
    rel2,
    near2,
    mrg2,
    hbuf,
    dbuf,
    vbuf,
    gbuf,
    rbuf,
    stat,
    totals,
    small,
    swb,
    bias,
    base,
    in_sem,
    ag_send,
    ag_recv,
    rs_send,
    rs_recv,
    st_send,
    st_recv,
    sm_send,
    sm_recv,
    w_send,
    w_send_d2d,
    w_recv,
    w_recv_d2d,
):
    zh, zl, x, y, c = (lax.axis_index(name) for name in AXES)
    z = zh * 4 + zl
    fs = zl * 4 + x
    other = 1 - c
    scope = jax.named_scope

    def at_z(w):
        w = lax.rem(w, 8)
        return {"zh": lax.div(w, 4), "zl": lax.rem(w, 4)}

    xs = ({"x": lax.rem(x + 1, 4)}, {"x": lax.rem(x + 3, 4)})
    zs = (at_z(z + 1), at_z(z + 7))
    xs_far = ({"x": lax.rem(x + 2, 4)},) * 2
    zs_far = (at_z(z + 2), at_z(z + 6))
    ynext, yprev, yfar = ({"y": lax.rem(y + k, 4)} for k in (1, 3, 2))
    sib = {"c": other}

    barrier = pltpu.get_barrier_semaphore()
    for to in (*xs, xs_far[0], *zs, *zs_far, ynext, yprev, yfar, sib):
        pl.semaphore_signal(barrier, inc=1, device_id=to, device_id_type=MESH)

    inputs = [
        pltpu.make_async_copy(src, dst, in_sem.at[k])
        for k, (src, dst) in enumerate(
            (
                (tokens, xbuf.at[pl.ds(SO * R, R)]),
                (mixer_gain_hbm, mixer_gain),
                (direct_weight_hbm, direct_weight),
                (direct_scale_hbm, direct_scale),
                (value_weight_hbm, value_weight),
                (value_scale_hbm, value_scale),
                (merge_weight_hbm, merge_weight),
                (merge_scale_hbm, merge_scale),
                (channel_gain_hbm, channel_gain),
                (expand_weight_hbm, expand_weight),
                (expand_scale_hbm, expand_scale),
                (reduce_weight_hbm, reduce_weight),
                (reduce_scale_hbm, reduce_scale),
                (value_gain_hbm, value_gain),
                (value_shift_hbm, value_shift),
                (spatial_bias_hbm, spatial_bias),
                (spatial_weight_hbm, spatial_weight),
            )
        )
    ]
    for copy in inputs:
        copy.start()

    def rcopy(src, dst, ssem, rsem, to):
        return pltpu.make_async_remote_copy(
            src_ref=src, dst_ref=dst, send_sem=ssem, recv_sem=rsem, device_id=to, device_id_type=MESH
        )

    def gather_copy(buf, phase, way, k):
        if k < 4:
            src = buf.at[pl.ds(SO * R + CHUNK * k, CHUNK)]
            dst = buf.at[pl.ds((SP, SN)[way] * R + CHUNK * k, CHUNK)]
            stage = k - 2 * way if k // 2 == way else 2
        else:
            row = 64 * way + CHUNK * (k - 4)
            src = buf.at[pl.ds((SP, SN)[way] * R + row, CHUNK)]
            dst = buf.at[pl.ds(SF * R + row, CHUNK)]
            stage = 3
        return rcopy(src, dst, ag_send.at[phase], ag_recv.at[phase, stage], (ynext, yprev)[way])

    def gather_landed(buf, phase, stage, chunks):
        ref = buf.at[pl.ds(0, chunks * CHUNK)]
        rcopy(ref, ref, ag_send.at[phase], ag_recv.at[phase, stage], sib).wait_recv()

    def gather_pass_on(buf, phase, k):
        gather_landed(buf, phase, k, 2)
        for way in range(2):
            gather_copy(buf, phase, way, 4 + k).start()

    def gather_near(buf, phase):
        gather_landed(buf, phase, 2, 4)

    def gather_far(buf, phase):
        gather_landed(buf, phase, 3, 4)

    class Scatter:
        def __init__(self, stage, part, near, rel, mrg, mine):
            self.stage, self.part, self.near, self.rel, self.mrg = stage, part, near, rel, mrg
            self.mine = mine

        def copy(self, src, dst, way, k):
            return rcopy(
                src, dst, rs_send.at[self.stage], rs_recv.at[self.stage, k], (ynext, yprev)[way]
            )

        def landed(self, k, rows):
            ref = self.part.at[pl.ds(0, rows)]
            rcopy(ref, ref, rs_send.at[self.stage], rs_recv.at[self.stage, k], sib).wait_recv()

        def own(self):
            for way in range(2):
                row = 64 * (1 - way)
                src = self.part.at[pl.ds((SN, SP)[way] * R + row, 64)]
                self.copy(src, self.near.at[way, pl.ds(row, 64)], way, 0).start()

        def far(self):
            for k in range(2):
                for way in range(2):
                    row = CHUNK * k
                    src = self.part.at[pl.ds(SF * R + 64 * way + row, CHUNK)]
                    self.copy(src, self.rel.at[way, pl.ds(row, CHUNK)], way, 1 + k).start()

        def join(self, k):
            self.landed(1 + k, 2 * CHUNK)
            for way in range(2):
                row = CHUNK * k
                mine = self.part[pl.ds((SN, SP)[way] * R + 64 * way + row, CHUNK), :].astype(F32)
                came = self.rel[way, pl.ds(row, CHUNK), :].astype(F32)
                joined = self.mrg.at[way, pl.ds(row, CHUNK)]
                joined[...] = (mine + came).astype(BF16)
                self.copy(joined, self.near.at[way, pl.ds(64 * way + row, CHUNK)], way, 3 + k).start()

        def finish(self, k, done):
            if k == 0:
                self.landed(0, 128)
            self.landed(3 + k, 2 * CHUNK)
            for way in range(2):
                row = 64 * way + CHUNK * k
                total = self.mine(row) + self.near[0, pl.ds(row, CHUNK), :].astype(F32)
                done(row, total + self.near[1, pl.ds(row, CHUNK), :].astype(F32))

    mixer_sums = Scatter(
        0, part1, near1, rel1, mrg1, lambda row: part1[pl.ds(SO * R + row, CHUNK), :].astype(F32)
    )
    ff_sums = [
        Scatter(
            1 + g,
            part2.at[g],
            near2.at[g],
            rel2.at[g],
            mrg2.at[g],
            lambda row, g=g: base[g, pl.ds(row, CHUNK), :],
        )
        for g in range(2)
    ]

    def view_rows(ref, low):
        def view(pz, px, half):
            row = (pz * 4 + px) * 128 + low
            if half is None:
                return ref.at[c, pl.ds(pl.multiple_of(row, 64), 64)]
            return ref.at[c, pl.ds(pl.multiple_of(row + 32 * half, 32), 32)]

        return view

    def span_rows(ref):
        return lambda count: ref.at[c, pl.ds(0, 64 * count)]

    def view_reduce(low):
        def view(pz, px, half):
            row = c * HW + low
            if half is None:
                return wr.at[pz * 4 + px, pl.ds(pl.multiple_of(row, 256), 256)]
            return wr.at[pz * 4 + px, pl.ds(pl.multiple_of(row + 128 * half, 128), 128)]

        return view

    def span_reduce(count):
        return wr.at[pl.ds(0, count), pl.ds(0, 256)]

    def weight(index, view, span, x_first, form=Gather):
        if x_first:
            a, b, pa, pb, turned = xs, zs, x, zl, lambda p, q, h: view(q, p, h)
        else:
            a, b, pa, pb, turned = zs, xs, zl, x, view
        blocks = form(
            turned,
            span,
            a,
            b,
            pa,
            pb,
            sib,
            w_send.at[index],
            w_send_d2d.at[index],
            w_recv.at[index],
            w_recv_d2d.at[index],
        )
        blocks.far_a = xs_far if x_first else zs_far
        return blocks

    class Pair:
        def __init__(self, index, low, high, span, form=Gather):
            self.index, self.span = index, span
            self.halves = (
                weight(index, low, span, True, form),
                weight(index + 1, high, span, False, form),
            )

        def wave(self, k):
            for half in self.halves:
                getattr(half, f"wave{k}")()

        def shared(self, group):
            for half in self.halves:
                ref = self.span(8)
                rcopy(ref, ref, half.send_d2d, half.recv_d2d.at[group], sib).wait_recv()

        def sent(self):
            for half in self.halves:
                ref = self.span(15)
                rcopy(ref, ref, half.send, half.recv_d2d.at[0], sib).wait_send()
                ref = self.span(16)
                rcopy(ref, ref, half.send_d2d, half.recv_d2d.at[0], sib).wait_send()

    value_blocks = Pair(0, view_rows(valw, 0), view_rows(valw, 64), span_rows(valw), DirectGather)
    dm_blocks = Pair(2, view_rows(dmw, 0), view_rows(dmw, 64), span_rows(dmw), DirectGather)
    expand_blocks = Pair(4, view_rows(we, 0), view_rows(we, 64), span_rows(we))
    reduce_low = Pair(6, view_reduce(0), view_reduce(256), span_reduce)
    reduce_high = Pair(8, view_reduce(512), view_reduce(768), span_reduce)

    def column(row):
        return jnp.transpose(jnp.broadcast_to(row, (128, 128)))

    with scope("wait_tokens"):
        inputs[0].wait()
    with scope("wait_barrier"):
        pl.semaphore_wait(barrier, 11)

    def send_tokens():
        for k in range(4):
            for way in range(2):
                gather_copy(xbuf, 0, way, (k + 2 * way) % 4).start()

    pl.when(c == 1)(send_tokens)
    with scope("wait_mix"):
        for copy in inputs[1:8]:
            copy.wait()

    fs_row = pl.ds(pl.multiple_of(fs * 128, 128), 128)
    gain = column(mixer_gain[pl.ds(fs, 1), :])
    valw[c, fs_row, :] = (value_weight[...] * gain * value_scale[...]).astype(BF16)
    dmw[c, fs_row, 0:128] = (direct_weight[...] * gain * direct_scale[...]).astype(BF16)
    dmw[c, fs_row, 128:256] = (merge_weight[...] * merge_scale[...]).astype(BF16)
    value_blocks.wave(0)
    dm_blocks.wave(0)
    for copy in inputs[8:]:
        copy.wait()
    gain = column(channel_gain[pl.ds(fs, 1), :])
    for k in range(8):
        lanes = slice(k * 128, (k + 1) * 128)
        we[c, fs_row, lanes] = (expand_weight[:, lanes] * gain * expand_scale[:, lanes]).astype(BF16)
    for k in range(8):
        rows = pl.ds(pl.multiple_of(c * HW + k * 128, 128), 128)
        wr[fs, rows, :] = (reduce_weight[k * 128 : (k + 1) * 128, :] * reduce_scale[...]).astype(BF16)
    small[c, 0:1, :] = value_gain[...]
    small[c, 1:2, :] = value_shift[...]
    small[c, 2:4, :] = spatial_bias[...]
    small[c, 4:8, :] = jnp.zeros((4, 128), F32)
    swb[c] = spatial_weight[...]
    small_copy = rcopy(small.at[c], small.at[c], sm_send.at[0], sm_recv.at[0], sib)
    spatial_copy = rcopy(spatial_weight, swb.at[c], sm_send.at[1], sm_recv.at[1], sib)
    small_copy.start()
    spatial_copy.start()

    def row_scales(buf, start, count):
        @pl.loop(0, count // 32)
        def _(i):
            rows = pl.ds(pl.multiple_of(start + i * 32, 32), 32)
            floats = buf[rows, :].astype(F32)
            power = jnp.mean(floats * floats, axis=-1, keepdims=True)
            rbuf[rows, :] = jnp.broadcast_to(lax.rsqrt(power + EPS), (32, 128))

    lane = lax.broadcasted_iota(jnp.int32, (128, 128), 1)
    block_of = {SP: lax.rem(y + 3, 4), SN: lax.rem(y + 1, 4), SF: lax.rem(y + 2, 4), SO: y}

    def project(slots):
        start, count = slots[0] * R, len(slots) * R
        rows = pl.ds(start, count)
        weights = jnp.concatenate([valw[0], valw[1]], axis=1)
        value = jnp.dot(xbuf[rows, :], weights, preferred_element_type=F32)
        scale = rbuf[rows, :]
        vbuf[rows, :] = gelu(value * jnp.concatenate([scale, scale], axis=1))
        for slot in slots:
            v = vbuf[pl.ds(slot * R, R), :]
            total = jnp.sum(v, axis=1, keepdims=True)
            squares = jnp.sum(v * v, axis=1, keepdims=True)
            tile = jnp.where(lane == 0, total, jnp.where(lane == 1, squares, 0.0))
            sums = jnp.transpose(tile)
            stat[0, pl.ds(block_of[slot], 1), :] = sums[0:1, :]
            stat[0, pl.ds(4 + block_of[slot], 1), :] = sums[1:2, :]

    def project_direct(start):
        weights = jnp.concatenate([dmw[0, :, 0:128], dmw[1, :, 0:128]], axis=1)
        rows = pl.ds(start, 256)
        direct = jnp.dot(xbuf[rows, :], weights, preferred_element_type=F32)
        scale = rbuf[rows, :]
        dbuf[rows, :] = gelu(direct * jnp.concatenate([scale, scale], axis=1))

    def mixing(slots):
        for slot in slots:
            rows = pl.ds(slot * R, R)
            block = block_of[slot]
            mean = column(totals[pl.ds(block, 1), :]) / BRANCH
            var = column(totals[pl.ds(4 + block, 1), :]) / BRANCH - mean * mean
            inv = lax.rsqrt(var + EPS)
            for k in range(2):
                lanes = slice(k * 128, (k + 1) * 128)
                v = vbuf[rows, lanes]
                g = ((v - mean) * inv * small[k, 0:1, :] + small[k, 1:2, :]).astype(BF16)
                low = jnp.dot(swb[k, 0], g, preferred_element_type=F32)
                high = jnp.dot(swb[k, 1], g, preferred_element_type=F32)
                mixed = jnp.where(lane < 64, low, high) + bias[k]
                gbuf[rows, lanes] = (dbuf[rows, lanes] * mixed).astype(BF16)
        rows = pl.ds(slots[0] * R, len(slots) * R)

        @pl.loop(0, 2)
        def _(j):
            weights = jnp.concatenate(
                [
                    jnp.concatenate(
                        [
                            dmw[k, pl.ds(pl.multiple_of(j * 1024 + i * 128, 128), 128), 128:256]
                            for i in range(8)
                        ],
                        axis=1,
                    )
                    for k in range(2)
                ],
                axis=0,
            )
            product = jnp.dot(gbuf[rows, :], weights, preferred_element_type=F32)
            part1[rows, pl.ds(pl.multiple_of(j * 1024, 1024), 1024)] = product.astype(BF16)

    def gathered_rows(ref, pieces):
        loaded = [ref[pl.ds(start, count), :] for start, count in pieces]
        return loaded[0] if len(loaded) == 1 else jnp.concatenate(loaded, axis=0)

    def store_rows(ref, pieces, cols, values):
        at = 0
        for start, count in pieces:
            ref[pl.ds(start, count), cols] = values[at : at + count, :]
            at += count

    def feed_up(pieces):
        for start, count in pieces:
            row_scales(x2buf, start, count)

        @pl.loop(0, 2)
        def _(j):
            upper = jnp.dot(gathered_rows(x2buf, pieces), we[j], preferred_element_type=F32)
            upper = upper * jnp.concatenate([gathered_rows(rbuf, pieces)] * 8, axis=1)
            hidden = jnp.square(jnp.maximum(upper, 0.0)).astype(BF16)
            store_rows(hbuf, pieces, pl.ds(pl.multiple_of(j * HW, HW), HW), hidden)

    def shard_of(dx, dz):
        return lax.rem(zl + 4 - dz, 4) * 4 + lax.rem(x + 4 - dx, 4)

    columns = [[shard_of(*offsets) for offsets in group] for group in (FIRST, LAST)]

    def feed_down(pieces, g):
        weights = jnp.concatenate([wr[shard] for shard in columns[g]], axis=1)
        product = jnp.dot(gathered_rows(hbuf, pieces), weights, preferred_element_type=F32)
        store_rows(part2.at[g], pieces, slice(None), product.astype(BF16))

    def feed_own(g):
        weights = jnp.concatenate([wr[shard] for shard in columns[g]], axis=1)
        rows = pl.ds(SO * R, R)
        middle = [x2buf[rows, pl.ds(pl.multiple_of(shard * 128, 128), 128)] for shard in columns[g]]
        product = jnp.dot(hbuf[rows, :], weights, preferred_element_type=F32)
        base[g] = jnp.concatenate(middle, axis=1).astype(F32) + product.astype(BF16).astype(F32)

    row_scales(xbuf, SO * R, R)
    with scope("v_w1"):
        value_blocks.wave(1)
    with scope("dm_w1"):
        dm_blocks.wave(1)
    pl.when(c == 0)(send_tokens)

    @pl.when(c == 1)
    def _():
        gather_pass_on(xbuf, 0, 0)
        gather_pass_on(xbuf, 0, 1)

    with scope("v_w2"):
        value_blocks.wave(2)

    with scope("dm_w2"):
        dm_blocks.wave(2)
    expand_blocks.wave(0)

    @pl.when(c == 1)
    def _():
        with scope("scales_1"):
            gather_near(xbuf, 0)
            row_scales(xbuf, 0, 2 * R)

    @pl.when(c == 0)
    def _():
        with scope("pass1_0"):
            gather_pass_on(xbuf, 0, 0)

    reduce_low.wave(0)
    with scope("v_w3"):
        value_blocks.wave(3)

    @pl.when(c == 1)
    def _():
        gather_far(xbuf, 0)
        row_scales(xbuf, 2 * R, R)

    @pl.when(c == 0)
    def _():
        with scope("pass1_1"):
            gather_pass_on(xbuf, 0, 1)

    with scope("v_d2d"):
        value_blocks.shared(0)
        value_blocks.shared(1)
    with scope("project_own"):
        project((SO,))

    @pl.when(c == 1)
    def _():
        project((SN, SP))

    with scope("dm_w3"):
        dm_blocks.wave(3)

    @pl.when(c == 0)
    def _():
        with scope("scales_0"):
            gather_near(xbuf, 0)
            row_scales(xbuf, 0, 2 * R)
        with scope("project_near"):
            project((SN, SP))
        with scope("far1"):
            gather_far(xbuf, 0)
            row_scales(xbuf, 2 * R, R)

    with scope("project_far"):
        project((SF,))
    stat_copies = [
        rcopy(stat.at[0], stat.at[k + 1], st_send.at[0], st_recv.at[0], to)
        for k, to in enumerate((ynext, yprev, yfar))
    ]
    for copy in stat_copies:
        copy.start()

    @pl.when(c == 0)
    def _():
        with scope("e_w1_0"):
            expand_blocks.wave(1)

    reduce_high.wave(0)
    with scope("dm_d2d"):
        dm_blocks.shared(0)
        dm_blocks.shared(1)
    with scope("direct"):
        project_direct(0)
        rcopy(small.at[other], small.at[other], sm_send.at[0], sm_recv.at[0], sib).wait_recv()
        rcopy(swb.at[other], swb.at[other], sm_send.at[1], sm_recv.at[1], sib).wait_recv()
        for k in range(2):
            rows = jnp.concatenate(
                [jnp.broadcast_to(small[k, 2 + g : 3 + g, :], (64, 128)) for g in range(2)], axis=0
            )
            bias[k] = jnp.transpose(rows)

    @pl.when(c == 1)
    def _():
        with scope("e_w1_1"):
            expand_blocks.wave(1)

    with scope("wait_stats"):
        all_stats = stat.at[pl.ds(1, 3)]
        rcopy(all_stats, all_stats, st_send.at[0], st_recv.at[0], sib).wait_recv()
        totals[...] = stat[0] + stat[1] + stat[2] + stat[3]
    with scope("mixing_near"):
        mixing((SN, SP))
    mixer_sums.own()
    project_direct(256)
    with scope("mixing_far"):
        mixing((SF,))
    mixer_sums.far()
    with scope("mixing_own"):
        mixing((SO,))

    @pl.when(c == 1)
    def _():
        with scope("join1_0_1"):
            mixer_sums.join(0)

    with scope("e_w2"):
        expand_blocks.wave(2)
    with scope("r0_w1"):
        reduce_low.wave(1)

    @pl.when(c == 0)
    def _():
        with scope("join1_0_0"):
            mixer_sums.join(0)

    with scope("join1_1"):
        mixer_sums.join(1)
    with scope("e_w3"):
        expand_blocks.wave(3)
    with scope("r1_w1"):
        reduce_high.wave(1)

    def middle_done(row, total):
        rows = pl.ds(SO * R + row, CHUNK)
        x2buf[rows, :] = (xbuf[rows, :].astype(F32) + total).astype(BF16)

    with scope("finish1_0"):
        mixer_sums.finish(0, middle_done)
    for way in range(2):
        gather_copy(x2buf, 1, way, 2 * way).start()
    with scope("finish1_1"):
        mixer_sums.finish(1, middle_done)
    for way in range(2):
        gather_copy(x2buf, 1, way, 2 * way + 1).start()
    with scope("r0_w2"):
        reduce_low.wave(2)
    with scope("e_w4"):
        expand_blocks.wave(4)
    with scope("pass2_0"):
        gather_pass_on(x2buf, 1, 0)
    with scope("r1_w2"):
        reduce_high.wave(2)
    with scope("pass2_1"):
        gather_pass_on(x2buf, 1, 1)
    for k in range(2):
        for way in range(2):
            gather_copy(x2buf, 1, way, 2 * (1 - way) + k).start()

    outer, inner = ((64, 128),), ((0, 64), (192, 64))
    far, own = ((SF * R, R),), ((SO * R, R),)
    with scope("e_d2d"):
        expand_blocks.shared(0)
        expand_blocks.shared(1)
    with scope("up_outer"):
        feed_up(outer)
    with scope("r0_w3"):
        reduce_low.wave(3)
    with scope("r_d2d_0"):
        reduce_low.shared(0)
        reduce_high.shared(0)
    with scope("down_outer_0"):
        feed_down(outer, 0)
    ff_sums[0].own()
    with scope("r1_w3"):
        reduce_high.wave(3)
    with scope("up_own"):
        feed_up(own)
    with scope("far2"):
        gather_far(x2buf, 1)
    with scope("r0_w4"):
        reduce_low.wave(4)
    with scope("r1_w4"):
        reduce_high.wave(4)
    with scope("feed_far_0"):
        feed_up(far)
        feed_down(far, 0)
    ff_sums[0].far()
    with scope("down_own_0"):
        feed_own(0)
    with scope("r_d2d_1"):
        reduce_low.shared(1)
        reduce_high.shared(1)
    with scope("down_outer_1"):
        feed_down(outer, 1)
    ff_sums[1].own()
    with scope("down_far_1"):
        feed_down(far, 1)
    ff_sums[1].far()
    with scope("near2"):
        gather_near(x2buf, 1)
    with scope("feed_inner_0"):
        feed_up(inner)
        feed_down(inner, 0)
    with scope("join2_0"):
        ff_sums[0].join(0)
        ff_sums[0].join(1)
    with scope("feed_inner_1"):
        feed_down(inner, 1)
    with scope("join2_1_0"):
        ff_sums[1].join(0)
    with scope("join2_1_1"):
        ff_sums[1].join(1)
    with scope("down_own_1"):
        feed_own(1)

    def result_done(g):
        def done(row, total):
            total = total.astype(BF16)
            for p, shard in enumerate(columns[g]):
                lanes = pl.ds(pl.multiple_of(shard * 128, 128), 128)
                out[pl.ds(row, CHUNK), lanes] = total[:, p * 128 : (p + 1) * 128]

        return done

    for g in range(2):
        for k in range(2):
            with scope(f"finish2_{g}_{k}"):
                ff_sums[g].finish(k, result_done(g))

    with scope("drain"):
        for phase, buf in ((0, xbuf), (1, x2buf)):
            ref = buf.at[pl.ds(0, 12 * CHUNK)]
            rcopy(ref, ref, ag_send.at[phase], ag_recv.at[phase, 0], sib).wait_send()
        for sums in (mixer_sums, *ff_sums):
            ref = sums.part.at[pl.ds(0, 12 * CHUNK)]
            rcopy(ref, ref, rs_send.at[sums.stage], rs_recv.at[sums.stage, 0], sib).wait_send()
        rcopy(all_stats, all_stats, st_send.at[0], st_recv.at[0], sib).wait_send()
        for copy in (small_copy, spatial_copy):
            copy.wait_send()
        for blocks in (value_blocks, dm_blocks, expand_blocks, reduce_low, reduce_high):
            blocks.sent()


def layer(*args):
    (
        tokens,
        mixer_gain,
        direct_weight,
        direct_scale,
        value_weight,
        value_scale,
        value_gain,
        value_shift,
        spatial_weight,
        spatial_bias,
        merge_weight,
        merge_scale,
        channel_gain,
        expand_weight,
        expand_scale,
        reduce_weight,
        reduce_scale,
    ) = args
    operands = (
        tokens,
        mixer_gain.reshape(16, 128),
        direct_weight,
        direct_scale.reshape(1, CW),
        value_weight,
        value_scale.reshape(1, CW),
        value_gain.reshape(1, CW),
        value_shift.reshape(1, CW),
        spatial_weight,
        spatial_bias,
        merge_weight,
        merge_scale.reshape(1, 128),
        channel_gain.reshape(16, 128),
        expand_weight,
        expand_scale.reshape(1, HW),
        reduce_weight,
        reduce_scale.reshape(1, 128),
    )
    dma = pltpu.SemaphoreType.DMA
    return pl.pallas_call(
        kernel,
        out_shape=jax.ShapeDtypeStruct((R, D), BF16),
        in_specs=[pl.BlockSpec(memory_space=pl.ANY)] * 17,
        out_specs=pl.BlockSpec(memory_space=pltpu.VMEM),
        scratch_shapes=[
            *(pltpu.VMEM(operand.shape, operand.dtype) for operand in operands[1:]),
            pltpu.VMEM((2, D, 128), BF16),
            pltpu.VMEM((2, D, 256), BF16),
            pltpu.VMEM((2, D, HW), BF16),
            pltpu.VMEM((16, 2 * HW, 128), BF16),
            pltpu.VMEM((4 * R, D), BF16),
            pltpu.VMEM((4 * R, D), BF16),
            pltpu.VMEM((4 * R, D), BF16),
            pltpu.VMEM((2, 4 * R, D // 2), BF16),
            pltpu.VMEM((2, 64, D), BF16),
            pltpu.VMEM((2, R, D), BF16),
            pltpu.VMEM((2, 64, D), BF16),
            pltpu.VMEM((2, 2, 64, D // 2), BF16),
            pltpu.VMEM((2, 2, R, D // 2), BF16),
            pltpu.VMEM((2, 2, 64, D // 2), BF16),
            pltpu.VMEM((4 * R, D), BF16),
            pltpu.VMEM((4 * R, 256), F32),
            pltpu.VMEM((4 * R, 256), F32),
            pltpu.VMEM((4 * R, 256), BF16),
            pltpu.VMEM((4 * R, 128), F32),
            pltpu.VMEM((4, 8, 128), F32),
            pltpu.VMEM((8, 128), F32),
            pltpu.VMEM((2, 8, 128), F32),
            pltpu.VMEM((2, 2, 128, 128), BF16),
            pltpu.VMEM((2, 128, 128), F32),
            pltpu.VMEM((2, R, D // 2), F32),
            dma((17,)),
            dma((2,)),
            dma((2, 4)),
            dma((3,)),
            dma((3, 5)),
            dma((1,)),
            dma((1,)),
            dma((2,)),
            dma((2,)),
            dma((10,)),
            dma((10,)),
            dma((10, 8)),
            dma((10, 2)),
        ],
        compiler_params=pltpu.CompilerParams(
            collective_id=0, has_side_effects=True, vmem_limit_bytes=52 * 1024 * 1024
        ),
        name="layer",
    )(*(pltpu.with_memory_space_constraint(operand, pltpu.HBM) for operand in operands))


def solution(mesh):
    finer = Mesh(mesh.devices.reshape(2, 4, 4, 4, 2), AXES)
    in_specs = (
        P(AXES, None),
        P(),
        P(FS, TP),
        P(TP),
        P(FS, TP),
        P(TP),
        P(TP),
        P(TP),
        P(TP, None, None),
        P(TP, None),
        P(TP, FS),
        P(FS),
        P(),
        P(FS, TP),
        P(TP),
        P(TP, FS),
        P(FS),
    )
    return jax.shard_map(layer, mesh=finer, in_specs=in_specs, out_specs=P(AXES, None), check_vma=False)
```

```python
import functools

import jax
import jax.numpy as jnp
from jax import lax
from jax.experimental import pallas as pl
from jax.experimental.pallas import tpu as pltpu
from jax.sharding import Mesh
from jax.sharding import PartitionSpec as P

AXES = ("zh", "zl", "x", "y", "c")
FS = ("zl", "x")
TP = ("y", "c")
EPS = 1e-6
MESH = pl.DeviceIdType.MESH
F32 = jnp.float32
BF16 = jnp.bfloat16

D = 2048
R = 128
CW = 128
HW = 1024
BRANCH = 1024
SN, SP, SF, SO = 0, 1, 2, 3
CHUNK = 32


def gelu(u):
    return jax.nn.gelu(u, approximate=True)


FIRST = ((0, 0), (1, 0), (3, 0), (0, 1), (0, 3), (1, 1), (1, 3), (3, 1))
LAST = ((3, 3), (2, 0), (0, 2), (2, 1), (2, 3), (1, 2), (3, 2), (2, 2))


class Gather:
    def __init__(self, view, span, a, b, pa, pb, sib, send, send_d2d, recv, recv_d2d):
        self.view, self.span = view, span
        self.a, self.b, self.pa, self.pb, self.sib = a, b, pa, pb, sib
        self.send, self.send_d2d, self.recv, self.recv_d2d = send, send_d2d, recv, recv_d2d

    def item(self, da, db, half=None):
        return self.view(lax.rem(self.pa + 4 - da, 4), lax.rem(self.pb + 4 - db, 4), half)

    def copy(self, ref, stage, to):
        return pltpu.make_async_remote_copy(
            src_ref=ref,
            dst_ref=ref,
            send_sem=self.send,
            recv_sem=self.recv.at[stage],
            device_id=to,
            device_id_type=MESH,
        )

    def landed(self, stage, count):
        self.copy(self.span(count), stage, self.sib).wait_recv()

    def along_b(self, da, stage):
        for k in range(2):
            self.copy(self.item(da, 0), stage, self.b[k]).start()

    def across(self, da, db):
        ref = self.item(da, db)
        pltpu.make_async_remote_copy(
            src_ref=ref,
            dst_ref=ref,
            send_sem=self.send_d2d,
            recv_sem=self.recv_d2d.at[0 if (da, db) in FIRST else 1],
            device_id=self.sib,
            device_id_type=MESH,
        ).start()

    def on_b(self, da, stage):
        for k in range(2):
            db = (1, 3)[k]
            self.copy(self.item(da, db, k), stage, self.b[k]).start()
            self.across(da, db)

    def wave0(self):
        for k in range(2):
            self.copy(self.item(0, 0), 0, self.a[k]).start()
        self.along_b(0, 1)
        self.across(0, 0)

    def wave1(self):
        self.landed(0, 2)
        for k in range(2):
            da = (1, 3)[k]
            self.copy(self.item(da, 0, k), 2, self.a[k]).start()
            self.along_b(da, 3)
            self.across(da, 0)
        self.landed(1, 2)
        self.on_b(0, 4)

    def wave2(self):
        self.landed(2, 1)
        self.along_b(2, 5)
        self.across(2, 0)
        self.landed(3, 4)
        self.on_b(1, 6)
        self.on_b(3, 6)
        self.landed(4, 1)
        self.across(0, 2)

    def wave3(self):
        self.landed(5, 2)
        self.on_b(2, 7)
        self.landed(6, 2)
        self.across(1, 2)
        self.across(3, 2)

    def wave4(self):
        self.landed(7, 1)
        self.across(2, 2)


class DirectGather(Gather):
    def wave0(self):
        for k in range(2):
            self.copy(self.item(0, 0), 0, self.a[k]).start()
        for k in range(2):
            self.copy(self.item(0, 0, k), 0, self.far_a[k]).start()
        self.along_b(0, 1)
        self.across(0, 0)

    def wave1(self):
        self.landed(0, 3)
        for da in (1, 3, 2):
            self.along_b(da, 2)
        self.landed(1, 2)
        self.on_b(0, 3)
        for da in (1, 3, 2):
            self.across(da, 0)

    def wave2(self):
        self.landed(2, 6)
        for da in (1, 3, 2):
            self.on_b(da, 4)
        self.landed(3, 1)
        self.across(0, 2)

    def wave3(self):
        self.landed(4, 3)
        for da in (1, 3, 2):
            self.across(da, 2)


def kernel(
    tokens,
    mixer_gain_hbm,
    direct_weight_hbm,
    direct_scale_hbm,
    value_weight_hbm,
    value_scale_hbm,
    value_gain_hbm,
    value_shift_hbm,
    spatial_weight_hbm,
    spatial_bias_hbm,
    merge_weight_hbm,
    merge_scale_hbm,
    channel_gain_hbm,
    expand_weight_hbm,
    expand_scale_hbm,
    reduce_weight_hbm,
    reduce_scale_hbm,
    out,
    mixer_gain,
    direct_weight,
    direct_scale,
    value_weight,
    value_scale,
    value_gain,
    value_shift,
    spatial_weight,
    spatial_bias,
    merge_weight,
    merge_scale,
    channel_gain,
    expand_weight,
    expand_scale,
    reduce_weight,
    reduce_scale,
    valw,
    dmw,
    we,
    wr,
    xbuf,
    x2buf,
    part1,
    part2,
    rel1,
    near1,
    mrg1,
    rel2,
    near2,
    mrg2,
    hbuf,
    dbuf,
    vbuf,
    gbuf,
    rbuf,
    stat,
    totals,
    small,
    swb,
    bias,
    base,
    in_sem,
    ag_send,
    ag_recv,
    rs_send,
    rs_recv,
    st_send,
    st_recv,
    sm_send,
    sm_recv,
    w_send,
    w_send_d2d,
    w_recv,
    w_recv_d2d,
):
    zh, zl, x, y, c = (lax.axis_index(name) for name in AXES)
    z = zh * 4 + zl
    fs = zl * 4 + x
    other = 1 - c
    scope = jax.named_scope

    def at_z(w):
        w = lax.rem(w, 8)
        return {"zh": lax.div(w, 4), "zl": lax.rem(w, 4)}

    xs = ({"x": lax.rem(x + 1, 4)}, {"x": lax.rem(x + 3, 4)})
    zs = (at_z(z + 1), at_z(z + 7))
    xs_far = ({"x": lax.rem(x + 2, 4)},) * 2
    zs_far = (at_z(z + 2), at_z(z + 6))
    ynext, yprev, yfar = ({"y": lax.rem(y + k, 4)} for k in (1, 3, 2))
    sib = {"c": other}

    barrier = pltpu.get_barrier_semaphore()
    for to in (*xs, xs_far[0], *zs, *zs_far, ynext, yprev, yfar, sib):
        pl.semaphore_signal(barrier, inc=1, device_id=to, device_id_type=MESH)

    inputs = [
        pltpu.make_async_copy(src, dst, in_sem.at[k])
        for k, (src, dst) in enumerate(
            (
                (tokens, xbuf.at[pl.ds(SO * R, R)]),
                (mixer_gain_hbm, mixer_gain),
                (direct_weight_hbm, direct_weight),
                (direct_scale_hbm, direct_scale),
                (value_weight_hbm, value_weight),
                (value_scale_hbm, value_scale),
                (merge_weight_hbm, merge_weight),
                (merge_scale_hbm, merge_scale),
                (channel_gain_hbm, channel_gain),
                (expand_weight_hbm, expand_weight),
                (expand_scale_hbm, expand_scale),
                (reduce_weight_hbm, reduce_weight),
                (reduce_scale_hbm, reduce_scale),
                (value_gain_hbm, value_gain),
                (value_shift_hbm, value_shift),
                (spatial_bias_hbm, spatial_bias),
                (spatial_weight_hbm, spatial_weight),
            )
        )
    ]
    for copy in inputs:
        copy.start()

    def rcopy(src, dst, ssem, rsem, to):
        return pltpu.make_async_remote_copy(
            src_ref=src, dst_ref=dst, send_sem=ssem, recv_sem=rsem, device_id=to, device_id_type=MESH
        )

    def gather_copy(buf, phase, way, k):
        if k < 4:
            src = buf.at[pl.ds(SO * R + CHUNK * k, CHUNK)]
            dst = buf.at[pl.ds((SP, SN)[way] * R + CHUNK * k, CHUNK)]
            stage = k - 2 * way if k // 2 == way else 2
        else:
            row = 64 * way + CHUNK * (k - 4)
            src = buf.at[pl.ds((SP, SN)[way] * R + row, CHUNK)]
            dst = buf.at[pl.ds(SF * R + row, CHUNK)]
            stage = 3
        return rcopy(src, dst, ag_send.at[phase], ag_recv.at[phase, stage], (ynext, yprev)[way])

    def gather_landed(buf, phase, stage, chunks):
        ref = buf.at[pl.ds(0, chunks * CHUNK)]
        rcopy(ref, ref, ag_send.at[phase], ag_recv.at[phase, stage], sib).wait_recv()

    def gather_pass_on(buf, phase, k):
        gather_landed(buf, phase, k, 2)
        for way in range(2):
            gather_copy(buf, phase, way, 4 + k).start()

    def gather_near(buf, phase):
        gather_landed(buf, phase, 2, 4)

    def gather_far(buf, phase):
        gather_landed(buf, phase, 3, 4)

    class Scatter:
        def __init__(self, stage, part, near, rel, mrg, mine):
            self.stage, self.part, self.near, self.rel, self.mrg = stage, part, near, rel, mrg
            self.mine = mine

        def copy(self, src, dst, way, k):
            return rcopy(
                src, dst, rs_send.at[self.stage], rs_recv.at[self.stage, k], (ynext, yprev)[way]
            )

        def landed(self, k, rows):
            ref = self.part.at[pl.ds(0, rows)]
            rcopy(ref, ref, rs_send.at[self.stage], rs_recv.at[self.stage, k], sib).wait_recv()

        def own(self):
            for way in range(2):
                row = 64 * (1 - way)
                src = self.part.at[pl.ds((SN, SP)[way] * R + row, 64)]
                self.copy(src, self.near.at[way, pl.ds(row, 64)], way, 0).start()

        def far(self):
            for k in range(2):
                for way in range(2):
                    row = CHUNK * k
                    src = self.part.at[pl.ds(SF * R + 64 * way + row, CHUNK)]
                    self.copy(src, self.rel.at[way, pl.ds(row, CHUNK)], way, 1 + k).start()

        def join(self, k):
            self.landed(1 + k, 2 * CHUNK)
            for way in range(2):
                row = CHUNK * k
                mine = self.part[pl.ds((SN, SP)[way] * R + 64 * way + row, CHUNK), :].astype(F32)
                came = self.rel[way, pl.ds(row, CHUNK), :].astype(F32)
                joined = self.mrg.at[way, pl.ds(row, CHUNK)]
                joined[...] = (mine + came).astype(BF16)
                self.copy(joined, self.near.at[way, pl.ds(64 * way + row, CHUNK)], way, 3 + k).start()

        def finish(self, k, done):
            if k == 0:
                self.landed(0, 128)
            self.landed(3 + k, 2 * CHUNK)
            for way in range(2):
                row = 64 * way + CHUNK * k
                total = self.mine(row) + self.near[0, pl.ds(row, CHUNK), :].astype(F32)
                done(row, total + self.near[1, pl.ds(row, CHUNK), :].astype(F32))

    mixer_sums = Scatter(
        0, part1, near1, rel1, mrg1, lambda row: part1[pl.ds(SO * R + row, CHUNK), :].astype(F32)
    )
    ff_sums = [
        Scatter(
            1 + g,
            part2.at[g],
            near2.at[g],
            rel2.at[g],
            mrg2.at[g],
            lambda row, g=g: base[g, pl.ds(row, CHUNK), :],
        )
        for g in range(2)
    ]

    def view_rows(ref, low):
        def view(pz, px, half):
            row = (pz * 4 + px) * 128 + low
            if half is None:
                return ref.at[c, pl.ds(pl.multiple_of(row, 64), 64)]
            return ref.at[c, pl.ds(pl.multiple_of(row + 32 * half, 32), 32)]

        return view

    def span_rows(ref):
        return lambda count: ref.at[c, pl.ds(0, 64 * count)]

    def view_reduce(low):
        def view(pz, px, half):
            row = c * HW + low
            if half is None:
                return wr.at[pz * 4 + px, pl.ds(pl.multiple_of(row, 256), 256)]
            return wr.at[pz * 4 + px, pl.ds(pl.multiple_of(row + 128 * half, 128), 128)]

        return view

    def span_reduce(count):
        return wr.at[pl.ds(0, count), pl.ds(0, 256)]

    def weight(index, view, span, x_first, form=Gather):
        if x_first:
            a, b, pa, pb, turned = xs, zs, x, zl, lambda p, q, h: view(q, p, h)
        else:
            a, b, pa, pb, turned = zs, xs, zl, x, view
        blocks = form(
            turned,
            span,
            a,
            b,
            pa,
            pb,
            sib,
            w_send.at[index],
            w_send_d2d.at[index],
            w_recv.at[index],
            w_recv_d2d.at[index],
        )
        blocks.far_a = xs_far if x_first else zs_far
        return blocks

    class Pair:
        def __init__(self, index, low, high, span, form=Gather):
            self.index, self.span = index, span
            self.halves = (
                weight(index, low, span, True, form),
                weight(index + 1, high, span, False, form),
            )

        def wave(self, k):
            for half in self.halves:
                getattr(half, f"wave{k}")()

        def shared(self, group):
            for half in self.halves:
                ref = self.span(8)
                rcopy(ref, ref, half.send_d2d, half.recv_d2d.at[group], sib).wait_recv()

        def sent(self):
            for half in self.halves:
                ref = self.span(15)
                rcopy(ref, ref, half.send, half.recv_d2d.at[0], sib).wait_send()
                ref = self.span(16)
                rcopy(ref, ref, half.send_d2d, half.recv_d2d.at[0], sib).wait_send()

    value_blocks = Pair(0, view_rows(valw, 0), view_rows(valw, 64), span_rows(valw), DirectGather)
    dm_blocks = Pair(2, view_rows(dmw, 0), view_rows(dmw, 64), span_rows(dmw), DirectGather)
    expand_blocks = Pair(4, view_rows(we, 0), view_rows(we, 64), span_rows(we))
    reduce_low = Pair(6, view_reduce(0), view_reduce(256), span_reduce)
    reduce_high = Pair(8, view_reduce(512), view_reduce(768), span_reduce)

    def column(row):
        return jnp.transpose(jnp.broadcast_to(row, (128, 128)))

    with scope("wait_tokens"):
        inputs[0].wait()
    with scope("wait_barrier"):
        pl.semaphore_wait(barrier, 11)

    def send_tokens():
        for k in range(4):
            for way in range(2):
                gather_copy(xbuf, 0, way, (k + 2 * way) % 4).start()

    pl.when(c == 1)(send_tokens)
    with scope("wait_mix"):
        for copy in inputs[1:8]:
            copy.wait()

    fs_row = pl.ds(pl.multiple_of(fs * 128, 128), 128)
    gain = column(mixer_gain[pl.ds(fs, 1), :])
    valw[c, fs_row, :] = (value_weight[...] * gain * value_scale[...]).astype(BF16)
    dmw[c, fs_row, 0:128] = (direct_weight[...] * gain * direct_scale[...]).astype(BF16)
    dmw[c, fs_row, 128:256] = (merge_weight[...] * merge_scale[...]).astype(BF16)
    value_blocks.wave(0)
    dm_blocks.wave(0)
    for copy in inputs[8:]:
        copy.wait()
    gain = column(channel_gain[pl.ds(fs, 1), :])
    for k in range(8):
        lanes = slice(k * 128, (k + 1) * 128)
        we[c, fs_row, lanes] = (expand_weight[:, lanes] * gain * expand_scale[:, lanes]).astype(BF16)
    for k in range(8):
        rows = pl.ds(pl.multiple_of(c * HW + k * 128, 128), 128)
        wr[fs, rows, :] = (reduce_weight[k * 128 : (k + 1) * 128, :] * reduce_scale[...]).astype(BF16)
    small[c, 0:1, :] = value_gain[...]
    small[c, 1:2, :] = value_shift[...]
    small[c, 2:4, :] = spatial_bias[...]
    small[c, 4:8, :] = jnp.zeros((4, 128), F32)
    swb[c] = spatial_weight[...]
    small_copy = rcopy(small.at[c], small.at[c], sm_send.at[0], sm_recv.at[0], sib)
    spatial_copy = rcopy(spatial_weight, swb.at[c], sm_send.at[1], sm_recv.at[1], sib)
    small_copy.start()
    spatial_copy.start()

    def row_scales(buf, start, count):
        @pl.loop(0, count // 32)
        def _(i):
            rows = pl.ds(pl.multiple_of(start + i * 32, 32), 32)
            floats = buf[rows, :].astype(F32)
            power = jnp.mean(floats * floats, axis=-1, keepdims=True)
            rbuf[rows, :] = jnp.broadcast_to(lax.rsqrt(power + EPS), (32, 128))

    lane = lax.broadcasted_iota(jnp.int32, (128, 128), 1)
    block_of = {SP: lax.rem(y + 3, 4), SN: lax.rem(y + 1, 4), SF: lax.rem(y + 2, 4), SO: y}

    def project(slots):
        start, count = slots[0] * R, len(slots) * R
        rows = pl.ds(start, count)
        weights = jnp.concatenate([valw[0], valw[1]], axis=1)
        value = jnp.dot(xbuf[rows, :], weights, preferred_element_type=F32)
        scale = rbuf[rows, :]
        vbuf[rows, :] = gelu(value * jnp.concatenate([scale, scale], axis=1))
        for slot in slots:
            v = vbuf[pl.ds(slot * R, R), :]
            total = jnp.sum(v, axis=1, keepdims=True)
            squares = jnp.sum(v * v, axis=1, keepdims=True)
            tile = jnp.where(lane == 0, total, jnp.where(lane == 1, squares, 0.0))
            sums = jnp.transpose(tile)
            stat[0, pl.ds(block_of[slot], 1), :] = sums[0:1, :]
            stat[0, pl.ds(4 + block_of[slot], 1), :] = sums[1:2, :]

    def project_direct(start):
        weights = jnp.concatenate([dmw[0, :, 0:128], dmw[1, :, 0:128]], axis=1)
        rows = pl.ds(start, 256)
        direct = jnp.dot(xbuf[rows, :], weights, preferred_element_type=F32)
        scale = rbuf[rows, :]
        dbuf[rows, :] = gelu(direct * jnp.concatenate([scale, scale], axis=1))

    def mixing(slots):
        for slot in slots:
            rows = pl.ds(slot * R, R)
            block = block_of[slot]
            mean = column(totals[pl.ds(block, 1), :]) / BRANCH
            var = column(totals[pl.ds(4 + block, 1), :]) / BRANCH - mean * mean
            inv = lax.rsqrt(var + EPS)
            for k in range(2):
                lanes = slice(k * 128, (k + 1) * 128)
                v = vbuf[rows, lanes]
                g = ((v - mean) * inv * small[k, 0:1, :] + small[k, 1:2, :]).astype(BF16)
                low = jnp.dot(swb[k, 0], g, preferred_element_type=F32)
                high = jnp.dot(swb[k, 1], g, preferred_element_type=F32)
                mixed = jnp.where(lane < 64, low, high) + bias[k]
                gbuf[rows, lanes] = (dbuf[rows, lanes] * mixed).astype(BF16)
        rows = pl.ds(slots[0] * R, len(slots) * R)

        @pl.loop(0, 2)
        def _(j):
            weights = jnp.concatenate(
                [
                    jnp.concatenate(
                        [
                            dmw[k, pl.ds(pl.multiple_of(j * 1024 + i * 128, 128), 128), 128:256]
                            for i in range(8)
                        ],
                        axis=1,
                    )
                    for k in range(2)
                ],
                axis=0,
            )
            product = jnp.dot(gbuf[rows, :], weights, preferred_element_type=F32)
            part1[rows, pl.ds(pl.multiple_of(j * 1024, 1024), 1024)] = product.astype(BF16)

    def gathered_rows(ref, pieces):
        loaded = [ref[pl.ds(start, count), :] for start, count in pieces]
        return loaded[0] if len(loaded) == 1 else jnp.concatenate(loaded, axis=0)

    def store_rows(ref, pieces, cols, values):
        at = 0
        for start, count in pieces:
            ref[pl.ds(start, count), cols] = values[at : at + count, :]
            at += count

    def feed_up(pieces):
        for start, count in pieces:
            row_scales(x2buf, start, count)

        @pl.loop(0, 2)
        def _(j):
            upper = jnp.dot(gathered_rows(x2buf, pieces), we[j], preferred_element_type=F32)
            upper = upper * jnp.concatenate([gathered_rows(rbuf, pieces)] * 8, axis=1)
            hidden = jnp.square(jnp.maximum(upper, 0.0)).astype(BF16)
            store_rows(hbuf, pieces, pl.ds(pl.multiple_of(j * HW, HW), HW), hidden)

    def shard_of(dx, dz):
        return lax.rem(zl + 4 - dz, 4) * 4 + lax.rem(x + 4 - dx, 4)

    columns = [[shard_of(*offsets) for offsets in group] for group in (FIRST, LAST)]

    def feed_down(pieces, g):
        weights = jnp.concatenate([wr[shard] for shard in columns[g]], axis=1)
        product = jnp.dot(gathered_rows(hbuf, pieces), weights, preferred_element_type=F32)
        store_rows(part2.at[g], pieces, slice(None), product.astype(BF16))

    def feed_own(g):
        weights = jnp.concatenate([wr[shard] for shard in columns[g]], axis=1)
        rows = pl.ds(SO * R, R)
        middle = [x2buf[rows, pl.ds(pl.multiple_of(shard * 128, 128), 128)] for shard in columns[g]]
        product = jnp.dot(hbuf[rows, :], weights, preferred_element_type=F32)
        base[g] = jnp.concatenate(middle, axis=1).astype(F32) + product.astype(BF16).astype(F32)

    row_scales(xbuf, SO * R, R)
    with scope("v_w1"):
        value_blocks.wave(1)
    with scope("dm_w1"):
        dm_blocks.wave(1)
    pl.when(c == 0)(send_tokens)

    @pl.when(c == 1)
    def _():
        gather_pass_on(xbuf, 0, 0)
        gather_pass_on(xbuf, 0, 1)

    with scope("v_w2"):
        value_blocks.wave(2)

    with scope("dm_w2"):
        dm_blocks.wave(2)
    expand_blocks.wave(0)

    @pl.when(c == 1)
    def _():
        with scope("scales_1"):
            gather_near(xbuf, 0)
            row_scales(xbuf, 0, 2 * R)

    @pl.when(c == 0)
    def _():
        with scope("pass1_0"):
            gather_pass_on(xbuf, 0, 0)

    reduce_low.wave(0)
    with scope("v_w3"):
        value_blocks.wave(3)

    @pl.when(c == 1)
    def _():
        gather_far(xbuf, 0)
        row_scales(xbuf, 2 * R, R)

    @pl.when(c == 0)
    def _():
        with scope("pass1_1"):
            gather_pass_on(xbuf, 0, 1)

    with scope("v_d2d"):
        value_blocks.shared(0)
        value_blocks.shared(1)

    @pl.when(c == 1)
    def _():
        with scope("project_all"):
            project((SN, SP, SF, SO))

    @pl.when(c == 0)
    def _():
        with scope("project_own"):
            project((SO,))

    with scope("dm_w3"):
        dm_blocks.wave(3)

    @pl.when(c == 0)
    def _():
        with scope("scales_0"):
            gather_near(xbuf, 0)
            row_scales(xbuf, 0, 2 * R)
        with scope("project_near"):
            project((SN, SP))
        with scope("far1"):
            gather_far(xbuf, 0)
            row_scales(xbuf, 2 * R, R)
        with scope("project_far"):
            project((SF,))

    stat_copies = [
        rcopy(stat.at[0], stat.at[k + 1], st_send.at[0], st_recv.at[0], to)
        for k, to in enumerate((ynext, yprev, yfar))
    ]
    for copy in stat_copies:
        copy.start()

    @pl.when(c == 0)
    def _():
        with scope("e_w1_0"):
            expand_blocks.wave(1)

    reduce_high.wave(0)
    with scope("dm_d2d"):
        dm_blocks.shared(0)
        dm_blocks.shared(1)
    with scope("direct"):
        project_direct(0)
        rcopy(small.at[other], small.at[other], sm_send.at[0], sm_recv.at[0], sib).wait_recv()
        rcopy(swb.at[other], swb.at[other], sm_send.at[1], sm_recv.at[1], sib).wait_recv()
        for k in range(2):
            rows = jnp.concatenate(
                [jnp.broadcast_to(small[k, 2 + g : 3 + g, :], (64, 128)) for g in range(2)], axis=0
            )
            bias[k] = jnp.transpose(rows)

    @pl.when(c == 1)
    def _():
        with scope("e_w1_1"):
            expand_blocks.wave(1)

    with scope("wait_stats"):
        all_stats = stat.at[pl.ds(1, 3)]
        rcopy(all_stats, all_stats, st_send.at[0], st_recv.at[0], sib).wait_recv()
        totals[...] = stat[0] + stat[1] + stat[2] + stat[3]
    with scope("mixing_near"):
        mixing((SN, SP))
    mixer_sums.own()
    project_direct(256)
    with scope("mixing_far"):
        mixing((SF,))
    mixer_sums.far()
    with scope("mixing_own"):
        mixing((SO,))

    @pl.when(c == 1)
    def _():
        with scope("join1_0_1"):
            mixer_sums.join(0)

    with scope("e_w2"):
        expand_blocks.wave(2)
    with scope("r0_w1"):
        reduce_low.wave(1)

    @pl.when(c == 0)
    def _():
        with scope("join1_0_0"):
            mixer_sums.join(0)

    with scope("join1_1"):
        mixer_sums.join(1)
    with scope("e_w3"):
        expand_blocks.wave(3)
    with scope("r1_w1"):
        reduce_high.wave(1)

    def middle_done(row, total):
        rows = pl.ds(SO * R + row, CHUNK)
        x2buf[rows, :] = (xbuf[rows, :].astype(F32) + total).astype(BF16)

    with scope("finish1_0"):
        mixer_sums.finish(0, middle_done)
    for way in range(2):
        gather_copy(x2buf, 1, way, 2 * way).start()
    with scope("finish1_1"):
        mixer_sums.finish(1, middle_done)
    for way in range(2):
        gather_copy(x2buf, 1, way, 2 * way + 1).start()
    with scope("r0_w2"):
        reduce_low.wave(2)
    with scope("e_w4"):
        expand_blocks.wave(4)
    with scope("pass2_0"):
        gather_pass_on(x2buf, 1, 0)
    with scope("r1_w2"):
        reduce_high.wave(2)
    with scope("pass2_1"):
        gather_pass_on(x2buf, 1, 1)
    for k in range(2):
        for way in range(2):
            gather_copy(x2buf, 1, way, 2 * (1 - way) + k).start()

    outer, inner = ((64, 128),), ((0, 64), (192, 64))
    far, own = ((SF * R, R),), ((SO * R, R),)
    with scope("e_d2d"):
        expand_blocks.shared(0)
        expand_blocks.shared(1)
    with scope("up_outer"):
        feed_up(outer)
    with scope("r0_w3"):
        reduce_low.wave(3)
    with scope("r_d2d_0"):
        reduce_low.shared(0)
        reduce_high.shared(0)
    with scope("down_outer_0"):
        feed_down(outer, 0)
    ff_sums[0].own()
    with scope("r1_w3"):
        reduce_high.wave(3)
    with scope("up_own"):
        feed_up(own)
    with scope("far2"):
        gather_far(x2buf, 1)
    with scope("r0_w4"):
        reduce_low.wave(4)
    with scope("r1_w4"):
        reduce_high.wave(4)
    with scope("feed_far_0"):
        feed_up(far)
        feed_down(far, 0)
    ff_sums[0].far()
    with scope("down_own_0"):
        feed_own(0)
    with scope("r_d2d_1"):
        reduce_low.shared(1)
        reduce_high.shared(1)
    with scope("down_outer_1"):
        feed_down(outer, 1)
    ff_sums[1].own()
    with scope("down_far_1"):
        feed_down(far, 1)
    ff_sums[1].far()
    with scope("near2"):
        gather_near(x2buf, 1)
    with scope("feed_inner_0"):
        feed_up(inner)
        feed_down(inner, 0)
    with scope("join2_0"):
        ff_sums[0].join(0)
        ff_sums[0].join(1)
    with scope("feed_inner_1"):
        feed_down(inner, 1)
    with scope("join2_1_0"):
        ff_sums[1].join(0)
    with scope("join2_1_1"):
        ff_sums[1].join(1)
    with scope("down_own_1"):
        feed_own(1)

    def result_done(g):
        def done(row, total):
            total = total.astype(BF16)
            for p, shard in enumerate(columns[g]):
                lanes = pl.ds(pl.multiple_of(shard * 128, 128), 128)
                out[pl.ds(row, CHUNK), lanes] = total[:, p * 128 : (p + 1) * 128]

        return done

    for g in range(2):
        for k in range(2):
            with scope(f"finish2_{g}_{k}"):
                ff_sums[g].finish(k, result_done(g))

    with scope("drain"):
        for phase, buf in ((0, xbuf), (1, x2buf)):
            ref = buf.at[pl.ds(0, 12 * CHUNK)]
            rcopy(ref, ref, ag_send.at[phase], ag_recv.at[phase, 0], sib).wait_send()
        for sums in (mixer_sums, *ff_sums):
            ref = sums.part.at[pl.ds(0, 12 * CHUNK)]
            rcopy(ref, ref, rs_send.at[sums.stage], rs_recv.at[sums.stage, 0], sib).wait_send()
        rcopy(all_stats, all_stats, st_send.at[0], st_recv.at[0], sib).wait_send()
        for copy in (small_copy, spatial_copy):
            copy.wait_send()
        for blocks in (value_blocks, dm_blocks, expand_blocks, reduce_low, reduce_high):
            blocks.sent()


def layer(*args):
    (
        tokens,
        mixer_gain,
        direct_weight,
        direct_scale,
        value_weight,
        value_scale,
        value_gain,
        value_shift,
        spatial_weight,
        spatial_bias,
        merge_weight,
        merge_scale,
        channel_gain,
        expand_weight,
        expand_scale,
        reduce_weight,
        reduce_scale,
    ) = args
    operands = (
        tokens,
        mixer_gain.reshape(16, 128),
        direct_weight,
        direct_scale.reshape(1, CW),
        value_weight,
        value_scale.reshape(1, CW),
        value_gain.reshape(1, CW),
        value_shift.reshape(1, CW),
        spatial_weight,
        spatial_bias,
        merge_weight,
        merge_scale.reshape(1, 128),
        channel_gain.reshape(16, 128),
        expand_weight,
        expand_scale.reshape(1, HW),
        reduce_weight,
        reduce_scale.reshape(1, 128),
    )
    dma = pltpu.SemaphoreType.DMA
    return pl.pallas_call(
        kernel,
        out_shape=jax.ShapeDtypeStruct((R, D), BF16),
        in_specs=[pl.BlockSpec(memory_space=pl.ANY)] * 17,
        out_specs=pl.BlockSpec(memory_space=pltpu.VMEM),
        scratch_shapes=[
            *(pltpu.VMEM(operand.shape, operand.dtype) for operand in operands[1:]),
            pltpu.VMEM((2, D, 128), BF16),
            pltpu.VMEM((2, D, 256), BF16),
            pltpu.VMEM((2, D, HW), BF16),
            pltpu.VMEM((16, 2 * HW, 128), BF16),
            pltpu.VMEM((4 * R, D), BF16),
            pltpu.VMEM((4 * R, D), BF16),
            pltpu.VMEM((4 * R, D), BF16),
            pltpu.VMEM((2, 4 * R, D // 2), BF16),
            pltpu.VMEM((2, 64, D), BF16),
            pltpu.VMEM((2, R, D), BF16),
            pltpu.VMEM((2, 64, D), BF16),
            pltpu.VMEM((2, 2, 64, D // 2), BF16),
            pltpu.VMEM((2, 2, R, D // 2), BF16),
            pltpu.VMEM((2, 2, 64, D // 2), BF16),
            pltpu.VMEM((4 * R, D), BF16),
            pltpu.VMEM((4 * R, 256), F32),
            pltpu.VMEM((4 * R, 256), F32),
            pltpu.VMEM((4 * R, 256), BF16),
            pltpu.VMEM((4 * R, 128), F32),
            pltpu.VMEM((4, 8, 128), F32),
            pltpu.VMEM((8, 128), F32),
            pltpu.VMEM((2, 8, 128), F32),
            pltpu.VMEM((2, 2, 128, 128), BF16),
            pltpu.VMEM((2, 128, 128), F32),
            pltpu.VMEM((2, R, D // 2), F32),
            dma((17,)),
            dma((2,)),
            dma((2, 4)),
            dma((3,)),
            dma((3, 5)),
            dma((1,)),
            dma((1,)),
            dma((2,)),
            dma((2,)),
            dma((10,)),
            dma((10,)),
            dma((10, 8)),
            dma((10, 2)),
        ],
        compiler_params=pltpu.CompilerParams(
            collective_id=0, has_side_effects=True, vmem_limit_bytes=52 * 1024 * 1024
        ),
        name="layer",
    )(*(pltpu.with_memory_space_constraint(operand, pltpu.HBM) for operand in operands))


def solution(mesh):
    finer = Mesh(mesh.devices.reshape(2, 4, 4, 4, 2), AXES)
    in_specs = (
        P(AXES, None),
        P(),
        P(FS, TP),
        P(TP),
        P(FS, TP),
        P(TP),
        P(TP),
        P(TP),
        P(TP, None, None),
        P(TP, None),
        P(TP, FS),
        P(FS),
        P(),
        P(FS, TP),
        P(TP),
        P(TP, FS),
        P(FS),
    )
    return jax.shard_map(layer, mesh=finer, in_specs=in_specs, out_specs=P(AXES, None), check_vma=False)
```
